32 devices in a mesh: grp: 2 (over y), sp: 4 (over z), tp: 4 (over x, core).
Axes of the slice: x: 2, y: 2, z: 4, core: 2. Of those that a mesh axis runs over, the one named last changes fastest.
Arguments:
- tokens: bfloat16 [2048, 4096], P(('grp', 'sp')), parts along dimension 0, may hold values from -6 to 6
- norm_gain: bfloat16 [2, 4096], replicated, may hold values from 0.099609375 to 1.8984375
- w_query: bfloat16 [2, 4096, 2048], P(None, 'sp', 'tp'), may hold values from -0.09375 to 0.09375
- w_key: bfloat16 [2, 4096, 2048], P(None, 'sp', 'tp'), may hold values from -0.09375 to 0.09375
- w_value: bfloat16 [2, 4096, 2048], P(None, 'sp', 'tp'), may hold values from -0.09375 to 0.09375
- w_out: bfloat16 [2, 2048, 4096], P(None, 'tp', 'sp'), may hold values from -0.125 to 0.125
- offset_bias: float32 [2, 16, 15, 31], P(None, 'tp'), may hold values from -4 to 300
Outputs:
- mixed: bfloat16 [2048, 4096], P(('grp', 'sp')), parts along dimension 0
The draws below stay inside these ranges and needn't reach their ends.
There are 2 independent parts, one for each index of `grp`. The reference program is written for one: setup_inputs(seed, part) draws one part's arguments, and reference() takes and returns one part's arrays. A program takes and returns all parts, laid end to end along the dimension named above; an argument that names none is the same for every part. Nothing has to cross between parts.
All inputs are finite; a program needn't handle non-finite values.
Results may differ from the reference program's by a relative error of at most 0.013.
Values may be sent and summed in bfloat16 or wider, within the bound.
No kernel may reach another device: no remote copies, remote signals or barrier semaphores. Data moves between devices by JAX's collectives and lax.ppermute only.
A program may use at most 128 MiB of HBM per device.

```python
import jax
import jax.numpy as jnp
from jax import lax

D = 4096
HEADS = 16
HD = 128
GRID_W = 64
KR = 8
KC = 16
LAYERS = 2
ROWS_DEV = 4
TOKENS = 1024
N_SP = 4
N_TP = 4


def draw_offset_bias(key, part):
    shape = (LAYERS, HEADS, 2 * KR - 1, 2 * KC - 1)
    first_key, second_key = jax.random.split(jax.random.fold_in(key, 17))
    base = jnp.clip(jax.random.normal(first_key, shape, jnp.float32), -4.0, 4.0)
    return base


def steps_of(key, shape, shards, least, largest):
    factor_of, own = 1.0, jax.random.fold_in(key, 6)
    for position, parts in shards:
        heights = jnp.exp(jax.random.uniform(jax.random.fold_in(own, position), (parts,), jnp.float32, least / len(shards), largest / len(shards)))
        factor_of = factor_of * jnp.repeat(heights, shape[position] // parts).reshape([-1 if axis == position else 1 for axis in range(len(shape))])
    return factor_of


def scatter_about(own_key, dims, scale, most, pieces=(), kind=jnp.bfloat16):
    values = jax.random.normal(own_key, dims, jnp.float32) * scale
    if len(pieces) > 0:
        values = steps_of(own_key, dims, pieces, -0.22, 0.18) * values
    return jnp.clip(values, min=-most, max=most).astype(kind)


def setup_inputs(seed: int = 0, part: int = 0) -> dict:
    key_list = jax.random.split(jax.random.key(seed), 8)
    part_keys = jax.random.split(jax.random.fold_in(key_list[7], part), 8)
    tokens = scatter_about(part_keys[0], (TOKENS, D), 1.0, 6.0, ((0, 4),))
    norm_gain = jnp.clip(1.0 + 0.18 * jax.random.normal(key_list[1], (LAYERS, D), jnp.float32), 0.099609375, 1.8984375).astype(jnp.bfloat16)
    w_query = scatter_about(key_list[2], (LAYERS, D, HEADS * HD), D ** -0.5, 0.09375, ((1, 4), (2, 4)))
    w_key = scatter_about(key_list[3], (LAYERS, D, HEADS * HD), D ** -0.5, 0.09375, ((1, 4), (2, 4)))
    w_value = scatter_about(key_list[4], (LAYERS, D, HEADS * HD), D ** -0.5, 0.09375, ((1, 4), (2, 4)))
    w_out = scatter_about(key_list[5], (LAYERS, HEADS * HD, D), (HEADS * HD) ** -0.5, 0.125, ((1, 4), (2, 4)))
    offset_bias = draw_offset_bias(jax.random.fold_in(key_list[7], 71), part)
    return dict(tokens=tokens, norm_gain=norm_gain, w_query=w_query, w_key=w_key, w_value=w_value, w_out=w_out, offset_bias=offset_bias)


norm_eps = 1e-06

def rms_rows(values, gain):
    wide = values.astype(jnp.float32)
    scaled = wide * lax.rsqrt(lax.optimization_barrier(jnp.mean(wide * wide, axis=-1, keepdims=True)) + norm_eps)
    return (scaled * gain.astype(jnp.float32)).astype(jnp.bfloat16)

def reference(tokens, norm_gain, w_query, w_key, w_value, w_out, offset_bias):
    grid_rows = ROWS_DEV * N_SP
    group_width = HEADS // N_TP * HD
    scale = HD ** (-0.5)
    columns = jnp.arange(GRID_W, dtype=jnp.int32)
    col_first = jnp.clip(columns - KC // 2, 0, GRID_W - KC)
    col_inside = (columns[None, :] >= col_first[:, None]) & (columns[None, :] < col_first[:, None] + KC)
    col_offset = jnp.clip(columns[None, :] - columns[:, None], 1 - KC, KC - 1) + KC - 1
    row_first = jnp.clip(jnp.arange(grid_rows, dtype=jnp.int32) - KR // 2, 0, grid_rows - KR)
    residual = tokens
    for layer_index in range(LAYERS):
        normed = rms_rows(residual, norm_gain[layer_index])
        queries = jnp.dot(normed, w_query[layer_index], preferred_element_type=jnp.float32).astype(jnp.bfloat16)
        keys = jnp.dot(normed, w_key[layer_index], preferred_element_type=jnp.float32).astype(jnp.bfloat16)
        values = jnp.dot(normed, w_value[layer_index], preferred_element_type=jnp.float32).astype(jnp.bfloat16)
        queries = queries.reshape(grid_rows, GRID_W, HEADS, HD)
        keys = keys.reshape(grid_rows, GRID_W, HEADS, HD)
        values = values.reshape(grid_rows, GRID_W, HEADS, HD)
        col_bias = offset_bias[layer_index].astype(jnp.float32)[:, :, col_offset]

        def attend_row(packed, keys=keys, values=values, col_bias=col_bias):
            row_index, row_queries = packed
            row_begin = row_first[row_index].astype(jnp.int32)
            row_keys = lax.dynamic_slice_in_dim(keys, row_begin, KR, 0).astype(jnp.float32)
            row_values = lax.dynamic_slice_in_dim(values, row_begin, KR, 0).astype(jnp.float32)
            picked = row_begin + jnp.arange(KR, dtype=jnp.int32) - row_index + KR - 1
            bias = jnp.transpose(col_bias[:, picked], (0, 2, 1, 3))
            scores = jnp.einsum('qhd,jkhd->hqjk', row_queries.astype(jnp.float32), row_keys) * scale + bias
            scores = jnp.where(col_inside[None, :, None, :], scores, -jnp.inf)
            weights = jax.nn.softmax(scores.reshape(HEADS, GRID_W, KR * GRID_W), axis=-1).astype(jnp.bfloat16)
            weights = lax.optimization_barrier(weights)
            weights = weights.reshape(HEADS, GRID_W, KR, GRID_W).astype(jnp.float32)
            return jnp.einsum('hqjk,jkhd->qhd', weights, row_values).astype(jnp.bfloat16)
        attended = lax.map(attend_row, (jnp.arange(grid_rows, dtype=jnp.int32), queries))
        attended = attended.reshape(grid_rows * GRID_W, HEADS * HD)
        branch = jnp.zeros(residual.shape, jnp.float32)
        for group_index in range(N_TP):
            lower = group_index * group_width
            rounded = jnp.dot(attended[:, lower:lower + group_width], w_out[layer_index][lower:lower + group_width], preferred_element_type=jnp.float32).astype(jnp.bfloat16)
            branch = branch + lax.optimization_barrier(rounded).astype(jnp.float32)
        residual = (residual.astype(jnp.float32) + branch).astype(jnp.bfloat16)
    return residual
```

```python
import functools

import jax
import jax.numpy as jnp
from jax import lax
from jax.experimental import pallas as pl
from jax.experimental.pallas import tpu as pltpu
from jax.sharding import PartitionSpec as P

HD = 128
GRID_W = 64
KR = 8
KC = 16
LAYERS = 2


norm_eps = 1e-06


def with_halo(block, sides, width):
    for axis, dim in sides:
        count = lax.axis_size(axis)
        forward = [(i, i + 1) for i in range(count - 1)]
        backward = [(target, source) for source, target in forward]
        low = lax.ppermute(
            lax.slice_in_dim(block, block.shape[dim] - width, None, axis=dim), axis, forward
        )
        high = lax.ppermute(lax.slice_in_dim(block, 0, width, axis=dim), axis, backward)
        block = jnp.concatenate([low, block, high], axis=dim)
    return block


def rms_rows(values, gain):
    wide = values.astype(jnp.float32)
    scaled = wide * lax.rsqrt(jnp.mean(wide * wide, axis=-1, keepdims=True) + norm_eps)
    return (scaled * gain.astype(jnp.float32)).astype(jnp.bfloat16)


def gathered_plan(tokens, norm_gain, w_query, w_key, w_value, w_out, offset_bias):
    sp_count = lax.axis_size("sp")
    sp_index = lax.axis_index("sp")
    tok_rows = tokens.shape[0]
    local_rows = tok_rows // GRID_W
    grid_rows = local_rows * sp_count
    heads_here = offset_bias.shape[1]
    head_width = heads_here * HD
    reach = KR // 2
    scale = HD ** (-0.5)
    columns = jnp.arange(GRID_W, dtype=jnp.int32)
    col_first = jnp.clip(columns - KC // 2, 0, GRID_W - KC)
    col_inside = (columns[None, :] >= col_first[:, None]) & (
        columns[None, :] < col_first[:, None] + KC
    )
    col_offset = jnp.clip(columns[None, :] - columns[:, None], 1 - KC, KC - 1) + KC - 1
    col_onehot = (
        jnp.arange(2 * KC - 1, dtype=jnp.int32)[:, None, None] == col_offset[None, :, :]
    ).astype(jnp.float32)
    first_row = sp_index * local_rows
    own_rows = first_row + jnp.arange(local_rows, dtype=jnp.int32)
    row_first = jnp.clip(own_rows - reach, 0, grid_rows - KR)
    band_start = row_first - first_row + reach
    row_offset = (
        row_first[:, None] + jnp.arange(KR, dtype=jnp.int32)[None, :] - own_rows[:, None] + KR - 1
    )
    row_onehot = (
        row_offset[:, :, None] == jnp.arange(2 * KR - 1, dtype=jnp.int32)[None, None, :]
    ).astype(jnp.float32)
    every_query, every_key, every_value, every_out = (
        lax.all_gather(w_query, "sp", axis=1, tiled=True),
        lax.all_gather(w_key, "sp", axis=1, tiled=True),
        lax.all_gather(w_value, "sp", axis=1, tiled=True),
        lax.all_gather(w_out, "sp", axis=2, tiled=True),
    )
    residual = tokens
    for layer_index in range(LAYERS):
        normed = rms_rows(residual, norm_gain[layer_index])
        queries = jnp.dot(normed, every_query[layer_index], preferred_element_type=jnp.float32)
        keys = jnp.dot(normed, every_key[layer_index], preferred_element_type=jnp.float32)
        values = jnp.dot(normed, every_value[layer_index], preferred_element_type=jnp.float32)
        out_weight = every_out[layer_index]
        queries = queries.astype(jnp.bfloat16).reshape(local_rows, GRID_W, heads_here, HD)
        key_values = jnp.concatenate(
            [keys.astype(jnp.bfloat16), values.astype(jnp.bfloat16)], axis=1
        )
        key_values = key_values.reshape(local_rows, GRID_W, 2 * head_width)
        padded = with_halo(key_values, (("sp", 0),), reach)
        bands = jax.vmap(lambda band_begin: lax.dynamic_slice_in_dim(padded, band_begin, KR, 0))(
            band_start
        )
        band_keys = bands[..., :head_width].reshape(local_rows, KR, GRID_W, heads_here, HD)
        band_values = bands[..., head_width:].reshape(local_rows, KR, GRID_W, heads_here, HD)
        col_bias = jnp.einsum(
            "hro,oqk->hrqk", offset_bias[layer_index], col_onehot, precision=lax.Precision.HIGHEST
        )
        full_bias = jnp.einsum(
            "ijr,hrqk->hiqjk", row_onehot, col_bias, precision=lax.Precision.HIGHEST
        )
        scores = jnp.einsum(
            "iqhd,ijkhd->hiqjk", queries, band_keys, preferred_element_type=jnp.float32
        )
        scores = scores * scale + full_bias
        scores = jnp.where(col_inside[None, None, :, None, :], scores, -jnp.inf)
        flattened = scores.reshape(heads_here, local_rows, GRID_W, KR * GRID_W)
        weights = jax.nn.softmax(flattened, axis=-1).astype(jnp.bfloat16)
        weights = weights.reshape(heads_here, local_rows, GRID_W, KR, GRID_W)
        attended = jnp.einsum(
            "hiqjk,ijkhd->iqhd", weights, band_values, preferred_element_type=jnp.float32
        )
        attended = attended.astype(jnp.bfloat16).reshape(tok_rows, head_width)
        branch = lax.psum(
            jnp.dot(attended, out_weight, preferred_element_type=jnp.float32).astype(jnp.bfloat16),
            "tp",
        ).astype(jnp.float32)
        residual = (residual.astype(jnp.float32) + branch).astype(jnp.bfloat16)
    return residual


def ring(count, shift):
    return [(i, (i + shift) % count) for i in range(count)]


def swapped(array, axis, distance):
    count = lax.axis_size(axis)
    return lax.ppermute(array, axis, [(i, i ^ distance) for i in range(count)])


def ordered(mine, theirs, mine_is_low, axis):
    low = jnp.where(mine_is_low, mine, theirs)
    high = jnp.where(mine_is_low, theirs, mine)
    return jnp.concatenate([low, high], axis=axis)


def summed_over(vector, axis):
    count = lax.axis_size(axis)
    distance = 1
    while distance < count:
        vector = vector + swapped(vector, axis, distance)
        distance *= 2
    return vector


def window_bias(table):
    heads = table.shape[0]
    columns = jnp.arange(GRID_W, dtype=jnp.int32)
    first = jnp.clip(columns - KC // 2, 0, GRID_W - KC)
    inside = (columns[None, :] >= first[:, None]) & (columns[None, :] < first[:, None] + KC)
    offset = jnp.clip(columns[None, :] - columns[:, None], 1 - KC, KC - 1) + KC - 1
    onehot = (
        jnp.arange(2 * KC - 1, dtype=jnp.int32)[:, None, None] == offset[None, :, :]
    ).astype(jnp.float32)
    wide = jnp.einsum("hro,oqk->hqrk", table, onehot, precision=lax.Precision.HIGHEST)
    wide = jnp.where(inside[None, :, None, :], wide, -jnp.inf)
    return wide.reshape(heads, GRID_W, (2 * KR - 1) * GRID_W)


def attend_kernel(heads, grid_rows, arrived_ref, own_ref, norm_ref, bias_ref, out_ref, qkv_ref):
    total = arrived_ref[...].astype(jnp.float32) + own_ref[...].astype(jnp.float32)
    qkv_ref[...] = (total * norm_ref[...]).astype(jnp.bfloat16)
    width = heads * HD
    for head in range(heads):
        lanes = head * HD
        for row in range(grid_rows):
            first = min(max(row - KR // 2, 0), grid_rows - KR)
            offset = first - row + KR - 1
            queries = qkv_ref[pl.ds(row * GRID_W, GRID_W), pl.ds(lanes, HD)]
            keys = qkv_ref[pl.ds(first * GRID_W, KR * GRID_W), pl.ds(width + lanes, HD)]
            values = qkv_ref[pl.ds(first * GRID_W, KR * GRID_W), pl.ds(2 * width + lanes, HD)]
            scores = lax.dot_general(
                queries, keys, (((1,), (1,)), ((), ())), preferred_element_type=jnp.float32
            )
            bias = bias_ref[head, :, pl.ds(offset * GRID_W, KR * GRID_W)]
            scores = scores * HD ** (-0.5) + bias
            powers = jnp.exp(scores - jnp.max(scores, axis=-1, keepdims=True))
            weights = powers / jnp.sum(powers, axis=-1, keepdims=True)
            mixed = jnp.dot(
                weights.astype(jnp.bfloat16), values, preferred_element_type=jnp.float32
            )
            out_ref[pl.ds(row * GRID_W, GRID_W), pl.ds(lanes, HD)] = mixed.astype(jnp.bfloat16)


def attend(arrived, own, norm, bias):
    tok, width = arrived.shape
    heads = bias.shape[0]
    grid_rows = tok // GRID_W
    return pl.pallas_call(
        functools.partial(attend_kernel, heads, grid_rows),
        out_shape=jax.ShapeDtypeStruct((tok, width // 3), jnp.bfloat16),
        in_specs=[pl.BlockSpec(memory_space=pltpu.VMEM)] * 4,
        out_specs=pl.BlockSpec(memory_space=pltpu.VMEM),
        scratch_shapes=[pltpu.VMEM((tok, width), jnp.bfloat16)],
        compiler_params=pltpu.CompilerParams(vmem_limit_bytes=32 * 1024 * 1024),
        cost_estimate=pl.CostEstimate(
            flops=4 * heads * tok * KR * GRID_W * HD,
            bytes_accessed=8 * tok * width,
            transcendentals=heads * tok * KR * GRID_W,
        ),
        name="attend",
    )(arrived, own, norm, bias)


def stationary_plan(tokens, norm_gain, w_query, w_key, w_value, w_out, offset_bias):
    sp_count, tp_count = lax.axis_size("sp"), lax.axis_size("tp")
    sp_index, tp_index = lax.axis_index("sp"), lax.axis_index("tp")
    core, far = tp_index % 2, tp_index // 2
    tok_here = tokens.shape[0]
    tok = tok_here * sp_count
    feats = w_query.shape[1]
    heads = offset_bias.shape[1] // sp_count
    width = heads * HD
    half, piece = feats // 2, feats // 4
    slot = core * 2 + far
    every_feat = feats * sp_count

    def source(shift):
        return (sp_index - shift) % sp_count

    held = jnp.zeros((tok, piece), jnp.bfloat16)
    for shift in range(sp_count):
        target = (sp_index + shift) % sp_count
        block = lax.dynamic_slice_in_dim(tokens, target * feats + slot * piece, piece, 1)
        if shift:
            block = lax.ppermute(block, "sp", ring(sp_count, shift))
        held = lax.dynamic_update_slice_in_dim(held, block, source(shift) * tok_here, 0)
    x_half = ordered(held, swapped(held, "tp", 2), far == 0, 1)
    x = ordered(x_half, swapped(x_half, "tp", 1), core == 0, 1)

    for layer in range(LAYERS):
        gain = lax.dynamic_slice_in_dim(norm_gain[layer], sp_index * feats, feats, 0)
        wide = x.astype(jnp.float32)
        scaled = (wide * gain.astype(jnp.float32)).astype(jnp.bfloat16)
        squares = summed_over(jnp.sum(wide * wide, axis=-1).reshape(tok // HD, HD), "sp")
        norm = lax.rsqrt(squares.reshape(tok, 1) / every_feat + norm_eps)

        def partial_of(chunk, layer=layer, scaled=scaled):
            weights = jnp.concatenate(
                [
                    lax.dynamic_slice_in_dim(w[layer], chunk * width, width, 1)
                    for w in (w_query, w_key, w_value)
                ],
                axis=1,
            )
            return jnp.dot(scaled, weights, preferred_element_type=jnp.float32)

        travelling = partial_of(source(1)).astype(jnp.bfloat16)
        for step in range(1, sp_count):
            travelling = lax.ppermute(travelling, "sp", ring(sp_count, 1))
            own = partial_of(source(step + 1))
            if step < sp_count - 1:
                travelling = (travelling.astype(jnp.float32) + own).astype(jnp.bfloat16)
        table = lax.dynamic_slice_in_dim(offset_bias[layer], sp_index * heads, heads, 0)
        attended = attend(travelling, own, norm, window_bias(table))

        gathered = [attended] + [
            lax.ppermute(attended, "sp", ring(sp_count, shift)) for shift in range(1, sp_count)
        ]
        out_rows = jnp.concatenate(
            [
                lax.dynamic_slice_in_dim(w_out[layer], source(shift) * width, width, 0)
                for shift in range(sp_count)
            ],
            axis=0,
        )
        product = jnp.dot(
            jnp.concatenate(gathered, axis=1), out_rows, preferred_element_type=jnp.float32
        ).astype(jnp.bfloat16)
        sent = lax.dynamic_slice_in_dim(product, (1 - core) * half, half, 1)
        kept = lax.dynamic_slice_in_dim(product, core * half, half, 1)
        pair = kept.astype(jnp.float32) + swapped(sent, "tp", 1).astype(jnp.float32)
        pair = pair.astype(jnp.bfloat16)
        if layer < LAYERS - 1:
            branch = pair.astype(jnp.float32) + swapped(pair, "tp", 2).astype(jnp.float32)
            x_half = (x_half.astype(jnp.float32) + branch).astype(jnp.bfloat16)
            x = ordered(x_half, swapped(x_half, "tp", 1), core == 0, 1)

    sent = lax.dynamic_slice_in_dim(pair, (1 - far) * piece, piece, 1)
    kept = lax.dynamic_slice_in_dim(pair, far * piece, piece, 1)
    branch = kept.astype(jnp.float32) + swapped(sent, "tp", 2).astype(jnp.float32)
    residual = lax.dynamic_slice_in_dim(x_half, far * piece, piece, 1)
    last = (residual.astype(jnp.float32) + branch).astype(jnp.bfloat16)
    mixed = jnp.zeros((tok_here, sp_count, piece), jnp.bfloat16)
    for shift in range(sp_count):
        target = (sp_index + shift) % sp_count
        block = lax.dynamic_slice_in_dim(last, target * tok_here, tok_here, 0)
        if shift:
            block = lax.ppermute(block, "sp", ring(sp_count, shift))
        mixed = lax.dynamic_update_slice_in_dim(mixed, block[:, None], source(shift), 1)
    mixed = ordered(mixed, swapped(mixed, "tp", 2), far == 0, 2)
    mixed = ordered(mixed, swapped(mixed, "tp", 1), core == 0, 2)
    return mixed.reshape(tok_here, every_feat)


def on_device(tokens, norm_gain, w_query, w_key, w_value, w_out, offset_bias):
    heads_here = offset_bias.shape[1]
    plan = gathered_plan
    if heads_here % lax.axis_size("sp") == 0 and lax.axis_size("tp") == 4:
        plan = stationary_plan
    return plan(tokens, norm_gain, w_query, w_key, w_value, w_out, offset_bias)


def solution(mesh):
    return jax.shard_map(
        on_device,
        mesh=mesh,
        in_specs=(
            P(("grp", "sp"), None),
            P(),
            P(None, "sp", "tp"),
            P(None, "sp", "tp"),
            P(None, "sp", "tp"),
            P(None, "tp", "sp"),
            P(None, "tp", None, None),
        ),
        out_specs=P(("grp", "sp"), None),
        check_vma=False,
    )
```

```python
import functools

import jax
import jax.numpy as jnp
from jax import lax
from jax.experimental import pallas as pl
from jax.experimental.pallas import tpu as pltpu
from jax.sharding import PartitionSpec as P

HD = 128
GRID_W = 64
KR = 8
KC = 16
LAYERS = 2


norm_eps = 1e-06


def with_halo(block, sides, width):
    for axis, dim in sides:
        count = lax.axis_size(axis)
        forward = [(i, i + 1) for i in range(count - 1)]
        backward = [(target, source) for source, target in forward]
        low = lax.ppermute(
            lax.slice_in_dim(block, block.shape[dim] - width, None, axis=dim), axis, forward
        )
        high = lax.ppermute(lax.slice_in_dim(block, 0, width, axis=dim), axis, backward)
        block = jnp.concatenate([low, block, high], axis=dim)
    return block


def rms_rows(values, gain):
    wide = values.astype(jnp.float32)
    scaled = wide * lax.rsqrt(jnp.mean(wide * wide, axis=-1, keepdims=True) + norm_eps)
    return (scaled * gain.astype(jnp.float32)).astype(jnp.bfloat16)


def gathered_plan(tokens, norm_gain, w_query, w_key, w_value, w_out, offset_bias):
    sp_count = lax.axis_size("sp")
    sp_index = lax.axis_index("sp")
    tok_rows = tokens.shape[0]
    local_rows = tok_rows // GRID_W
    grid_rows = local_rows * sp_count
    heads_here = offset_bias.shape[1]
    head_width = heads_here * HD
    reach = KR // 2
    scale = HD ** (-0.5)
    columns = jnp.arange(GRID_W, dtype=jnp.int32)
    col_first = jnp.clip(columns - KC // 2, 0, GRID_W - KC)
    col_inside = (columns[None, :] >= col_first[:, None]) & (
        columns[None, :] < col_first[:, None] + KC
    )
    col_offset = jnp.clip(columns[None, :] - columns[:, None], 1 - KC, KC - 1) + KC - 1
    col_onehot = (
        jnp.arange(2 * KC - 1, dtype=jnp.int32)[:, None, None] == col_offset[None, :, :]
    ).astype(jnp.float32)
    first_row = sp_index * local_rows
    own_rows = first_row + jnp.arange(local_rows, dtype=jnp.int32)
    row_first = jnp.clip(own_rows - reach, 0, grid_rows - KR)
    band_start = row_first - first_row + reach
    row_offset = (
        row_first[:, None] + jnp.arange(KR, dtype=jnp.int32)[None, :] - own_rows[:, None] + KR - 1
    )
    row_onehot = (
        row_offset[:, :, None] == jnp.arange(2 * KR - 1, dtype=jnp.int32)[None, None, :]
    ).astype(jnp.float32)
    every_query, every_key, every_value, every_out = (
        lax.all_gather(w_query, "sp", axis=1, tiled=True),
        lax.all_gather(w_key, "sp", axis=1, tiled=True),
        lax.all_gather(w_value, "sp", axis=1, tiled=True),
        lax.all_gather(w_out, "sp", axis=2, tiled=True),
    )
    residual = tokens
    for layer_index in range(LAYERS):
        normed = rms_rows(residual, norm_gain[layer_index])
        queries = jnp.dot(normed, every_query[layer_index], preferred_element_type=jnp.float32)
        keys = jnp.dot(normed, every_key[layer_index], preferred_element_type=jnp.float32)
        values = jnp.dot(normed, every_value[layer_index], preferred_element_type=jnp.float32)
        out_weight = every_out[layer_index]
        queries = queries.astype(jnp.bfloat16).reshape(local_rows, GRID_W, heads_here, HD)
        key_values = jnp.concatenate(
            [keys.astype(jnp.bfloat16), values.astype(jnp.bfloat16)], axis=1
        )
        key_values = key_values.reshape(local_rows, GRID_W, 2 * head_width)
        padded = with_halo(key_values, (("sp", 0),), reach)
        bands = jax.vmap(lambda band_begin: lax.dynamic_slice_in_dim(padded, band_begin, KR, 0))(
            band_start
        )
        band_keys = bands[..., :head_width].reshape(local_rows, KR, GRID_W, heads_here, HD)
        band_values = bands[..., head_width:].reshape(local_rows, KR, GRID_W, heads_here, HD)
        col_bias = jnp.einsum(
            "hro,oqk->hrqk", offset_bias[layer_index], col_onehot, precision=lax.Precision.HIGHEST
        )
        full_bias = jnp.einsum(
            "ijr,hrqk->hiqjk", row_onehot, col_bias, precision=lax.Precision.HIGHEST
        )
        scores = jnp.einsum(
            "iqhd,ijkhd->hiqjk", queries, band_keys, preferred_element_type=jnp.float32
        )
        scores = scores * scale + full_bias
        scores = jnp.where(col_inside[None, None, :, None, :], scores, -jnp.inf)
        flattened = scores.reshape(heads_here, local_rows, GRID_W, KR * GRID_W)
        weights = jax.nn.softmax(flattened, axis=-1).astype(jnp.bfloat16)
        weights = weights.reshape(heads_here, local_rows, GRID_W, KR, GRID_W)
        attended = jnp.einsum(
            "hiqjk,ijkhd->iqhd", weights, band_values, preferred_element_type=jnp.float32
        )
        attended = attended.astype(jnp.bfloat16).reshape(tok_rows, head_width)
        branch = lax.psum(
            jnp.dot(attended, out_weight, preferred_element_type=jnp.float32).astype(jnp.bfloat16),
            "tp",
        ).astype(jnp.float32)
        residual = (residual.astype(jnp.float32) + branch).astype(jnp.bfloat16)
    return residual


VMEM_BYTES = 40 * 1024 * 1024


def ring(count, shift):
    return [(i, (i + shift) % count) for i in range(count)]


def swapped(array, axis, distance):
    count = lax.axis_size(axis)
    return lax.ppermute(array, axis, [(i, i ^ distance) for i in range(count)])


def summed_over(vector, axis):
    count = lax.axis_size(axis)
    distance = 1
    while distance < count:
        vector = vector + swapped(vector, axis, distance)
        distance *= 2
    return vector


def aligned(index, size):
    return pl.ds(pl.multiple_of(index * size, size), size)


def local_kernel(body, place, arrays, outs, name, scratch=(), hbm=(), flops=0):
    vmem, smem = pl.BlockSpec(memory_space=pltpu.VMEM), pl.BlockSpec(memory_space=pltpu.SMEM)
    moved = sum(a.size * a.dtype.itemsize for a in (*arrays, *outs))
    return pl.pallas_call(
        body,
        out_shape=list(outs),
        in_specs=[smem] + [vmem] * len(arrays) + [pl.BlockSpec(memory_space=pl.ANY)] * len(hbm),
        out_specs=[vmem] * len(outs),
        scratch_shapes=list(scratch),
        compiler_params=pltpu.CompilerParams(vmem_limit_bytes=VMEM_BYTES),
        cost_estimate=pl.CostEstimate(flops=flops, bytes_accessed=moved, transcendentals=0),
        name=name,
    )(place, *arrays, *hbm)


def shaped(*shape, dtype=jnp.bfloat16):
    return jax.ShapeDtypeStruct(shape, dtype)


def window_bias(table):
    heads = table.shape[0]
    columns = jnp.arange(GRID_W, dtype=jnp.int32)
    first = jnp.clip(columns - KC // 2, 0, GRID_W - KC)
    inside = (columns[None, :] >= first[:, None]) & (columns[None, :] < first[:, None] + KC)
    offset = jnp.clip(columns[None, :] - columns[:, None], 1 - KC, KC - 1) + KC - 1
    onehot = (
        jnp.arange(2 * KC - 1, dtype=jnp.int32)[:, None, None] == offset[None, :, :]
    ).astype(jnp.float32)
    wide = jnp.einsum("hro,oqk->hqrk", table, onehot, precision=lax.Precision.HIGHEST)
    wide = jnp.where(inside[None, :, None, :], wide, -jnp.inf)
    return wide.reshape(heads, GRID_W, (2 * KR - 1) * GRID_W)


def scatter_tokens(tokens, place, sp_count, feats, piece):
    tok_here = tokens.shape[0]
    rows = tok_here // 2

    def body(place_ref, tokens_ref, *rest):
        out_refs, (buffer, sem) = rest[:-2], rest[-2:]
        slot = place_ref[1] * 2 + place_ref[2]
        copies = []
        for shift in range(sp_count):
            target = lax.rem(place_ref[0] + shift, sp_count)
            column = pl.multiple_of(target * feats + slot * piece, piece)
            copy = pltpu.make_async_copy(
                tokens_ref.at[:, pl.ds(column, piece)], buffer.at[shift], sem.at[shift]
            )
            copy.start()
            copies.append(copy)
        for shift in range(sp_count):
            copies[shift].wait()
            for part in range(2):
                out_refs[part * sp_count + shift][...] = buffer[shift, pl.ds(part * rows, rows), :]

    blocks = local_kernel(
        body,
        place,
        (),
        [shaped(rows, piece)] * (2 * sp_count),
        "scatter_tokens",
        scratch=[
            pltpu.VMEM((sp_count, tok_here, piece), jnp.bfloat16),
            pltpu.SemaphoreType.DMA((sp_count,)),
        ],
        hbm=(tokens,),
    )
    return blocks[:sp_count], blocks[sp_count:]


def stack_blocks(blocks, place):
    count = len(blocks)
    rows, width = blocks[0].shape

    def body(place_ref, *refs):
        out_ref = refs[-1]
        for shift in range(count):
            source = lax.rem(place_ref[0] + count - shift, count)
            out_ref[aligned(source, rows), :] = refs[shift][...]

    return local_kernel(body, place, blocks, [shaped(rows * count, width)], "stack_blocks")[0]


def over_sp(blocks, count):
    return [blocks[0]] + [
        lax.ppermute(blocks[shift], "sp", ring(count, shift)) for shift in range(1, count)
    ]


def project(pieces, slots, gain, weights, layer, place, chunk_shift, width, arrived, last):
    tok = pieces[0].shape[0]
    feats = weights[0].shape[1]
    sp_count = lax.axis_size("sp")
    count = len(pieces)

    def body(place_ref, *refs):
        piece_refs, refs = refs[:count], refs[count:]
        gain_ref, refs = refs[0], refs[1:]
        arrived_ref = None
        if arrived is not None:
            arrived_ref, refs = refs[0], refs[1:]
        weight_refs, (out_ref, held, sem) = refs[:3], refs[3:]
        chunk = lax.rem(place_ref[0] + chunk_shift, sp_count)
        copies = []
        for index, weight_ref in enumerate(weight_refs):
            copy = pltpu.make_async_copy(
                weight_ref.at[layer, :, aligned(chunk, width)],
                held.at[:, pl.ds(index * width, width)],
                sem.at[index],
            )
            copy.start()
            copies.append(copy)
        for copy in copies:
            copy.wait()
        total = jnp.zeros((tok, 3 * width), jnp.float32)
        if arrived is not None:
            total = arrived_ref[...].astype(jnp.float32)
        for piece_ref, slot in zip(piece_refs, slots):
            span = aligned(slot(place_ref[1], place_ref[2]), piece_ref.shape[1])
            scaled = piece_ref[...].astype(jnp.float32) * gain_ref[layer, :, span]
            total += jnp.dot(
                scaled.astype(jnp.bfloat16), held[span, :], preferred_element_type=jnp.float32
            )
        out_ref[...] = total.astype(out_ref.dtype)

    arrays = (*pieces, gain) + (() if arrived is None else (arrived,))
    return local_kernel(
        body,
        place,
        arrays,
        [shaped(tok, 3 * width, dtype=jnp.float32 if last else jnp.bfloat16)],
        "project",
        scratch=[
            pltpu.VMEM((feats, 3 * width), jnp.bfloat16),
            pltpu.SemaphoreType.DMA((3,)),
        ],
        hbm=weights,
        flops=2 * tok * feats * 3 * width,
    )[0]


def attend(arrived, own, norms, bias, place, sp_count):
    rows, total_width = arrived[0].shape
    heads = bias.shape[0]
    width = heads * HD
    part_rows = rows // sp_count
    grid_rows = 2 * rows // GRID_W
    part_grid = part_rows // GRID_W

    def body(place_ref, a0, a1, o0, o1, n0, n1, bias_ref, out0, out1, qkv_ref):
        for part, (a_ref, o_ref, n_ref) in enumerate(((a0, o0, n0), (a1, o1, n1))):
            for plane in range(sp_count):
                span = pl.ds(plane * part_rows, part_rows)
                total = a_ref[span, :].astype(jnp.float32) + o_ref[span, :]
                qkv_ref[pl.ds((2 * plane + part) * part_rows, part_rows), :] = (
                    total * n_ref[span, :]
                ).astype(jnp.bfloat16)
        for head in range(heads):
            lanes = head * HD
            for row in range(grid_rows):
                first = min(max(row - KR // 2, 0), grid_rows - KR)
                offset = first - row + KR - 1
                queries = qkv_ref[pl.ds(row * GRID_W, GRID_W), pl.ds(lanes, HD)]
                span = pl.ds(first * GRID_W, KR * GRID_W)
                keys = qkv_ref[span, pl.ds(width + lanes, HD)]
                values = qkv_ref[span, pl.ds(2 * width + lanes, HD)]
                scores = lax.dot_general(
                    queries, keys, (((1,), (1,)), ((), ())), preferred_element_type=jnp.float32
                )
                bias_here = bias_ref[head, :, pl.ds(offset * GRID_W, KR * GRID_W)]
                scores = scores * HD ** (-0.5) + bias_here
                powers = jnp.exp(scores - jnp.max(scores, axis=-1, keepdims=True))
                weights = powers / jnp.sum(powers, axis=-1, keepdims=True)
                mixed = jnp.dot(
                    weights.astype(jnp.bfloat16), values, preferred_element_type=jnp.float32
                )
                block, inner = divmod(row, part_grid)
                out_ref = (out0, out1)[block % 2]
                at = (block // 2) * part_rows + inner * GRID_W
                out_ref[pl.ds(at, GRID_W), pl.ds(lanes, HD)] = mixed.astype(jnp.bfloat16)

    return local_kernel(
        body,
        place,
        (*arrived, *own, *norms, bias),
        [shaped(rows, width)] * 2,
        "attend",
        scratch=[pltpu.VMEM((2 * rows, total_width), jnp.bfloat16)],
        flops=8 * heads * rows * KR * GRID_W * HD,
    )


def spread(attended, w_out, layer, place):
    count = len(attended)
    rows, width = attended[0].shape
    inner, feats = w_out.shape[1:]
    half = feats // 2

    def body(place_ref, *refs):
        piece_refs, (w_ref, sent_ref, kept_ref, gathered, held, sem) = refs[:count], refs[count:]
        copy = pltpu.make_async_copy(w_ref.at[layer], held, sem.at[0])
        copy.start()
        for shift in range(count):
            source = lax.rem(place_ref[0] + count - shift, count)
            gathered[:, aligned(source, width)] = piece_refs[shift][...]
        copy.wait()
        core = place_ref[1]
        for index, out_ref in ((1 - core, sent_ref), (core, kept_ref)):
            out_ref[...] = jnp.dot(
                gathered[...], held[:, aligned(index, half)], preferred_element_type=jnp.float32
            ).astype(jnp.bfloat16)

    return local_kernel(
        body,
        place,
        attended,
        [shaped(rows, half)] * 2,
        "spread",
        scratch=[
            pltpu.VMEM((rows, inner), jnp.bfloat16),
            pltpu.VMEM((inner, feats), jnp.bfloat16),
            pltpu.SemaphoreType.DMA((1,)),
        ],
        hbm=(w_out,),
        flops=2 * rows * inner * feats,
    )


def total_of(*refs):
    total = refs[0][...].astype(jnp.float32)
    for ref in refs[1:]:
        total += ref[...].astype(jnp.float32)
    return total


def pair_up(kept, came, place):
    def body(place_ref, kept_ref, came_ref, out_ref):
        out_ref[...] = total_of(kept_ref, came_ref).astype(jnp.bfloat16)

    return local_kernel(body, place, (kept, came), [shaped(*kept.shape)], "pair_up")[0]


def pair_apart(kept, came, place):
    rows, half = kept.shape
    piece = half // 2

    def body(place_ref, kept_ref, came_ref, sent_ref, stay_ref):
        far = place_ref[2]
        for index, out_ref in ((1 - far, sent_ref), (far, stay_ref)):
            span = aligned(index, piece)
            out_ref[...] = (
                kept_ref[:, span].astype(jnp.float32) + came_ref[:, span].astype(jnp.float32)
            ).astype(jnp.bfloat16)

    return local_kernel(body, place, (kept, came), [shaped(rows, piece)] * 2, "pair_apart")


def renew(residual, pair, came, place):
    count = len(residual)

    def body(place_ref, *refs):
        piece_refs, (pair_ref, came_ref, out_ref) = refs[:count], refs[count:]
        if count == 1:
            branch = total_of(pair_ref, came_ref)
            out_ref[...] = (piece_refs[0][...].astype(jnp.float32) + branch).astype(jnp.bfloat16)
            return
        far = place_ref[2]
        for index, ref in ((far, piece_refs[0]), (1 - far, piece_refs[1])):
            span = aligned(index, ref.shape[1])
            branch = pair_ref[:, span].astype(jnp.float32) + came_ref[:, span].astype(jnp.float32)
            out_ref[:, span] = (ref[...].astype(jnp.float32) + branch).astype(jnp.bfloat16)

    return local_kernel(body, place, (*residual, pair, came), [shaped(*pair.shape)], "renew")[0]


def finish(residual, stay, came, place, sp_count):
    rows, piece = stay.shape
    part = rows // sp_count

    def body(place_ref, x_ref, stay_ref, came_ref, *out_refs):
        for shift in range(sp_count):
            target = lax.rem(place_ref[0] + shift, sp_count)
            span = aligned(target, part)
            branch = stay_ref[span, :].astype(jnp.float32) + came_ref[span, :].astype(jnp.float32)
            x_here = x_ref[span, aligned(place_ref[2], piece)].astype(jnp.float32)
            out_refs[shift][...] = (x_here + branch).astype(jnp.bfloat16)

    return local_kernel(
        body, place, (residual, stay, came), [shaped(part, piece)] * sp_count, "finish"
    )


SLOTS = (
    lambda core, far: core * 2 + far,
    lambda core, far: core * 2 + 1 - far,
    lambda core, far: (1 - core) * 2 + far,
    lambda core, far: (1 - core) * 2 + 1 - far,
)


def assemble(parts, place, sp_count):
    rows, piece = parts[0][0].shape
    part = rows // sp_count
    count = len(parts[0])

    def body(place_ref, *refs):
        out_ref = refs[-1]
        for index in range(len(parts)):
            for which in range(count):
                slot = SLOTS[which](place_ref[1], place_ref[2])
                for plane in range(sp_count):
                    out_ref[pl.ds(index * part, part), aligned(plane * count + slot, piece)] = refs[
                        index * count + which
                    ][pl.ds(plane * part, part), :]

    flat = [array for pieces in parts for array in pieces]
    return local_kernel(
        body, place, flat, [shaped(part * len(parts), piece * count * sp_count)], "assemble"
    )[0]


def exchanged(held):
    far = swapped(held, "tp", 2)
    return [held, far, swapped(held, "tp", 1), swapped(far, "tp", 1)]


def stationary_plan(tokens, norm_gain, w_query, w_key, w_value, w_out, offset_bias):
    sp_count = lax.axis_size("sp")
    sp_index, tp_index = lax.axis_index("sp"), lax.axis_index("tp")
    place = jnp.stack([sp_index, tp_index % 2, tp_index // 2]).astype(jnp.int32)
    feats = w_query.shape[1]
    heads = offset_bias.shape[1] // sp_count
    width = heads * HD
    piece = feats // 4
    every_feat = feats * sp_count
    weights = (w_query, w_key, w_value)
    tables = lax.dynamic_slice_in_dim(offset_bias, sp_index * heads, heads, 1)
    gain = lax.dynamic_slice_in_dim(norm_gain, sp_index * feats, feats, 1)[:, None, :]

    halves = []
    for blocks in scatter_tokens(tokens, place, sp_count, feats, piece):
        halves.append(exchanged(stack_blocks(over_sp(blocks, sp_count), place)))
    slots = SLOTS
    shifts = (1, -1)

    for layer in range(LAYERS):
        squares = jnp.concatenate(
            [
                sum(jnp.sum(jnp.square(p.astype(jnp.float32)), axis=-1) for p in pieces)
                for pieces in halves
            ]
        )
        squares = summed_over(squares.reshape(-1, HD), "sp").reshape(2, -1, 1)
        norms = lax.rsqrt(squares / every_feat + norm_eps)
        bias = window_bias(tables[layer])

        arrived, own = [], []
        travelling = [None, None]
        for step in range(sp_count):
            for part in range(2):
                chunk_shift = (-shifts[part] * (step + 1)) % sp_count
                final = step == sp_count - 1
                made = project(
                    halves[part],
                    slots,
                    gain,
                    weights,
                    layer,
                    place,
                    chunk_shift,
                    width,
                    None if final else travelling[part],
                    final,
                )
                if final:
                    arrived.append(travelling[part])
                    own.append(made)
                else:
                    travelling[part] = lax.ppermute(made, "sp", ring(sp_count, shifts[part]))
        attended = attend(arrived, own, (norms[0], norms[1]), bias, place, sp_count)

        residuals = [pieces[:2] if layer == 0 else pieces[:1] for pieces in halves]
        halves = []
        for part in range(2):
            gathered = over_sp([attended[part]] * sp_count, sp_count)
            sent, kept = spread(gathered, w_out, layer, place)
            came = swapped(sent, "tp", 1)
            if layer < LAYERS - 1:
                pair = pair_up(kept, came, place)
                mine = renew(residuals[part], pair, swapped(pair, "tp", 2), place)
                halves.append([mine, swapped(mine, "tp", 1)])
            else:
                sent, stay = pair_apart(kept, came, place)
                blocks = finish(
                    residuals[part][0], stay, swapped(sent, "tp", 2), place, sp_count
                )
                halves.append(exchanged(stack_blocks(over_sp(blocks, sp_count), place)))
        slots = (lambda core, far: core, lambda core, far: 1 - core)
    return assemble(halves, place, sp_count)


def on_device(tokens, norm_gain, w_query, w_key, w_value, w_out, offset_bias):
    heads_here, sp_count = offset_bias.shape[1], lax.axis_size("sp")
    part_rows = tokens.shape[0] // 2
    plan = gathered_plan
    if heads_here % sp_count == 0 and lax.axis_size("tp") == 4 and part_rows % GRID_W == 0:
        plan = stationary_plan
    return plan(tokens, norm_gain, w_query, w_key, w_value, w_out, offset_bias)


def solution(mesh):
    return jax.shard_map(
        on_device,
        mesh=mesh,
        in_specs=(
            P(("grp", "sp"), None),
            P(),
            P(None, "sp", "tp"),
            P(None, "sp", "tp"),
            P(None, "sp", "tp"),
            P(None, "tp", "sp"),
            P(None, "tp", None, None),
        ),
        out_specs=P(("grp", "sp"), None),
        check_vma=False,
    )
```

```python
import functools

import jax
import jax.numpy as jnp
from jax import lax
from jax.experimental import pallas as pl
from jax.experimental.pallas import tpu as pltpu
from jax.sharding import PartitionSpec as P

HD = 128
GRID_W = 64
KR = 8
KC = 16
LAYERS = 2


norm_eps = 1e-06


def with_halo(block, sides, width):
    for axis, dim in sides:
        count = lax.axis_size(axis)
        forward = [(i, i + 1) for i in range(count - 1)]
        backward = [(target, source) for source, target in forward]
        low = lax.ppermute(
            lax.slice_in_dim(block, block.shape[dim] - width, None, axis=dim), axis, forward
        )
        high = lax.ppermute(lax.slice_in_dim(block, 0, width, axis=dim), axis, backward)
        block = jnp.concatenate([low, block, high], axis=dim)
    return block


def rms_rows(values, gain):
    wide = values.astype(jnp.float32)
    scaled = wide * lax.rsqrt(jnp.mean(wide * wide, axis=-1, keepdims=True) + norm_eps)
    return (scaled * gain.astype(jnp.float32)).astype(jnp.bfloat16)


def gathered_plan(tokens, norm_gain, w_query, w_key, w_value, w_out, offset_bias):
    sp_count = lax.axis_size("sp")
    sp_index = lax.axis_index("sp")
    tok_rows = tokens.shape[0]
    local_rows = tok_rows // GRID_W
    grid_rows = local_rows * sp_count
    heads_here = offset_bias.shape[1]
    head_width = heads_here * HD
    reach = KR // 2
    scale = HD ** (-0.5)
    columns = jnp.arange(GRID_W, dtype=jnp.int32)
    col_first = jnp.clip(columns - KC // 2, 0, GRID_W - KC)
    col_inside = (columns[None, :] >= col_first[:, None]) & (
        columns[None, :] < col_first[:, None] + KC
    )
    col_offset = jnp.clip(columns[None, :] - columns[:, None], 1 - KC, KC - 1) + KC - 1
    col_onehot = (
        jnp.arange(2 * KC - 1, dtype=jnp.int32)[:, None, None] == col_offset[None, :, :]
    ).astype(jnp.float32)
    first_row = sp_index * local_rows
    own_rows = first_row + jnp.arange(local_rows, dtype=jnp.int32)
    row_first = jnp.clip(own_rows - reach, 0, grid_rows - KR)
    band_start = row_first - first_row + reach
    row_offset = (
        row_first[:, None] + jnp.arange(KR, dtype=jnp.int32)[None, :] - own_rows[:, None] + KR - 1
    )
    row_onehot = (
        row_offset[:, :, None] == jnp.arange(2 * KR - 1, dtype=jnp.int32)[None, None, :]
    ).astype(jnp.float32)
    every_query, every_key, every_value, every_out = (
        lax.all_gather(w_query, "sp", axis=1, tiled=True),
        lax.all_gather(w_key, "sp", axis=1, tiled=True),
        lax.all_gather(w_value, "sp", axis=1, tiled=True),
        lax.all_gather(w_out, "sp", axis=2, tiled=True),
    )
    residual = tokens
    for layer_index in range(LAYERS):
        normed = rms_rows(residual, norm_gain[layer_index])
        queries = jnp.dot(normed, every_query[layer_index], preferred_element_type=jnp.float32)
        keys = jnp.dot(normed, every_key[layer_index], preferred_element_type=jnp.float32)
        values = jnp.dot(normed, every_value[layer_index], preferred_element_type=jnp.float32)
        out_weight = every_out[layer_index]
        queries = queries.astype(jnp.bfloat16).reshape(local_rows, GRID_W, heads_here, HD)
        key_values = jnp.concatenate(
            [keys.astype(jnp.bfloat16), values.astype(jnp.bfloat16)], axis=1
        )
        key_values = key_values.reshape(local_rows, GRID_W, 2 * head_width)
        padded = with_halo(key_values, (("sp", 0),), reach)
        bands = jax.vmap(lambda band_begin: lax.dynamic_slice_in_dim(padded, band_begin, KR, 0))(
            band_start
        )
        band_keys = bands[..., :head_width].reshape(local_rows, KR, GRID_W, heads_here, HD)
        band_values = bands[..., head_width:].reshape(local_rows, KR, GRID_W, heads_here, HD)
        col_bias = jnp.einsum(
            "hro,oqk->hrqk", offset_bias[layer_index], col_onehot, precision=lax.Precision.HIGHEST
        )
        full_bias = jnp.einsum(
            "ijr,hrqk->hiqjk", row_onehot, col_bias, precision=lax.Precision.HIGHEST
        )
        scores = jnp.einsum(
            "iqhd,ijkhd->hiqjk", queries, band_keys, preferred_element_type=jnp.float32
        )
        scores = scores * scale + full_bias
        scores = jnp.where(col_inside[None, None, :, None, :], scores, -jnp.inf)
        flattened = scores.reshape(heads_here, local_rows, GRID_W, KR * GRID_W)
        weights = jax.nn.softmax(flattened, axis=-1).astype(jnp.bfloat16)
        weights = weights.reshape(heads_here, local_rows, GRID_W, KR, GRID_W)
        attended = jnp.einsum(
            "hiqjk,ijkhd->iqhd", weights, band_values, preferred_element_type=jnp.float32
        )
        attended = attended.astype(jnp.bfloat16).reshape(tok_rows, head_width)
        branch = lax.psum(
            jnp.dot(attended, out_weight, preferred_element_type=jnp.float32).astype(jnp.bfloat16),
            "tp",
        ).astype(jnp.float32)
        residual = (residual.astype(jnp.float32) + branch).astype(jnp.bfloat16)
    return residual


VMEM_BYTES = 24 * 1024 * 1024


def ring(count, shift):
    return [(i, (i + shift) % count) for i in range(count)]


def swapped(array, axis, distance):
    count = lax.axis_size(axis)
    return lax.ppermute(array, axis, [(i, i ^ distance) for i in range(count)])


def summed_over(vector, axis):
    count = lax.axis_size(axis)
    distance = 1
    while distance < count:
        vector = vector + swapped(vector, axis, distance)
        distance *= 2
    return vector


def aligned(index, size):
    return pl.ds(pl.multiple_of(index * size, size), size)


def local_kernel(body, place, arrays, outs, name, scratch=(), hbm=(), flops=0, after=()):
    vmem, smem = pl.BlockSpec(memory_space=pltpu.VMEM), pl.BlockSpec(memory_space=pltpu.SMEM)
    moved = sum(a.size * a.dtype.itemsize for a in (*arrays, *outs))
    inputs = 1 + len(arrays) + len(hbm)

    def ordered(*refs):
        body(*refs[:inputs], *refs[inputs + len(after) :])

    return pl.pallas_call(
        ordered,
        out_shape=list(outs),
        in_specs=[smem]
        + [vmem] * len(arrays)
        + [pl.BlockSpec(memory_space=pltpu.HBM)] * len(hbm)
        + [pl.BlockSpec(memory_space=pl.ANY)] * len(after),
        out_specs=[vmem] * len(outs),
        scratch_shapes=list(scratch),
        compiler_params=pltpu.CompilerParams(vmem_limit_bytes=VMEM_BYTES),
        cost_estimate=pl.CostEstimate(flops=flops, bytes_accessed=moved, transcendentals=0),
        name=name,
    )(place, *arrays, *(pltpu.with_memory_space_constraint(a, pltpu.HBM) for a in hbm), *after)


def shaped(*shape, dtype=jnp.bfloat16):
    return jax.ShapeDtypeStruct(shape, dtype)


def window_bias(table):
    heads = table.shape[0]
    columns = jnp.arange(GRID_W, dtype=jnp.int32)
    first = jnp.clip(columns - KC // 2, 0, GRID_W - KC)
    inside = (columns[None, :] >= first[:, None]) & (columns[None, :] < first[:, None] + KC)
    offset = jnp.clip(columns[None, :] - columns[:, None], 1 - KC, KC - 1) + KC - 1
    onehot = (
        jnp.arange(2 * KC - 1, dtype=jnp.int32)[:, None, None] == offset[None, :, :]
    ).astype(jnp.float32)
    wide = jnp.einsum("hro,oqk->hqrk", table, onehot, precision=lax.Precision.HIGHEST)
    wide = jnp.where(inside[None, :, None, :], wide, -jnp.inf)
    return wide.reshape(heads, GRID_W, (2 * KR - 1) * GRID_W)


def scatter_tokens(tokens, place, sp_count, feats, piece):
    tok_here = tokens.shape[0]

    def body(place_ref, tokens_ref, *rest):
        out_refs, sem = rest[:-1], rest[-1]
        slot = place_ref[1] * 2 + place_ref[2]
        copies = []
        for shift in range(sp_count):
            target = lax.rem(place_ref[0] + shift, sp_count)
            column = pl.multiple_of(target * feats + slot * piece, piece)
            copy = pltpu.make_async_copy(
                tokens_ref.at[:, pl.ds(column, piece)], out_refs[shift], sem.at[shift]
            )
            copy.start()
            copies.append(copy)
        for copy in copies:
            copy.wait()

    return local_kernel(
        body,
        place,
        (),
        [shaped(tok_here, piece)] * sp_count,
        "scatter_tokens",
        scratch=[pltpu.SemaphoreType.DMA((sp_count,))],
        hbm=(tokens,),
    )


def stack_blocks(blocks, place, parts=1):
    count = len(blocks)
    rows, width = blocks[0].shape
    rows = rows // parts

    def body(place_ref, *refs):
        for part in range(parts):
            for shift in range(count):
                source = lax.rem(place_ref[0] + count - shift, count)
                refs[count + part][aligned(source, rows), :] = refs[shift][
                    pl.ds(part * rows, rows), :
                ]

    return local_kernel(
        body, place, blocks, [shaped(rows * count, width)] * parts, "stack_blocks"
    )


def over_sp(blocks, count):
    return [blocks[0]] + [
        lax.ppermute(blocks[shift], "sp", ring(count, shift)) for shift in range(1, count)
    ]


def project(pieces, slots, gain, weights, layer, place, chunk_shift, width, arrived, last):
    tok = pieces[0].shape[0]
    feats = weights[0].shape[1]
    sp_count = lax.axis_size("sp")
    count = len(pieces)

    def body(place_ref, *refs):
        piece_refs, refs = refs[:count], refs[count:]
        gain_ref, refs = refs[0], refs[1:]
        arrived_ref = None
        if arrived is not None:
            arrived_ref, refs = refs[0], refs[1:]
        weight_refs, (out_ref, held, sem) = refs[:3], refs[3:]
        chunk = lax.rem(place_ref[0] + chunk_shift, sp_count)
        copies = []
        for index, weight_ref in enumerate(weight_refs):
            copy = pltpu.make_async_copy(
                weight_ref.at[layer, :, aligned(chunk, width)],
                held.at[:, pl.ds(index * width, width)],
                sem.at[index],
            )
            copy.start()
            copies.append(copy)
        for copy in copies:
            copy.wait()
        total = jnp.zeros((tok, 3 * width), jnp.float32)
        if arrived is not None:
            total = arrived_ref[...].astype(jnp.float32)
        for piece_ref, slot in zip(piece_refs, slots):
            span = aligned(slot(place_ref[1], place_ref[2]), piece_ref.shape[1])
            scaled = piece_ref[...].astype(jnp.float32) * gain_ref[layer, :, span]
            total += jnp.dot(
                scaled.astype(jnp.bfloat16), held[span, :], preferred_element_type=jnp.float32
            )
        out_ref[...] = total.astype(out_ref.dtype)

    arrays = (*pieces, gain) + (() if arrived is None else (arrived,))
    return local_kernel(
        body,
        place,
        arrays,
        [shaped(tok, 3 * width, dtype=jnp.float32 if last else jnp.bfloat16)],
        "project",
        scratch=[
            pltpu.VMEM((feats, 3 * width), jnp.bfloat16),
            pltpu.SemaphoreType.DMA((3,)),
        ],
        hbm=weights,
        flops=2 * tok * feats * 3 * width,
    )[0]


def attend_rows(qkv_ref, bias_ref, out_ref, part, sp_count, heads):
    grid_rows = qkv_ref.shape[0] // GRID_W
    width = heads * HD
    part_grid = grid_rows // sp_count // 2
    for head in range(heads):
        lanes = head * HD
        for index in range(sp_count * part_grid):
            plane, inner = divmod(index, part_grid)
            row = (2 * plane + part) * part_grid + inner
            first = min(max(row - KR // 2, 0), grid_rows - KR)
            offset = first - row + KR - 1
            queries = qkv_ref[pl.ds(row * GRID_W, GRID_W), pl.ds(lanes, HD)]
            span = pl.ds(first * GRID_W, KR * GRID_W)
            keys = qkv_ref[span, pl.ds(width + lanes, HD)]
            values = qkv_ref[span, pl.ds(2 * width + lanes, HD)]
            scores = lax.dot_general(
                queries, keys, (((1,), (1,)), ((), ())), preferred_element_type=jnp.float32
            )
            bias_here = bias_ref[head, :, pl.ds(offset * GRID_W, KR * GRID_W)]
            scores = scores * HD ** (-0.5) + bias_here
            powers = jnp.exp(scores - jnp.max(scores, axis=-1, keepdims=True))
            weights = powers * (1.0 / jnp.sum(powers, axis=-1, keepdims=True))
            mixed = jnp.dot(
                weights.astype(jnp.bfloat16), values, preferred_element_type=jnp.float32
            )
            out_ref[pl.ds(index * GRID_W, GRID_W), pl.ds(lanes, HD)] = mixed.astype(jnp.bfloat16)


def attend(arrived, own, norms, bias, place, sp_count):
    rows, total_width = arrived[0].shape
    heads = bias.shape[0]
    width = heads * HD
    part_rows = rows // sp_count
    flops = 4 * heads * rows * KR * GRID_W * HD

    def low(place_ref, a0, a1, o0, o1, n0, n1, bias_ref, out_ref, qkv_ref):
        for part, (a_ref, o_ref, n_ref) in enumerate(((a0, o0, n0), (a1, o1, n1))):
            for plane in range(sp_count):
                span = pl.ds(plane * part_rows, part_rows)
                total = a_ref[span, :].astype(jnp.float32) + o_ref[span, :]
                qkv_ref[pl.ds((2 * plane + part) * part_rows, part_rows), :] = (
                    total * n_ref[span, :]
                ).astype(jnp.bfloat16)
        attend_rows(qkv_ref, bias_ref, out_ref, 0, sp_count, heads)

    def high(place_ref, qkv_ref, bias_ref, out_ref):
        attend_rows(qkv_ref, bias_ref, out_ref, 1, sp_count, heads)

    out0, qkv = local_kernel(
        low,
        place,
        (*arrived, *own, *norms, bias),
        [shaped(rows, width), shaped(2 * rows, total_width)],
        "attend_low",
        flops=flops,
    )
    out1 = local_kernel(high, place, (qkv, bias), [shaped(rows, width)], "attend_high", flops=flops)
    return out0, out1[0]


def spread(attended, w_out, layer, place, after):
    count = len(attended)
    rows, width = attended[0].shape
    inner, feats = w_out.shape[1:]
    half = feats // 2

    def body(place_ref, *refs):
        piece_refs, (w_ref, sent_ref, kept_ref, gathered, held, sem) = refs[:count], refs[count:]
        copy = pltpu.make_async_copy(w_ref.at[layer], held, sem.at[0])
        copy.start()
        for shift in range(count):
            source = lax.rem(place_ref[0] + count - shift, count)
            gathered[:, aligned(source, width)] = piece_refs[shift][...]
        copy.wait()
        core = place_ref[1]
        for index, out_ref in ((1 - core, sent_ref), (core, kept_ref)):
            out_ref[...] = jnp.dot(
                gathered[...], held[:, aligned(index, half)], preferred_element_type=jnp.float32
            ).astype(jnp.bfloat16)

    return local_kernel(
        body,
        place,
        attended,
        [shaped(rows, half)] * 2,
        "spread",
        scratch=[
            pltpu.VMEM((rows, inner), jnp.bfloat16),
            pltpu.VMEM((inner, feats), jnp.bfloat16),
            pltpu.SemaphoreType.DMA((1,)),
        ],
        hbm=(w_out,),
        flops=2 * rows * inner * feats,
        after=after,
    )


def total_of(*refs):
    total = refs[0][...].astype(jnp.float32)
    for ref in refs[1:]:
        total += ref[...].astype(jnp.float32)
    return total


def pair_up(kept, came, place):
    def body(place_ref, kept_ref, came_ref, out_ref):
        out_ref[...] = total_of(kept_ref, came_ref).astype(jnp.bfloat16)

    return local_kernel(body, place, (kept, came), [shaped(*kept.shape)], "pair_up")


def pair_apart(kept, came, place):
    rows, half = kept.shape
    piece = half // 2

    def body(place_ref, kept_ref, came_ref, sent_ref, stay_ref):
        far = place_ref[2]
        for index, out_ref in ((1 - far, sent_ref), (far, stay_ref)):
            span = aligned(index, piece)
            out_ref[...] = (
                kept_ref[:, span].astype(jnp.float32) + came_ref[:, span].astype(jnp.float32)
            ).astype(jnp.bfloat16)

    return local_kernel(body, place, (kept, came), [shaped(rows, piece)] * 2, "pair_apart")


def renew(residual, pair, came, place, after):
    count = len(residual)

    def body(place_ref, *refs):
        piece_refs, (pair_ref, came_ref, out_ref) = refs[:count], refs[count:]
        if count == 1:
            branch = total_of(pair_ref, came_ref)
            out_ref[...] = (piece_refs[0][...].astype(jnp.float32) + branch).astype(jnp.bfloat16)
            return
        far = place_ref[2]
        for index, ref in ((far, piece_refs[0]), (1 - far, piece_refs[1])):
            span = aligned(index, ref.shape[1])
            branch = pair_ref[:, span].astype(jnp.float32) + came_ref[:, span].astype(jnp.float32)
            out_ref[:, span] = (ref[...].astype(jnp.float32) + branch).astype(jnp.bfloat16)

    return local_kernel(
        body, place, (*residual, pair, came), [shaped(*pair.shape)], "renew", after=after
    )[0]


def finish(residual, stay, came, place, sp_count):
    rows, piece = stay.shape
    part = rows // sp_count

    def body(place_ref, x_ref, stay_ref, came_ref, *out_refs):
        for shift in range(sp_count):
            target = lax.rem(place_ref[0] + shift, sp_count)
            span = aligned(target, part)
            branch = stay_ref[span, :].astype(jnp.float32) + came_ref[span, :].astype(jnp.float32)
            x_here = x_ref[span, aligned(place_ref[2], piece)].astype(jnp.float32)
            out_refs[shift][...] = (x_here + branch).astype(jnp.bfloat16)

    return local_kernel(
        body, place, (residual, stay, came), [shaped(part, piece)] * sp_count, "finish"
    )


SLOTS = (
    lambda core, far: core * 2 + far,
    lambda core, far: core * 2 + 1 - far,
    lambda core, far: (1 - core) * 2 + far,
    lambda core, far: (1 - core) * 2 + 1 - far,
)


HALF_SLOTS = (lambda core, far: core, lambda core, far: 1 - core)


def assemble(parts, place, sp_count):
    rows, piece = parts[0][0].shape
    part = rows // sp_count
    count = len(parts[0])

    def body(place_ref, *refs):
        out_ref = refs[-1]
        for index in range(len(parts)):
            for which in range(count):
                slot = SLOTS[which](place_ref[1], place_ref[2])
                for plane in range(sp_count):
                    out_ref[pl.ds(index * part, part), aligned(plane * count + slot, piece)] = refs[
                        index * count + which
                    ][pl.ds(plane * part, part), :]

    flat = [array for pieces in parts for array in pieces]
    return local_kernel(
        body, place, flat, [shaped(part * len(parts), piece * count * sp_count)], "assemble"
    )[0]


def exchanged(held):
    far = swapped(held, "tp", 2)
    return [held, far, swapped(held, "tp", 1), swapped(far, "tp", 1)]


def stationary_plan(tokens, norm_gain, w_query, w_key, w_value, w_out, offset_bias):
    sp_count = lax.axis_size("sp")
    sp_index, tp_index = lax.axis_index("sp"), lax.axis_index("tp")
    place = jnp.stack([sp_index, tp_index % 2, tp_index // 2]).astype(jnp.int32)
    feats = w_query.shape[1]
    heads = offset_bias.shape[1] // sp_count
    width = heads * HD
    piece = feats // 4
    every_feat = feats * sp_count
    weights = (w_query, w_key, w_value)
    tables = lax.dynamic_slice_in_dim(offset_bias, sp_index * heads, heads, 1)
    biases = window_bias(tables.reshape(LAYERS * heads, *tables.shape[2:]))
    gain = lax.dynamic_slice_in_dim(norm_gain, sp_index * feats, feats, 1)[:, None, :]
    shifts = (1, -1)
    halves = [None, None]
    travelling = [None, None]

    def shared(part, step, layer, arrived=None):
        slots = SLOTS if layer == 0 else HALF_SLOTS
        final = step == sp_count - 1
        chunk = (-shifts[part] * (step + 1)) % sp_count
        return project(
            halves[part], slots, gain, weights, layer, place, chunk, width, arrived, final
        )

    def sent_on(made, part):
        return lax.ppermute(made, "sp", ring(sp_count, shifts[part]))

    blocks = over_sp(scatter_tokens(tokens, place, sp_count, feats, piece), sp_count)
    held = stack_blocks(blocks, place, 2)
    far = [swapped(h, "tp", 2) for h in held]
    near = [swapped(h, "tp", 1) for h in held]
    halves[0] = [held[0], far[0], near[0], swapped(far[0], "tp", 1)]
    made = [shared(0, 0, 0), None]
    far[1] = lax.optimization_barrier((far[1], made[0]))[0]
    halves[1] = [held[1], far[1], near[1], swapped(far[1], "tp", 1)]
    made[1] = shared(1, 0, 0)

    for layer in range(LAYERS):
        summed = lax.optimization_barrier((halves, made))[0]
        travelling = [sent_on(made[part], part) for part in range(2)]
        squares = jnp.concatenate(
            [
                sum(jnp.sum(jnp.square(p.astype(jnp.float32)), axis=-1) for p in pieces)
                for pieces in summed
            ]
        )
        squares = summed_over(squares.reshape(-1, HD), "sp").reshape(2, -1, 1)
        norms = lax.rsqrt(squares / every_feat + norm_eps)
        for step in range(1, sp_count - 1):
            for part in range(2):
                travelling[part] = sent_on(shared(part, step, layer, travelling[part]), part)
        own = [shared(part, sp_count - 1, layer) for part in range(2)]
        bias = biases[layer * heads : (layer + 1) * heads]
        attended = attend(travelling, own, (norms[0], norms[1]), bias, place, sp_count)

        residuals = [pieces[:2] if layer == 0 else pieces[:1] for pieces in halves]
        pairs, after = [], (attended[1],)
        for part in range(2):
            gathered = over_sp([attended[part]] * sp_count, sp_count)
            sent, kept = spread(gathered, w_out, layer, place, after)
            came = swapped(sent, "tp", 1)
            pair = (pair_up if layer < LAYERS - 1 else pair_apart)(kept, came, place)
            pairs.append(pair)
            after = (pair[0],)
        after = ()
        for part in range(2):
            if layer < LAYERS - 1:
                pair = pairs[part][0]
                mine = renew(residuals[part], pair, swapped(pair, "tp", 2), place, after)
                halves[part] = [mine, swapped(mine, "tp", 1)]
                made[part] = shared(part, 0, layer + 1)
                after = (made[part],)
            else:
                sent, stay = pairs[part]
                blocks = finish(
                    residuals[part][0], stay, swapped(sent, "tp", 2), place, sp_count
                )
                stacked = stack_blocks(over_sp(blocks, sp_count), place)[0]
                halves[part] = exchanged(stacked)
    return assemble(halves, place, sp_count)


def on_device(tokens, norm_gain, w_query, w_key, w_value, w_out, offset_bias):
    heads_here, sp_count = offset_bias.shape[1], lax.axis_size("sp")
    part_rows = tokens.shape[0] // 2
    plan = gathered_plan
    if heads_here % sp_count == 0 and lax.axis_size("tp") == 4 and part_rows % GRID_W == 0:
        plan = stationary_plan
    return plan(tokens, norm_gain, w_query, w_key, w_value, w_out, offset_bias)


def solution(mesh):
    return jax.shard_map(
        on_device,
        mesh=mesh,
        in_specs=(
            P(("grp", "sp"), None),
            P(),
            P(None, "sp", "tp"),
            P(None, "sp", "tp"),
            P(None, "sp", "tp"),
            P(None, "tp", "sp"),
            P(None, "tp", None, None),
        ),
        out_specs=P(("grp", "sp"), None),
        check_vma=False,
    )
```

```python
import jax
import jax.numpy as jnp
from jax import lax
from jax.experimental import pallas as pl
from jax.experimental.pallas import tpu as pltpu
from jax.sharding import PartitionSpec as P


HD = 128
GRID_W = 64
KR = 8
KC = 16
LAYERS = 2


norm_eps = 1e-06


def with_halo(block, sides, width):
    for axis, dim in sides:
        count = lax.axis_size(axis)
        forward = [(i, i + 1) for i in range(count - 1)]
        backward = [(target, source) for source, target in forward]
        low = lax.ppermute(
            lax.slice_in_dim(block, block.shape[dim] - width, None, axis=dim), axis, forward
        )
        high = lax.ppermute(lax.slice_in_dim(block, 0, width, axis=dim), axis, backward)
        block = jnp.concatenate([low, block, high], axis=dim)
    return block


def rms_rows(values, gain):
    wide = values.astype(jnp.float32)
    scaled = wide * lax.rsqrt(jnp.mean(wide * wide, axis=-1, keepdims=True) + norm_eps)
    return (scaled * gain.astype(jnp.float32)).astype(jnp.bfloat16)


def gathered_plan(tokens, norm_gain, w_query, w_key, w_value, w_out, offset_bias):
    sp_count = lax.axis_size("sp")
    sp_index = lax.axis_index("sp")
    tok_rows = tokens.shape[0]
    local_rows = tok_rows // GRID_W
    grid_rows = local_rows * sp_count
    heads_here = offset_bias.shape[1]
    head_width = heads_here * HD
    reach = KR // 2
    scale = HD ** (-0.5)
    columns = jnp.arange(GRID_W, dtype=jnp.int32)
    col_first = jnp.clip(columns - KC // 2, 0, GRID_W - KC)
    col_inside = (columns[None, :] >= col_first[:, None]) & (
        columns[None, :] < col_first[:, None] + KC
    )
    col_offset = jnp.clip(columns[None, :] - columns[:, None], 1 - KC, KC - 1) + KC - 1
    col_onehot = (
        jnp.arange(2 * KC - 1, dtype=jnp.int32)[:, None, None] == col_offset[None, :, :]
    ).astype(jnp.float32)
    first_row = sp_index * local_rows
    own_rows = first_row + jnp.arange(local_rows, dtype=jnp.int32)
    row_first = jnp.clip(own_rows - reach, 0, grid_rows - KR)
    band_start = row_first - first_row + reach
    row_offset = (
        row_first[:, None] + jnp.arange(KR, dtype=jnp.int32)[None, :] - own_rows[:, None] + KR - 1
    )
    row_onehot = (
        row_offset[:, :, None] == jnp.arange(2 * KR - 1, dtype=jnp.int32)[None, None, :]
    ).astype(jnp.float32)
    every_query, every_key, every_value, every_out = (
        lax.all_gather(w_query, "sp", axis=1, tiled=True),
        lax.all_gather(w_key, "sp", axis=1, tiled=True),
        lax.all_gather(w_value, "sp", axis=1, tiled=True),
        lax.all_gather(w_out, "sp", axis=2, tiled=True),
    )
    residual = tokens
    for layer_index in range(LAYERS):
        normed = rms_rows(residual, norm_gain[layer_index])
        queries = jnp.dot(normed, every_query[layer_index], preferred_element_type=jnp.float32)
        keys = jnp.dot(normed, every_key[layer_index], preferred_element_type=jnp.float32)
        values = jnp.dot(normed, every_value[layer_index], preferred_element_type=jnp.float32)
        out_weight = every_out[layer_index]
        queries = queries.astype(jnp.bfloat16).reshape(local_rows, GRID_W, heads_here, HD)
        key_values = jnp.concatenate(
            [keys.astype(jnp.bfloat16), values.astype(jnp.bfloat16)], axis=1
        )
        key_values = key_values.reshape(local_rows, GRID_W, 2 * head_width)
        padded = with_halo(key_values, (("sp", 0),), reach)
        bands = jax.vmap(lambda band_begin: lax.dynamic_slice_in_dim(padded, band_begin, KR, 0))(
            band_start
        )
        band_keys = bands[..., :head_width].reshape(local_rows, KR, GRID_W, heads_here, HD)
        band_values = bands[..., head_width:].reshape(local_rows, KR, GRID_W, heads_here, HD)
        col_bias = jnp.einsum(
            "hro,oqk->hrqk", offset_bias[layer_index], col_onehot, precision=lax.Precision.HIGHEST
        )
        full_bias = jnp.einsum(
            "ijr,hrqk->hiqjk", row_onehot, col_bias, precision=lax.Precision.HIGHEST
        )
        scores = jnp.einsum(
            "iqhd,ijkhd->hiqjk", queries, band_keys, preferred_element_type=jnp.float32
        )
        scores = scores * scale + full_bias
        scores = jnp.where(col_inside[None, None, :, None, :], scores, -jnp.inf)
        flattened = scores.reshape(heads_here, local_rows, GRID_W, KR * GRID_W)
        weights = jax.nn.softmax(flattened, axis=-1).astype(jnp.bfloat16)
        weights = weights.reshape(heads_here, local_rows, GRID_W, KR, GRID_W)
        attended = jnp.einsum(
            "hiqjk,ijkhd->iqhd", weights, band_values, preferred_element_type=jnp.float32
        )
        attended = attended.astype(jnp.bfloat16).reshape(tok_rows, head_width)
        branch = lax.psum(
            jnp.dot(attended, out_weight, preferred_element_type=jnp.float32).astype(jnp.bfloat16),
            "tp",
        ).astype(jnp.float32)
        residual = (residual.astype(jnp.float32) + branch).astype(jnp.bfloat16)
    return residual


VMEM_BYTES = 24 * 1024 * 1024


def ring(count, shift):
    return [(i, (i + shift) % count) for i in range(count)]


def swapped(array, axis, distance):
    count = lax.axis_size(axis)
    return lax.ppermute(array, axis, [(i, i ^ distance) for i in range(count)])


def aligned(index, size):
    return pl.ds(pl.multiple_of(index * size, size), size)


def local_kernel(body, place, arrays, outs, scratch=(), hbm=(), flops=0, after=()):
    vmem, smem = pl.BlockSpec(memory_space=pltpu.VMEM), pl.BlockSpec(memory_space=pltpu.SMEM)
    moved = sum(a.size * a.dtype.itemsize for a in (*arrays, *outs))
    inputs = 1 + len(arrays) + len(hbm)

    def ordered(*refs):
        body(*refs[:inputs], *refs[inputs + len(after) :])

    return pl.pallas_call(
        ordered,
        out_shape=list(outs),
        in_specs=[smem]
        + [vmem] * len(arrays)
        + [pl.BlockSpec(memory_space=pltpu.HBM)] * len(hbm)
        + [pl.BlockSpec(memory_space=pl.ANY)] * len(after),
        out_specs=[vmem] * len(outs),
        scratch_shapes=list(scratch),
        compiler_params=pltpu.CompilerParams(vmem_limit_bytes=VMEM_BYTES),
        cost_estimate=pl.CostEstimate(flops=flops, bytes_accessed=moved, transcendentals=0),
    )(place, *arrays, *(pltpu.with_memory_space_constraint(a, pltpu.HBM) for a in hbm), *after)


def shaped(*shape, dtype=jnp.bfloat16):
    return jax.ShapeDtypeStruct(shape, dtype)


def window_bias(offset_bias, place, heads):
    layers, _, offsets, reach = offset_bias.shape
    pairs = -(-offsets // 2)
    lanes = 2 * GRID_W

    def body(place_ref, table_ref, out_ref, padded):
        padded[...] = jnp.zeros_like(padded)
        lane = lax.broadcasted_iota(jnp.int32, (GRID_W, lanes), 1)
        query = lax.broadcasted_iota(jnp.int32, (GRID_W, lanes), 0)
        column = jnp.where(lane < GRID_W, lane, lane - GRID_W)
        first = jnp.clip(query - KC // 2, 0, GRID_W - KC)
        inside = (column >= first) & (column < first + KC)
        for layer in range(layers):
            for head in range(heads):
                padded[pl.ds(0, offsets), pl.ds(0, reach)] = table_ref[
                    layer, place_ref[0] * heads + head
                ]
                for pair in range(pairs):
                    sides = []
                    for side in range(2):
                        row = jnp.broadcast_to(
                            padded[pl.ds(2 * pair + side, 1), :], (GRID_W, lanes)
                        )
                        start = (side * GRID_W - (KC - 1)) % lanes
                        sides.append(pltpu.roll(row, start, 1, stride=1, stride_axis=0))
                    both = jnp.where(lane < GRID_W, sides[0], sides[1])
                    out_ref[layer * heads + head, :, pl.ds(pair * lanes, lanes)] = jnp.where(
                        inside, both, -jnp.inf
                    )

    return local_kernel(
        body,
        place,
        (offset_bias,),
        [shaped(layers * heads, GRID_W, pairs * lanes, dtype=jnp.float32)],
        scratch=[pltpu.VMEM((2 * pairs, lanes), jnp.float32)],
    )[0]


def squares_of(halves, place):
    flat = [piece for pieces in halves for piece in pieces]
    count = len(halves[0])
    runs = halves[0][0].shape[0] // HD

    def body(place_ref, *refs):
        out_ref = refs[-1]
        for index in range(len(halves)):
            for run in range(runs):
                total = jnp.zeros((HD, HD), jnp.float32)
                for ref in refs[index * count : (index + 1) * count]:
                    for lane in range(ref.shape[1] // HD):
                        part = ref[pl.ds(run * HD, HD), pl.ds(lane * HD, HD)].astype(jnp.float32)
                        total += part * part
                out_ref[pl.ds(index * runs + run, 1), :] = jnp.sum(total.T, axis=0, keepdims=True)

    return local_kernel(body, place, flat, [shaped(len(halves) * runs, HD, dtype=jnp.float32)])[0]


def scatter_tokens(tokens, place, sp_count, feats, piece):
    tok_here = tokens.shape[0]

    def body(place_ref, tokens_ref, *rest):
        out_refs, sem = rest[:-1], rest[-1]
        slot = place_ref[1] * 2 + place_ref[2]
        copies = []
        for shift in range(sp_count):
            target = lax.rem(place_ref[0] + shift, sp_count)
            column = pl.multiple_of(target * feats + slot * piece, piece)
            copy = pltpu.make_async_copy(
                tokens_ref.at[:, pl.ds(column, piece)], out_refs[shift], sem.at[shift]
            )
            copy.start()
            copies.append(copy)
        for copy in copies:
            copy.wait()

    return local_kernel(
        body,
        place,
        (),
        [shaped(tok_here, piece)] * sp_count,
        scratch=[pltpu.SemaphoreType.DMA((sp_count,))],
        hbm=(tokens,),
    )


def stack_blocks(blocks, place, parts=1, after=()):
    count = len(blocks)
    rows, width = blocks[0].shape
    rows = rows // parts

    def body(place_ref, *refs):
        for part in range(parts):
            for shift in range(count):
                source = lax.rem(place_ref[0] + count - shift, count)
                refs[count + part][aligned(source, rows), :] = refs[shift][
                    pl.ds(part * rows, rows), :
                ]

    return local_kernel(body, place, blocks, [shaped(rows * count, width)] * parts, after=after)


def over_sp(blocks, count):
    return [blocks[0]] + [
        lax.ppermute(blocks[shift], "sp", ring(count, shift)) for shift in range(1, count)
    ]


def scaled_by(slots, layer, feats, place_ref, piece_refs, gain_ref, out_ref):
    for piece_ref, slot in zip(piece_refs, slots):
        span = aligned(slot(place_ref[1], place_ref[2]), piece_ref.shape[1])
        start = pl.multiple_of(
            place_ref[0] * feats + slot(place_ref[1], place_ref[2]) * piece_ref.shape[1],
            piece_ref.shape[1],
        )
        factor = gain_ref[pl.ds(layer, 1), pl.ds(start, piece_ref.shape[1])].astype(jnp.float32)
        out_ref[:, span] = (piece_ref[...].astype(jnp.float32) * factor).astype(jnp.bfloat16)


def project(source, weights, layer, place, chunk_shift, width, arrived=None, last=False):
    fresh = isinstance(source, tuple)
    feats = weights[0].shape[1]
    sp_count = lax.axis_size("sp")
    arrays = (*source[0], source[2]) if fresh else (source,)
    tok = arrays[0].shape[0]
    if arrived is not None:
        arrays += (arrived,)
    count = len(arrays)

    def body(place_ref, *refs):
        array_refs, weight_refs, refs = refs[:count], refs[count : count + 3], refs[count + 3 :]
        out_ref, held, sem = refs[0], refs[-2], refs[-1]
        chunk = lax.rem(place_ref[0] + chunk_shift, sp_count)
        copies = []
        for index, weight_ref in enumerate(weight_refs):
            copy = pltpu.make_async_copy(
                weight_ref.at[layer, :, aligned(chunk, width)],
                held.at[:, pl.ds(index * width, width)],
                sem.at[index],
            )
            copy.start()
            copies.append(copy)
        scaled_ref = array_refs[0]
        if fresh:
            scaled_ref = refs[1]
            pieces, slots, _ = source
            scaled_by(
                slots, layer, feats, place_ref,
                array_refs[: len(pieces)], array_refs[len(pieces)], scaled_ref,
            )
        for copy in copies:
            copy.wait()
        total = jnp.dot(scaled_ref[...], held[...], preferred_element_type=jnp.float32)
        if arrived is not None:
            total += array_refs[-1][...].astype(jnp.float32)
        out_ref[...] = total.astype(out_ref.dtype)

    outs = [shaped(tok, 3 * width, dtype=jnp.float32 if last else jnp.bfloat16)]
    return local_kernel(
        body,
        place,
        arrays,
        outs + [shaped(tok, feats)] * fresh,
        scratch=[
            pltpu.VMEM((feats, 3 * width), jnp.bfloat16),
            pltpu.SemaphoreType.DMA((3,)),
        ],
        hbm=weights,
        flops=2 * tok * feats * 3 * width,
    )


def attend_rows(qkv_ref, bias_ref, out_ref, part, sp_count, heads, layer):
    grid_rows = qkv_ref.shape[0] // GRID_W
    width = heads * HD
    part_grid = grid_rows // sp_count // 2
    for head in range(heads):
        lanes = head * HD
        for index in range(sp_count * part_grid):
            plane, inner = divmod(index, part_grid)
            row = (2 * plane + part) * part_grid + inner
            first = min(max(row - KR // 2, 0), grid_rows - KR)
            offset = first - row + KR - 1
            queries = qkv_ref[pl.ds(row * GRID_W, GRID_W), pl.ds(lanes, HD)]
            span = pl.ds(first * GRID_W, KR * GRID_W)
            keys = qkv_ref[span, pl.ds(width + lanes, HD)]
            values = qkv_ref[span, pl.ds(2 * width + lanes, HD)]
            scores = lax.dot_general(
                queries, keys, (((1,), (1,)), ((), ())), preferred_element_type=jnp.float32
            )
            bias_here = bias_ref[layer * heads + head, :, pl.ds(offset * GRID_W, KR * GRID_W)]
            scores = scores * HD ** (-0.5) + bias_here
            powers = jnp.exp(scores - jnp.max(scores, axis=-1, keepdims=True))
            weights = powers * (1.0 / jnp.sum(powers, axis=-1, keepdims=True))
            mixed = jnp.dot(
                weights.astype(jnp.bfloat16), values, preferred_element_type=jnp.float32
            )
            out_ref[pl.ds(index * GRID_W, GRID_W), pl.ds(lanes, HD)] = mixed.astype(jnp.bfloat16)


def attend(arrived, own, squares, bias, place, sp_count, heads, layer, every_feat):
    rows, total_width = arrived[0].shape
    width = heads * HD
    part_rows = rows // sp_count
    runs = rows // HD
    flops = 4 * heads * rows * KR * GRID_W * HD

    def low(place_ref, a0, a1, o0, o1, *refs):
        square_refs, (bias_ref, out_ref, qkv_ref) = refs[:-3], refs[-3:]
        norm = lax.rsqrt(total_of(*square_refs) / every_feat + norm_eps)
        for part, (a_ref, o_ref) in enumerate(((a0, o0), (a1, o1))):
            for run in range(runs):
                row = part * runs + run
                factor = jnp.broadcast_to(norm[row : row + 1, :], (HD, HD)).T
                plane, inner = divmod(run * HD, part_rows)
                to = pl.ds((2 * plane + part) * part_rows + inner, HD)
                span = pl.ds(run * HD, HD)
                for lane in range(total_width // HD):
                    lanes = pl.ds(lane * HD, HD)
                    total = a_ref[span, lanes].astype(jnp.float32) + o_ref[span, lanes]
                    qkv_ref[to, lanes] = (total * factor).astype(jnp.bfloat16)
        attend_rows(qkv_ref, bias_ref, out_ref, 0, sp_count, heads, layer)

    def high(place_ref, qkv_ref, bias_ref, out_ref):
        attend_rows(qkv_ref, bias_ref, out_ref, 1, sp_count, heads, layer)

    out0, qkv = local_kernel(
        low,
        place,
        (*arrived, *own, *squares, bias),
        [shaped(rows, width), shaped(2 * rows, total_width)],
        flops=flops,
    )
    out1 = local_kernel(high, place, (qkv, bias), [shaped(rows, width)], flops=flops)
    return out0, out1[0]


def spread(attended, w_out, layer, place, after):
    count = len(attended)
    rows, width = attended[0].shape
    inner, feats = w_out.shape[1:]
    half = feats // 2

    def body(place_ref, *refs):
        piece_refs, (w_ref, sent_ref, kept_ref, gathered, held, sem) = refs[:count], refs[count:]
        copy = pltpu.make_async_copy(w_ref.at[layer], held, sem.at[0])
        copy.start()
        for shift in range(count):
            source = lax.rem(place_ref[0] + count - shift, count)
            gathered[:, aligned(source, width)] = piece_refs[shift][...]
        copy.wait()
        core = place_ref[1]
        for index, out_ref in ((1 - core, sent_ref), (core, kept_ref)):
            out_ref[...] = jnp.dot(
                gathered[...], held[:, aligned(index, half)], preferred_element_type=jnp.float32
            ).astype(jnp.bfloat16)

    return local_kernel(
        body,
        place,
        attended,
        [shaped(rows, half)] * 2,
        scratch=[
            pltpu.VMEM((rows, inner), jnp.bfloat16),
            pltpu.VMEM((inner, feats), jnp.bfloat16),
            pltpu.SemaphoreType.DMA((1,)),
        ],
        hbm=(w_out,),
        flops=2 * rows * inner * feats,
        after=after,
    )


def total_of(*refs):
    total = refs[0][...].astype(jnp.float32)
    for ref in refs[1:]:
        total += ref[...].astype(jnp.float32)
    return total


def pair_up(kept, came, place):
    def body(place_ref, kept_ref, came_ref, out_ref):
        out_ref[...] = total_of(kept_ref, came_ref).astype(jnp.bfloat16)

    return local_kernel(body, place, (kept, came), [shaped(*kept.shape)])


def pair_apart(kept, came, place):
    rows, half = kept.shape
    piece = half // 2

    def body(place_ref, kept_ref, came_ref, sent_ref, stay_ref):
        far = place_ref[2]
        for index, out_ref in ((1 - far, sent_ref), (far, stay_ref)):
            span = aligned(index, piece)
            out_ref[...] = (
                kept_ref[:, span].astype(jnp.float32) + came_ref[:, span].astype(jnp.float32)
            ).astype(jnp.bfloat16)

    return local_kernel(body, place, (kept, came), [shaped(rows, piece)] * 2)


def renew(residual, pair, came, place, after):
    count = len(residual)

    def body(place_ref, *refs):
        piece_refs, (pair_ref, came_ref, out_ref) = refs[:count], refs[count:]
        if count == 1:
            branch = total_of(pair_ref, came_ref)
            out_ref[...] = (piece_refs[0][...].astype(jnp.float32) + branch).astype(jnp.bfloat16)
            return
        far = place_ref[2]
        for index, ref in ((far, piece_refs[0]), (1 - far, piece_refs[1])):
            span = aligned(index, ref.shape[1])
            branch = pair_ref[:, span].astype(jnp.float32) + came_ref[:, span].astype(jnp.float32)
            out_ref[:, span] = (ref[...].astype(jnp.float32) + branch).astype(jnp.bfloat16)

    return local_kernel(body, place, (*residual, pair, came), [shaped(*pair.shape)], after=after)[0]


def finish(residual, stay, came, place, sp_count):
    rows, piece = stay.shape
    part = rows // sp_count

    def body(place_ref, x_ref, stay_ref, came_ref, *out_refs):
        for shift in range(sp_count):
            target = lax.rem(place_ref[0] + shift, sp_count)
            span = aligned(target, part)
            branch = stay_ref[span, :].astype(jnp.float32) + came_ref[span, :].astype(jnp.float32)
            x_here = x_ref[span, aligned(place_ref[2], piece)].astype(jnp.float32)
            out_refs[shift][...] = (x_here + branch).astype(jnp.bfloat16)

    return local_kernel(body, place, (residual, stay, came), [shaped(part, piece)] * sp_count)


SLOTS = (
    lambda core, far: core * 2 + far,
    lambda core, far: core * 2 + 1 - far,
    lambda core, far: (1 - core) * 2 + far,
    lambda core, far: (1 - core) * 2 + 1 - far,
)


HALF_SLOTS = (lambda core, far: core, lambda core, far: 1 - core)


def assemble(parts, place, sp_count):
    rows, piece = parts[0][0].shape
    part = rows // sp_count
    count = len(parts[0])

    def body(place_ref, *refs):
        out_ref = refs[-1]
        for index in range(len(parts)):
            for which in range(count):
                slot = SLOTS[which](place_ref[1], place_ref[2])
                for plane in range(sp_count):
                    out_ref[pl.ds(index * part, part), aligned(plane * count + slot, piece)] = refs[
                        index * count + which
                    ][pl.ds(plane * part, part), :]

    flat = [array for pieces in parts for array in pieces]
    return local_kernel(body, place, flat, [shaped(part * len(parts), piece * count * sp_count)])[0]


def exchanged(held):
    far = swapped(held, "tp", 2)
    return [held, far, swapped(held, "tp", 1), swapped(far, "tp", 1)]


def stationary_plan(tokens, norm_gain, w_query, w_key, w_value, w_out, offset_bias):
    sp_count = lax.axis_size("sp")
    sp_index, tp_index = lax.axis_index("sp"), lax.axis_index("tp")
    place = jnp.stack([sp_index, tp_index % 2, tp_index // 2]).astype(jnp.int32)
    feats = w_query.shape[1]
    heads = offset_bias.shape[1] // sp_count
    width = heads * HD
    piece = feats // 4
    every_feat = feats * sp_count
    weights = (w_query, w_key, w_value)
    shifts = (1, -1)
    halves, scaled, made = [None, None], [None, None], [None, None]

    def chunk_of(part, step):
        return (-shifts[part] * (step + 1)) % sp_count

    def first_share(part, layer):
        slots = SLOTS if layer == 0 else HALF_SLOTS
        made[part], scaled[part] = project(
            (halves[part], slots, norm_gain), weights, layer, place, chunk_of(part, 0), width
        )

    def share(part, step, layer, arrived=None):
        last = step == sp_count - 1
        return project(
            scaled[part], weights, layer, place, chunk_of(part, step), width, arrived, last
        )[0]

    def sent_on(block, part):
        return lax.ppermute(block, "sp", ring(sp_count, shifts[part]))

    bias = window_bias(offset_bias, place, heads)
    blocks = over_sp(scatter_tokens(tokens, place, sp_count, feats, piece), sp_count)
    held = stack_blocks(blocks, place, 2, (bias,))
    far = [swapped(h, "tp", 2) for h in held]
    near = [swapped(h, "tp", 1) for h in held]
    halves[0] = [held[0], far[0], near[0], swapped(far[0], "tp", 1)]
    first_share(0, 0)
    far[1] = lax.optimization_barrier((far[1], made[0]))[0]
    near_far = swapped(far[1], "tp", 1)
    halves[1] = [held[1], far[1], near[1], near_far]
    first_share(1, 0)

    for layer in range(LAYERS):
        travelling = [sent_on(made[part], part) for part in range(2)]
        summed = lax.optimization_barrier((halves, made))[0]
        squares = over_sp([squares_of(summed, place)] * sp_count, sp_count)
        for step in range(1, sp_count - 1):
            for part in range(2):
                travelling[part] = sent_on(share(part, step, layer, travelling[part]), part)
        own = [share(part, sp_count - 1, layer) for part in range(2)]
        attended = attend(travelling, own, squares, bias, place, sp_count, heads, layer, every_feat)

        residuals = [pieces[:2] if layer == 0 else pieces[:1] for pieces in halves]
        pairs, after = [], (attended[1],)
        for part in range(2):
            gathered = over_sp([attended[part]] * sp_count, sp_count)
            sent, kept = spread(gathered, w_out, layer, place, after)
            came = swapped(sent, "tp", 1)
            pair = (pair_up if layer < LAYERS - 1 else pair_apart)(kept, came, place)
            pairs.append((pair, swapped(pair[0], "tp", 2)))
            after = (pair[0],)
        after = ()
        for part in range(2):
            pair, came = pairs[part]
            if layer < LAYERS - 1:
                mine = renew(residuals[part], pair[0], came, place, after)
                halves[part] = [mine, swapped(mine, "tp", 1)]
                first_share(part, layer + 1)
                after = (made[part],)
            else:
                blocks = finish(residuals[part][0], pair[1], came, place, sp_count)
                stacked = stack_blocks(over_sp(blocks, sp_count), place)[0]
                halves[part] = exchanged(stacked)
    return assemble(halves, place, sp_count)


def on_device(tokens, norm_gain, w_query, w_key, w_value, w_out, offset_bias):
    heads_here, sp_count = offset_bias.shape[1], lax.axis_size("sp")
    part_rows = tokens.shape[0] // 2
    arrays = (tokens, norm_gain, w_query, w_key, w_value, w_out, offset_bias)
    if heads_here % sp_count == 0 and lax.axis_size("tp") == 4 and part_rows % HD == 0:
        return stationary_plan(*arrays)
    return gathered_plan(*arrays)


def solution(mesh):
    return jax.shard_map(
        on_device,
        mesh=mesh,
        in_specs=(
            P(("grp", "sp"), None),
            P(),
            P(None, "sp", "tp"),
            P(None, "sp", "tp"),
            P(None, "sp", "tp"),
            P(None, "tp", "sp"),
            P(None, "tp", None, None),
        ),
        out_specs=P(("grp", "sp"), None),
        check_vma=False,
    )
```

```python
import jax
import jax.numpy as jnp
from jax import lax
from jax.experimental import pallas as pl
from jax.experimental.pallas import tpu as pltpu
from jax.sharding import PartitionSpec as P


HD = 128
GRID_W = 64
KR = 8
KC = 16
LAYERS = 2


norm_eps = 1e-06


def with_halo(block, sides, width):
    for axis, dim in sides:
        count = lax.axis_size(axis)
        forward = [(i, i + 1) for i in range(count - 1)]
        backward = [(target, source) for source, target in forward]
        low = lax.ppermute(
            lax.slice_in_dim(block, block.shape[dim] - width, None, axis=dim), axis, forward
        )
        high = lax.ppermute(lax.slice_in_dim(block, 0, width, axis=dim), axis, backward)
        block = jnp.concatenate([low, block, high], axis=dim)
    return block


def rms_rows(values, gain):
    wide = values.astype(jnp.float32)
    scaled = wide * lax.rsqrt(jnp.mean(wide * wide, axis=-1, keepdims=True) + norm_eps)
    return (scaled * gain.astype(jnp.float32)).astype(jnp.bfloat16)


def gathered_plan(tokens, norm_gain, w_query, w_key, w_value, w_out, offset_bias):
    sp_count = lax.axis_size("sp")
    sp_index = lax.axis_index("sp")
    tok_rows = tokens.shape[0]
    local_rows = tok_rows // GRID_W
    grid_rows = local_rows * sp_count
    heads_here = offset_bias.shape[1]
    head_width = heads_here * HD
    reach = KR // 2
    scale = HD ** (-0.5)
    columns = jnp.arange(GRID_W, dtype=jnp.int32)
    col_first = jnp.clip(columns - KC // 2, 0, GRID_W - KC)
    col_inside = (columns[None, :] >= col_first[:, None]) & (
        columns[None, :] < col_first[:, None] + KC
    )
    col_offset = jnp.clip(columns[None, :] - columns[:, None], 1 - KC, KC - 1) + KC - 1
    col_onehot = (
        jnp.arange(2 * KC - 1, dtype=jnp.int32)[:, None, None] == col_offset[None, :, :]
    ).astype(jnp.float32)
    first_row = sp_index * local_rows
    own_rows = first_row + jnp.arange(local_rows, dtype=jnp.int32)
    row_first = jnp.clip(own_rows - reach, 0, grid_rows - KR)
    band_start = row_first - first_row + reach
    row_offset = (
        row_first[:, None] + jnp.arange(KR, dtype=jnp.int32)[None, :] - own_rows[:, None] + KR - 1
    )
    row_onehot = (
        row_offset[:, :, None] == jnp.arange(2 * KR - 1, dtype=jnp.int32)[None, None, :]
    ).astype(jnp.float32)
    every_query, every_key, every_value, every_out = (
        lax.all_gather(w_query, "sp", axis=1, tiled=True),
        lax.all_gather(w_key, "sp", axis=1, tiled=True),
        lax.all_gather(w_value, "sp", axis=1, tiled=True),
        lax.all_gather(w_out, "sp", axis=2, tiled=True),
    )
    residual = tokens
    for layer_index in range(LAYERS):
        normed = rms_rows(residual, norm_gain[layer_index])
        queries = jnp.dot(normed, every_query[layer_index], preferred_element_type=jnp.float32)
        keys = jnp.dot(normed, every_key[layer_index], preferred_element_type=jnp.float32)
        values = jnp.dot(normed, every_value[layer_index], preferred_element_type=jnp.float32)
        out_weight = every_out[layer_index]
        queries = queries.astype(jnp.bfloat16).reshape(local_rows, GRID_W, heads_here, HD)
        key_values = jnp.concatenate(
            [keys.astype(jnp.bfloat16), values.astype(jnp.bfloat16)], axis=1
        )
        key_values = key_values.reshape(local_rows, GRID_W, 2 * head_width)
        padded = with_halo(key_values, (("sp", 0),), reach)
        bands = jax.vmap(lambda band_begin: lax.dynamic_slice_in_dim(padded, band_begin, KR, 0))(
            band_start
        )
        band_keys = bands[..., :head_width].reshape(local_rows, KR, GRID_W, heads_here, HD)
        band_values = bands[..., head_width:].reshape(local_rows, KR, GRID_W, heads_here, HD)
        col_bias = jnp.einsum(
            "hro,oqk->hrqk", offset_bias[layer_index], col_onehot, precision=lax.Precision.HIGHEST
        )
        full_bias = jnp.einsum(
            "ijr,hrqk->hiqjk", row_onehot, col_bias, precision=lax.Precision.HIGHEST
        )
        scores = jnp.einsum(
            "iqhd,ijkhd->hiqjk", queries, band_keys, preferred_element_type=jnp.float32
        )
        scores = scores * scale + full_bias
        scores = jnp.where(col_inside[None, None, :, None, :], scores, -jnp.inf)
        flattened = scores.reshape(heads_here, local_rows, GRID_W, KR * GRID_W)
        weights = jax.nn.softmax(flattened, axis=-1).astype(jnp.bfloat16)
        weights = weights.reshape(heads_here, local_rows, GRID_W, KR, GRID_W)
        attended = jnp.einsum(
            "hiqjk,ijkhd->iqhd", weights, band_values, preferred_element_type=jnp.float32
        )
        attended = attended.astype(jnp.bfloat16).reshape(tok_rows, head_width)
        branch = lax.psum(
            jnp.dot(attended, out_weight, preferred_element_type=jnp.float32).astype(jnp.bfloat16),
            "tp",
        ).astype(jnp.float32)
        residual = (residual.astype(jnp.float32) + branch).astype(jnp.bfloat16)
    return residual


VMEM_BYTES = 24 * 1024 * 1024


def ring(count, shift):
    return [(i, (i + shift) % count) for i in range(count)]


def swapped(array, axis, distance):
    count = lax.axis_size(axis)
    return lax.ppermute(array, axis, [(i, i ^ distance) for i in range(count)])


def aligned(index, size):
    return pl.ds(pl.multiple_of(index * size, size), size)


def local_kernel(body, place, arrays, outs, scratch=(), hbm=(), flops=0, after=()):
    vmem, smem = pl.BlockSpec(memory_space=pltpu.VMEM), pl.BlockSpec(memory_space=pltpu.SMEM)
    moved = sum(a.size * a.dtype.itemsize for a in (*arrays, *outs))
    inputs = 1 + len(arrays) + len(hbm)

    def ordered(*refs):
        body(*refs[:inputs], *refs[inputs + len(after) :])

    return pl.pallas_call(
        ordered,
        out_shape=list(outs),
        in_specs=[smem]
        + [vmem] * len(arrays)
        + [pl.BlockSpec(memory_space=pltpu.HBM)] * len(hbm)
        + [pl.BlockSpec(memory_space=pl.ANY)] * len(after),
        out_specs=[vmem] * len(outs),
        scratch_shapes=list(scratch),
        compiler_params=pltpu.CompilerParams(vmem_limit_bytes=VMEM_BYTES),
        cost_estimate=pl.CostEstimate(flops=flops, bytes_accessed=moved, transcendentals=0),
    )(place, *arrays, *(pltpu.with_memory_space_constraint(a, pltpu.HBM) for a in hbm), *after)


def shaped(*shape, dtype=jnp.bfloat16):
    return jax.ShapeDtypeStruct(shape, dtype)


def window_bias(offset_bias, place, heads):
    layers, _, offsets, reach = offset_bias.shape
    pairs = -(-offsets // 2)
    lanes = 2 * GRID_W

    def body(place_ref, table_ref, out_ref, padded):
        padded[...] = jnp.zeros_like(padded)
        lane = lax.broadcasted_iota(jnp.int32, (GRID_W, lanes), 1)
        query = lax.broadcasted_iota(jnp.int32, (GRID_W, lanes), 0)
        column = jnp.where(lane < GRID_W, lane, lane - GRID_W)
        first = jnp.clip(query - KC // 2, 0, GRID_W - KC)
        inside = (column >= first) & (column < first + KC)
        for layer in range(layers):
            for head in range(heads):
                padded[pl.ds(0, offsets), pl.ds(0, reach)] = table_ref[
                    layer, place_ref[0] * heads + head
                ]
                for pair in range(pairs):
                    sides = []
                    for side in range(2):
                        row = jnp.broadcast_to(
                            padded[pl.ds(2 * pair + side, 1), :], (GRID_W, lanes)
                        )
                        start = (side * GRID_W - (KC - 1)) % lanes
                        sides.append(pltpu.roll(row, start, 1, stride=1, stride_axis=0))
                    both = jnp.where(lane < GRID_W, sides[0], sides[1])
                    out_ref[layer * heads + head, :, pl.ds(pair * lanes, lanes)] = jnp.where(
                        inside, both, -jnp.inf
                    )

    return local_kernel(
        body,
        place,
        (offset_bias,),
        [shaped(layers * heads, GRID_W, pairs * lanes, dtype=jnp.float32)],
        scratch=[pltpu.VMEM((2 * pairs, lanes), jnp.float32)],
    )[0]


def scatter_tokens(tokens, place, sp_count, feats, piece):
    tok_here = tokens.shape[0]

    def body(place_ref, tokens_ref, *rest):
        out_refs, sem = rest[:-1], rest[-1]
        slot = place_ref[1] * 2 + place_ref[2]
        copies = []
        for shift in range(sp_count):
            target = lax.rem(place_ref[0] + shift, sp_count)
            column = pl.multiple_of(target * feats + slot * piece, piece)
            copy = pltpu.make_async_copy(
                tokens_ref.at[:, pl.ds(column, piece)], out_refs[shift], sem.at[shift]
            )
            copy.start()
            copies.append(copy)
        for copy in copies:
            copy.wait()

    return local_kernel(
        body,
        place,
        (),
        [shaped(tok_here, piece)] * sp_count,
        scratch=[pltpu.SemaphoreType.DMA((sp_count,))],
        hbm=(tokens,),
    )


def stack_blocks(blocks, place, parts=1, after=()):
    count = len(blocks)
    rows, width = blocks[0].shape
    rows = rows // parts

    def body(place_ref, *refs):
        for part in range(parts):
            for shift in range(count):
                source = lax.rem(place_ref[0] + count - shift, count)
                refs[count + part][aligned(source, rows), :] = refs[shift][
                    pl.ds(part * rows, rows), :
                ]

    return local_kernel(body, place, blocks, [shaped(rows * count, width)] * parts, after=after)


def over_sp(blocks, count):
    return [blocks[0]] + [
        lax.ppermute(blocks[shift], "sp", ring(count, shift)) for shift in range(1, count)
    ]


def scaled_by(slots, layer, feats, place_ref, piece_refs, gain_ref, out_ref):
    for piece_ref, slot in zip(piece_refs, slots):
        span = aligned(slot(place_ref[1], place_ref[2]), piece_ref.shape[1])
        start = pl.multiple_of(
            place_ref[0] * feats + slot(place_ref[1], place_ref[2]) * piece_ref.shape[1],
            piece_ref.shape[1],
        )
        factor = gain_ref[pl.ds(layer, 1), pl.ds(start, piece_ref.shape[1])].astype(jnp.float32)
        out_ref[:, span] = (piece_ref[...].astype(jnp.float32) * factor).astype(jnp.bfloat16)


def stage_weights(weights, layer, place, sp_count):
    feats, every_width = weights[0].shape[1:]
    width = every_width // sp_count
    count = len(weights)

    def body(place_ref, *refs):
        weight_refs, (out_ref, sem) = refs[:count], refs[count:]
        copies = []
        for chunk in range(sp_count):
            for index, weight_ref in enumerate(weight_refs):
                copy = pltpu.make_async_copy(
                    weight_ref.at[layer, :, pl.ds(chunk * width, width)],
                    out_ref.at[chunk, :, pl.ds(index * width, width)],
                    sem.at[chunk, index],
                )
                copy.start()
                copies.append(copy)
        for copy in copies:
            copy.wait()

    return local_kernel(
        body,
        place,
        (),
        [shaped(sp_count, feats, count * width)],
        scratch=[pltpu.SemaphoreType.DMA((sp_count, count))],
        hbm=weights,
    )[0]


EXTRA = 16


def put_squares(out_ref, squares, tok):
    for term in range(3):
        part = squares.astype(jnp.bfloat16)
        out_ref[pl.ds(tok, EXTRA), pl.ds(term * HD, HD)] = part
        squares = squares - part.astype(jnp.float32)


def get_squares(ref, tok):
    terms = [ref[pl.ds(tok, EXTRA), pl.ds(term * HD, HD)].astype(jnp.float32) for term in range(3)]
    return terms[0] + (terms[1] + terms[2])


def share(source, staged, layer, place, link, message, arrived=None):
    fresh = len(source) == 3
    sp_count, feats, total_width = staged.shape
    arrays = (*source[0], source[2]) if fresh else source
    tok = arrays[0].shape[0]
    count = len(arrays)
    inputs = (*arrays, staged) + (() if arrived is None else (arrived,))

    def body(place_ref, *refs):
        array_refs, staged_ref = refs[:count], refs[count]
        out_ref = refs[len(inputs)]
        if fresh:
            scaled_ref, squares_ref = refs[len(inputs) + 1 :]
            pieces, slots, _ = source
            scaled_by(
                slots,
                layer,
                feats,
                place_ref,
                array_refs[: len(pieces)],
                array_refs[len(pieces)],
                scaled_ref,
            )
            squares_ref[...] = jnp.zeros_like(squares_ref)
            for run in range(tok // HD):
                total = jnp.zeros((HD, HD), jnp.float32)
                for ref in array_refs[: len(pieces)]:
                    for lane in range(ref.shape[1] // HD):
                        part = ref[pl.ds(run * HD, HD), pl.ds(lane * HD, HD)].astype(jnp.float32)
                        total += part * part
                squares_ref[pl.ds(run, 1), :] = jnp.sum(total.T, axis=0, keepdims=True)
        else:
            scaled_ref, squares_ref = array_refs
        forward = place_ref[0] == link
        backward = place_ref[0] == sp_count - 1 - link

        @pl.when(forward | backward)
        def _():
            chunk = jnp.where(forward, sp_count - 1 - message, message)
            total = jnp.dot(
                scaled_ref[...], staged_ref[chunk], preferred_element_type=jnp.float32
            )
            squares = squares_ref[...]
            if arrived is not None:
                arrived_ref = refs[count + 1]
                total += arrived_ref[pl.ds(0, tok), :].astype(jnp.float32)
                squares += get_squares(arrived_ref, tok)
            out_ref[pl.ds(0, tok), :] = total.astype(jnp.bfloat16)
            put_squares(out_ref, squares, tok)

    outs = [shaped(tok + EXTRA, total_width)]
    if fresh:
        outs += [shaped(tok, feats), shaped(EXTRA, HD, dtype=jnp.float32)]
    return local_kernel(body, place, inputs, outs, flops=2 * tok * feats * total_width)


def own_share(scaled, staged, place):
    tok = scaled.shape[0]
    total_width = staged.shape[2]

    def body(place_ref, scaled_ref, staged_ref, out_ref):
        out_ref[...] = jnp.dot(
            scaled_ref[...], staged_ref[place_ref[0]], preferred_element_type=jnp.float32
        )

    return local_kernel(
        body,
        place,
        (scaled, staged),
        [shaped(tok, total_width, dtype=jnp.float32)],
        flops=2 * tok * scaled.shape[1] * total_width,
    )[0]


def attend_rows(qkv_ref, bias_ref, out_ref, part, sp_count, heads, layer):
    grid_rows = qkv_ref.shape[0] // GRID_W
    width = heads * HD
    part_grid = grid_rows // sp_count // 2
    for head in range(heads):
        lanes = head * HD
        for index in range(sp_count * part_grid):
            plane, inner = divmod(index, part_grid)
            row = (2 * plane + part) * part_grid + inner
            first = min(max(row - KR // 2, 0), grid_rows - KR)
            offset = first - row + KR - 1
            queries = qkv_ref[pl.ds(row * GRID_W, GRID_W), pl.ds(lanes, HD)]
            span = pl.ds(first * GRID_W, KR * GRID_W)
            keys = qkv_ref[span, pl.ds(width + lanes, HD)]
            values = qkv_ref[span, pl.ds(2 * width + lanes, HD)]
            scores = lax.dot_general(
                queries, keys, (((1,), (1,)), ((), ())), preferred_element_type=jnp.float32
            )
            bias_here = bias_ref[layer * heads + head, :, pl.ds(offset * GRID_W, KR * GRID_W)]
            scores = scores * HD ** (-0.5) + bias_here
            powers = jnp.exp(scores - jnp.max(scores, axis=-1, keepdims=True))
            weights = powers * (1.0 / jnp.sum(powers, axis=-1, keepdims=True))
            mixed = jnp.dot(
                weights.astype(jnp.bfloat16), values, preferred_element_type=jnp.float32
            )
            out_ref[pl.ds(index * GRID_W, GRID_W), pl.ds(lanes, HD)] = mixed.astype(jnp.bfloat16)


def attend(arrived, own, squares, bias, place, sp_count, heads, layer, every_feat, after):
    rows, total_width = own[0].shape
    width = heads * HD
    part_rows = rows // sp_count
    runs = rows // HD
    flops = 4 * heads * rows * KR * GRID_W * HD
    count = len(arrived[0])

    def low(place_ref, *refs):
        arrived_refs, refs = (refs[:count], refs[count : 2 * count]), refs[2 * count :]
        own_refs, square_refs, (bias_ref, out_ref, qkv_ref) = refs[:2], refs[2:4], refs[4:]
        for part in range(2):
            total_squares = square_refs[part][...]
            for ref in arrived_refs[part]:
                total_squares += get_squares(ref, rows)
            norm = lax.rsqrt(total_squares / every_feat + norm_eps)
            for run in range(runs):
                factor = jnp.broadcast_to(norm[run : run + 1, :], (HD, HD)).T
                plane, inner = divmod(run * HD, part_rows)
                to = pl.ds((2 * plane + part) * part_rows + inner, HD)
                span = pl.ds(run * HD, HD)
                for lane in range(total_width // HD):
                    lanes = pl.ds(lane * HD, HD)
                    total = own_refs[part][span, lanes]
                    for ref in arrived_refs[part]:
                        total += ref[span, lanes].astype(jnp.float32)
                    qkv_ref[to, lanes] = (total * factor).astype(jnp.bfloat16)
        attend_rows(qkv_ref, bias_ref, out_ref, 0, sp_count, heads, layer)

    def high(place_ref, qkv_ref, bias_ref, out_ref):
        attend_rows(qkv_ref, bias_ref, out_ref, 1, sp_count, heads, layer)

    out0, qkv = local_kernel(
        low,
        place,
        (*arrived[0], *arrived[1], *own, *squares, bias),
        [shaped(rows, width), shaped(2 * rows, total_width)],
        flops=flops,
        after=after,
    )
    out1 = local_kernel(high, place, (qkv, bias), [shaped(rows, width)], flops=flops)
    return out0, out1[0]


def gathered_on_line(block):
    count = lax.axis_size("sp")
    up = [(i, i + 1) for i in range(count - 1)]
    across = lax.ppermute(block, "sp", ring(count, 2))
    below = lax.ppermute(block, "sp", up)
    above = lax.ppermute(block, "sp", [(target, source) for source, target in up])
    relayed = lax.ppermute(across, "sp", [(count - 2, count - 1), (1, 0)])
    return block, below, above, across, relayed


def spread(attended, w_out, layer, place, after):
    sp_count = lax.axis_size("sp")
    rows, width = attended[0].shape
    inner, feats = w_out.shape[1:]
    half = feats // 2

    def body(place_ref, own_ref, below_ref, above_ref, across_ref, relayed_ref, w_ref, *rest):
        sent_ref, kept_ref, gathered = rest
        here = place_ref[0]

        def put(ref, index):
            gathered[:, aligned(lax.rem(index + sp_count, sp_count), width)] = ref[...]

        put(own_ref, here)
        put(across_ref, here + 2)

        @pl.when(here > 0)
        def _():
            put(below_ref, here - 1)

        @pl.when(here < sp_count - 1)
        def _():
            put(above_ref, here + 1)

        @pl.when((here == 0) | (here == sp_count - 1))
        def _():
            put(relayed_ref, sp_count - 1 - here)

        core = place_ref[1]
        for index, out_ref in ((1 - core, sent_ref), (core, kept_ref)):
            out_ref[...] = jnp.dot(
                gathered[...],
                w_ref[layer, :, aligned(index, half)],
                preferred_element_type=jnp.float32,
            ).astype(jnp.bfloat16)

    return local_kernel(
        body,
        place,
        (*attended, w_out),
        [shaped(rows, half)] * 2,
        scratch=[pltpu.VMEM((rows, inner), jnp.bfloat16)],
        flops=2 * rows * inner * feats,
        after=after,
    )


def total_of(*refs):
    total = refs[0][...].astype(jnp.float32)
    for ref in refs[1:]:
        total += ref[...].astype(jnp.float32)
    return total


def pair_up(kept, came, place):
    def body(place_ref, kept_ref, came_ref, out_ref):
        out_ref[...] = total_of(kept_ref, came_ref).astype(jnp.bfloat16)

    return local_kernel(body, place, (kept, came), [shaped(*kept.shape)])


def pair_apart(kept, came, place):
    rows, half = kept.shape
    piece = half // 2

    def body(place_ref, kept_ref, came_ref, sent_ref, stay_ref):
        far = place_ref[2]
        for index, out_ref in ((1 - far, sent_ref), (far, stay_ref)):
            span = aligned(index, piece)
            out_ref[...] = (
                kept_ref[:, span].astype(jnp.float32) + came_ref[:, span].astype(jnp.float32)
            ).astype(jnp.bfloat16)

    return local_kernel(body, place, (kept, came), [shaped(rows, piece)] * 2)


def renew(residual, pair, came, place, after):
    count = len(residual)

    def body(place_ref, *refs):
        piece_refs, (pair_ref, came_ref, out_ref) = refs[:count], refs[count:]
        if count == 1:
            branch = total_of(pair_ref, came_ref)
            out_ref[...] = (piece_refs[0][...].astype(jnp.float32) + branch).astype(jnp.bfloat16)
            return
        far = place_ref[2]
        for index, ref in ((far, piece_refs[0]), (1 - far, piece_refs[1])):
            span = aligned(index, ref.shape[1])
            branch = pair_ref[:, span].astype(jnp.float32) + came_ref[:, span].astype(jnp.float32)
            out_ref[:, span] = (ref[...].astype(jnp.float32) + branch).astype(jnp.bfloat16)

    return local_kernel(body, place, (*residual, pair, came), [shaped(*pair.shape)], after=after)[0]


def finish(residual, stay, came, place, sp_count):
    rows, piece = stay.shape
    part = rows // sp_count

    def body(place_ref, x_ref, stay_ref, came_ref, *out_refs):
        for shift in range(sp_count):
            target = lax.rem(place_ref[0] + shift, sp_count)
            span = aligned(target, part)
            branch = stay_ref[span, :].astype(jnp.float32) + came_ref[span, :].astype(jnp.float32)
            x_here = x_ref[span, aligned(place_ref[2], piece)].astype(jnp.float32)
            out_refs[shift][...] = (x_here + branch).astype(jnp.bfloat16)

    return local_kernel(body, place, (residual, stay, came), [shaped(part, piece)] * sp_count)


SLOTS = (
    lambda core, far: core * 2 + far,
    lambda core, far: core * 2 + 1 - far,
    lambda core, far: (1 - core) * 2 + far,
    lambda core, far: (1 - core) * 2 + 1 - far,
)


HALF_SLOTS = (lambda core, far: core, lambda core, far: 1 - core)


def assemble(parts, place, sp_count):
    rows, piece = parts[0][0].shape
    part = rows // sp_count
    count = len(parts[0])

    def body(place_ref, *refs):
        out_ref = refs[-1]
        for index in range(len(parts)):
            for which in range(count):
                slot = SLOTS[which](place_ref[1], place_ref[2])
                for plane in range(sp_count):
                    out_ref[pl.ds(index * part, part), aligned(plane * count + slot, piece)] = refs[
                        index * count + which
                    ][pl.ds(plane * part, part), :]

    flat = [array for pieces in parts for array in pieces]
    return local_kernel(body, place, flat, [shaped(part * len(parts), piece * count * sp_count)])[0]


def exchanged(held):
    far = swapped(held, "tp", 2)
    return [held, far, swapped(held, "tp", 1), swapped(far, "tp", 1)]


def stationary_plan(tokens, norm_gain, w_query, w_key, w_value, w_out, offset_bias):
    sp_count = lax.axis_size("sp")
    sp_index, tp_index = lax.axis_index("sp"), lax.axis_index("tp")
    place = jnp.stack([sp_index, tp_index % 2, tp_index // 2]).astype(jnp.int32)
    feats = w_query.shape[1]
    heads = offset_bias.shape[1] // sp_count
    piece = feats // 4
    every_feat = feats * sp_count
    weights = (w_query, w_key, w_value)
    halves = [None, None]
    sources = [None, None]
    links = sp_count - 1

    def line(block, link):
        pairs = [(link, link + 1), (sp_count - 1 - link, sp_count - 2 - link)]
        return lax.ppermute(block, "sp", pairs)

    def made(layer, link, message, part, arrived=None):
        return share(sources[part], staged[layer], layer, place, link, message, arrived)

    def first_made(layer, part):
        sources[part] = (halves[part], SLOTS if layer == 0 else HALF_SLOTS, norm_gain)
        block, scaled, squares = made(layer, 0, 0, part)
        sources[part] = (scaled, squares)
        return block

    bias = window_bias(offset_bias, place, heads)
    staged = []
    for layer in range(LAYERS):
        staged.append(stage_weights(weights, layer, place, sp_count))
    blocks = over_sp(scatter_tokens(tokens, place, sp_count, feats, piece), sp_count)
    held = stack_blocks(blocks, place, 2, (bias, staged[0]))
    far = [swapped(h, "tp", 2) for h in held]
    near = [swapped(h, "tp", 1) for h in held]
    halves[0] = [held[0], far[0], near[0], swapped(far[0], "tp", 1)]
    first = [first_made(0, 0), None]
    far[1] = lax.optimization_barrier((far[1], first[0]))[0]
    near_far = swapped(far[1], "tp", 1)
    halves[1] = [held[1], far[1], near[1], near_far]
    first[1] = first_made(0, 1)

    for layer in range(LAYERS):
        came = [{}, {}]
        for link in range(links):
            for message in range(links - link):
                for part in range(2):
                    if link == 0 and message == 0:
                        block = first[part]
                    else:
                        arrived = came[part].get((link - 1, message))
                        block = made(layer, link, message, part, arrived)[0]
                    came[part][link, message] = line(block, link)
        arrived = [[came[part][link, links - 1 - link] for link in range(links)] for part in range(2)]
        own = []
        for part in range(2):
            own.append(own_share(sources[part][0], staged[layer], place))
        squares = [source[1] for source in sources]
        attended = attend(
            arrived,
            own,
            squares,
            bias,
            place,
            sp_count,
            heads,
            layer,
            every_feat,
            staged[layer + 1 : layer + 2],
        )

        residuals = [pieces[:2] if layer == 0 else pieces[:1] for pieces in halves]
        pairs, after = [], (attended[1],)
        for part in range(2):
            gathered = gathered_on_line(attended[part])
            sent, kept = spread(gathered, w_out, layer, place, after)
            other = swapped(sent, "tp", 1)
            pair = (pair_up if layer < LAYERS - 1 else pair_apart)(kept, other, place)
            pairs.append((pair, swapped(pair[0], "tp", 2)))
            after = (pair[0],)
        after = ()
        for part in range(2):
            pair, other = pairs[part]
            if layer < LAYERS - 1:
                mine = renew(residuals[part], pair[0], other, place, after)
                halves[part] = [mine, swapped(mine, "tp", 1)]
                first[part] = first_made(layer + 1, part)
                after = (first[part],)
            else:
                blocks = finish(residuals[part][0], pair[1], other, place, sp_count)
                stacked = stack_blocks(over_sp(blocks, sp_count), place)[0]
                halves[part] = exchanged(stacked)
    return assemble(halves, place, sp_count)


def on_device(tokens, norm_gain, w_query, w_key, w_value, w_out, offset_bias):
    heads_here, sp_count = offset_bias.shape[1], lax.axis_size("sp")
    part_rows = tokens.shape[0] // 2
    arrays = (tokens, norm_gain, w_query, w_key, w_value, w_out, offset_bias)
    if heads_here == sp_count == 4 and lax.axis_size("tp") == 4 and part_rows % HD == 0:
        return stationary_plan(*arrays)
    return gathered_plan(*arrays)


def solution(mesh):
    return jax.shard_map(
        on_device,
        mesh=mesh,
        in_specs=(
            P(("grp", "sp"), None),
            P(),
            P(None, "sp", "tp"),
            P(None, "sp", "tp"),
            P(None, "sp", "tp"),
            P(None, "tp", "sp"),
            P(None, "tp", None, None),
        ),
        out_specs=P(("grp", "sp"), None),
        check_vma=False,
    )
```

```python
import jax
import jax.numpy as jnp
from jax import lax
from jax.experimental import pallas as pl
from jax.experimental.pallas import tpu as pltpu
from jax.sharding import PartitionSpec as P


HD = 128
GRID_W = 64
KR = 8
KC = 16
LAYERS = 2


norm_eps = 1e-06


def with_halo(block, sides, width):
    for axis, dim in sides:
        count = lax.axis_size(axis)
        forward = [(i, i + 1) for i in range(count - 1)]
        backward = [(target, source) for source, target in forward]
        low = lax.ppermute(
            lax.slice_in_dim(block, block.shape[dim] - width, None, axis=dim), axis, forward
        )
        high = lax.ppermute(lax.slice_in_dim(block, 0, width, axis=dim), axis, backward)
        block = jnp.concatenate([low, block, high], axis=dim)
    return block


def rms_rows(values, gain):
    wide = values.astype(jnp.float32)
    scaled = wide * lax.rsqrt(jnp.mean(wide * wide, axis=-1, keepdims=True) + norm_eps)
    return (scaled * gain.astype(jnp.float32)).astype(jnp.bfloat16)


def gathered_plan(tokens, norm_gain, w_query, w_key, w_value, w_out, offset_bias):
    sp_count = lax.axis_size("sp")
    sp_index = lax.axis_index("sp")
    tok_rows = tokens.shape[0]
    local_rows = tok_rows // GRID_W
    grid_rows = local_rows * sp_count
    heads_here = offset_bias.shape[1]
    head_width = heads_here * HD
    reach = KR // 2
    scale = HD ** (-0.5)
    columns = jnp.arange(GRID_W, dtype=jnp.int32)
    col_first = jnp.clip(columns - KC // 2, 0, GRID_W - KC)
    col_inside = (columns[None, :] >= col_first[:, None]) & (
        columns[None, :] < col_first[:, None] + KC
    )
    col_offset = jnp.clip(columns[None, :] - columns[:, None], 1 - KC, KC - 1) + KC - 1
    col_onehot = (
        jnp.arange(2 * KC - 1, dtype=jnp.int32)[:, None, None] == col_offset[None, :, :]
    ).astype(jnp.float32)
    first_row = sp_index * local_rows
    own_rows = first_row + jnp.arange(local_rows, dtype=jnp.int32)
    row_first = jnp.clip(own_rows - reach, 0, grid_rows - KR)
    band_start = row_first - first_row + reach
    row_offset = (
        row_first[:, None] + jnp.arange(KR, dtype=jnp.int32)[None, :] - own_rows[:, None] + KR - 1
    )
    row_onehot = (
        row_offset[:, :, None] == jnp.arange(2 * KR - 1, dtype=jnp.int32)[None, None, :]
    ).astype(jnp.float32)
    every_query, every_key, every_value, every_out = (
        lax.all_gather(w_query, "sp", axis=1, tiled=True),
        lax.all_gather(w_key, "sp", axis=1, tiled=True),
        lax.all_gather(w_value, "sp", axis=1, tiled=True),
        lax.all_gather(w_out, "sp", axis=2, tiled=True),
    )
    residual = tokens
    for layer_index in range(LAYERS):
        normed = rms_rows(residual, norm_gain[layer_index])
        queries = jnp.dot(normed, every_query[layer_index], preferred_element_type=jnp.float32)
        keys = jnp.dot(normed, every_key[layer_index], preferred_element_type=jnp.float32)
        values = jnp.dot(normed, every_value[layer_index], preferred_element_type=jnp.float32)
        out_weight = every_out[layer_index]
        queries = queries.astype(jnp.bfloat16).reshape(local_rows, GRID_W, heads_here, HD)
        key_values = jnp.concatenate(
            [keys.astype(jnp.bfloat16), values.astype(jnp.bfloat16)], axis=1
        )
        key_values = key_values.reshape(local_rows, GRID_W, 2 * head_width)
        padded = with_halo(key_values, (("sp", 0),), reach)
        bands = jax.vmap(lambda band_begin: lax.dynamic_slice_in_dim(padded, band_begin, KR, 0))(
            band_start
        )
        band_keys = bands[..., :head_width].reshape(local_rows, KR, GRID_W, heads_here, HD)
        band_values = bands[..., head_width:].reshape(local_rows, KR, GRID_W, heads_here, HD)
        col_bias = jnp.einsum(
            "hro,oqk->hrqk", offset_bias[layer_index], col_onehot, precision=lax.Precision.HIGHEST
        )
        full_bias = jnp.einsum(
            "ijr,hrqk->hiqjk", row_onehot, col_bias, precision=lax.Precision.HIGHEST
        )
        scores = jnp.einsum(
            "iqhd,ijkhd->hiqjk", queries, band_keys, preferred_element_type=jnp.float32
        )
        scores = scores * scale + full_bias
        scores = jnp.where(col_inside[None, None, :, None, :], scores, -jnp.inf)
        flattened = scores.reshape(heads_here, local_rows, GRID_W, KR * GRID_W)
        weights = jax.nn.softmax(flattened, axis=-1).astype(jnp.bfloat16)
        weights = weights.reshape(heads_here, local_rows, GRID_W, KR, GRID_W)
        attended = jnp.einsum(
            "hiqjk,ijkhd->iqhd", weights, band_values, preferred_element_type=jnp.float32
        )
        attended = attended.astype(jnp.bfloat16).reshape(tok_rows, head_width)
        branch = lax.psum(
            jnp.dot(attended, out_weight, preferred_element_type=jnp.float32).astype(jnp.bfloat16),
            "tp",
        ).astype(jnp.float32)
        residual = (residual.astype(jnp.float32) + branch).astype(jnp.bfloat16)
    return residual


VMEM_BYTES = 24 * 1024 * 1024


def ring(count, shift):
    return [(i, (i + shift) % count) for i in range(count)]


def swapped(array, axis, distance):
    count = lax.axis_size(axis)
    return lax.ppermute(array, axis, [(i, i ^ distance) for i in range(count)])


def aligned(index, size):
    return pl.ds(pl.multiple_of(index * size, size), size)


def local_kernel(body, place, arrays, outs, scratch=(), hbm=(), flops=0, after=()):
    vmem, smem = pl.BlockSpec(memory_space=pltpu.VMEM), pl.BlockSpec(memory_space=pltpu.SMEM)
    moved = sum(a.size * a.dtype.itemsize for a in (*arrays, *outs))
    inputs = 1 + len(arrays) + len(hbm)

    def ordered(*refs):
        body(*refs[:inputs], *refs[inputs + len(after) :])

    return pl.pallas_call(
        ordered,
        out_shape=list(outs),
        in_specs=[smem]
        + [vmem] * len(arrays)
        + [pl.BlockSpec(memory_space=pltpu.HBM)] * len(hbm)
        + [pl.BlockSpec(memory_space=pl.ANY)] * len(after),
        out_specs=[vmem] * len(outs),
        scratch_shapes=list(scratch),
        compiler_params=pltpu.CompilerParams(vmem_limit_bytes=VMEM_BYTES),
        cost_estimate=pl.CostEstimate(flops=flops, bytes_accessed=moved, transcendentals=0),
    )(place, *arrays, *(pltpu.with_memory_space_constraint(a, pltpu.HBM) for a in hbm), *after)


def shaped(*shape, dtype=jnp.bfloat16):
    return jax.ShapeDtypeStruct(shape, dtype)


def window_bias(offset_bias, place, heads):
    layers, _, offsets, reach = offset_bias.shape
    pairs = -(-offsets // 2)
    lanes = 2 * GRID_W

    def body(place_ref, table_ref, out_ref, padded):
        padded[...] = jnp.zeros_like(padded)
        lane = lax.broadcasted_iota(jnp.int32, (GRID_W, lanes), 1)
        query = lax.broadcasted_iota(jnp.int32, (GRID_W, lanes), 0)
        column = jnp.where(lane < GRID_W, lane, lane - GRID_W)
        first = jnp.clip(query - KC // 2, 0, GRID_W - KC)
        inside = (column >= first) & (column < first + KC)
        for layer in range(layers):
            for head in range(heads):
                padded[pl.ds(0, offsets), pl.ds(0, reach)] = table_ref[
                    layer, place_ref[0] * heads + head
                ]
                for pair in range(pairs):
                    sides = []
                    for side in range(2):
                        row = jnp.broadcast_to(
                            padded[pl.ds(2 * pair + side, 1), :], (GRID_W, lanes)
                        )
                        start = (side * GRID_W - (KC - 1)) % lanes
                        sides.append(pltpu.roll(row, start, 1, stride=1, stride_axis=0))
                    both = jnp.where(lane < GRID_W, sides[0], sides[1])
                    out_ref[layer * heads + head, :, pl.ds(pair * lanes, lanes)] = jnp.where(
                        inside, both, -jnp.inf
                    )

    return local_kernel(
        body,
        place,
        (offset_bias,),
        [shaped(layers * heads, GRID_W, pairs * lanes, dtype=jnp.float32)],
        scratch=[pltpu.VMEM((2 * pairs, lanes), jnp.float32)],
    )[0]


def scatter_tokens(tokens, place, sp_count, feats, piece):
    tok_here = tokens.shape[0]

    def body(place_ref, tokens_ref, *rest):
        out_refs, sem = rest[:-1], rest[-1]
        slot = place_ref[1] * 2 + place_ref[2]
        copies = []
        for shift in range(sp_count):
            target = lax.rem(place_ref[0] + shift, sp_count)
            column = pl.multiple_of(target * feats + slot * piece, piece)
            copy = pltpu.make_async_copy(
                tokens_ref.at[:, pl.ds(column, piece)], out_refs[shift], sem.at[shift]
            )
            copy.start()
            copies.append(copy)
        for copy in copies:
            copy.wait()

    return local_kernel(
        body,
        place,
        (),
        [shaped(tok_here, piece)] * sp_count,
        scratch=[pltpu.SemaphoreType.DMA((sp_count,))],
        hbm=(tokens,),
    )


def stack_blocks(blocks, place, parts=1, after=()):
    count = len(blocks)
    rows, width = blocks[0].shape
    rows = rows // parts

    def body(place_ref, *refs):
        for part in range(parts):
            for shift in range(count):
                source = lax.rem(place_ref[0] + count - shift, count)
                refs[count + part][aligned(source, rows), :] = refs[shift][
                    pl.ds(part * rows, rows), :
                ]

    return local_kernel(body, place, blocks, [shaped(rows * count, width)] * parts, after=after)


def over_sp(blocks, count):
    return [blocks[0]] + [
        lax.ppermute(blocks[shift], "sp", ring(count, shift)) for shift in range(1, count)
    ]


def scaled_by(slots, layer, feats, place_ref, piece_refs, gain_ref, out_ref):
    for piece_ref, slot in zip(piece_refs, slots):
        span = aligned(slot(place_ref[1], place_ref[2]), piece_ref.shape[1])
        start = pl.multiple_of(
            place_ref[0] * feats + slot(place_ref[1], place_ref[2]) * piece_ref.shape[1],
            piece_ref.shape[1],
        )
        factor = gain_ref[pl.ds(layer, 1), pl.ds(start, piece_ref.shape[1])].astype(jnp.float32)
        out_ref[:, span] = (piece_ref[...].astype(jnp.float32) * factor).astype(jnp.bfloat16)


def stage_weights(weights, layer, place, sp_count):
    feats, every_width = weights[0].shape[1:]
    width = every_width // sp_count
    count = len(weights)

    def body(place_ref, *refs):
        weight_refs, (out_ref, sem) = refs[:count], refs[count:]
        copies = []
        for chunk in range(sp_count):
            for index, weight_ref in enumerate(weight_refs):
                copy = pltpu.make_async_copy(
                    weight_ref.at[layer, :, pl.ds(chunk * width, width)],
                    out_ref.at[chunk, :, pl.ds(index * width, width)],
                    sem.at[chunk, index],
                )
                copy.start()
                copies.append(copy)
        for copy in copies:
            copy.wait()

    return local_kernel(
        body,
        place,
        (),
        [shaped(sp_count, feats, count * width)],
        scratch=[pltpu.SemaphoreType.DMA((sp_count, count))],
        hbm=weights,
    )[0]


EXTRA = 16


def put_squares(out_ref, squares, tok):
    for term in range(3):
        part = squares.astype(jnp.bfloat16)
        out_ref[pl.ds(tok, EXTRA), pl.ds(term * HD, HD)] = part
        squares = squares - part.astype(jnp.float32)


def get_squares(ref, tok):
    terms = [ref[pl.ds(tok, EXTRA), pl.ds(term * HD, HD)].astype(jnp.float32) for term in range(3)]
    return terms[0] + (terms[1] + terms[2])


def share(source, staged, layer, place, chunk_shift, arrived=None):
    fresh = len(source) == 3
    sp_count, feats, total_width = staged.shape
    arrays = (*source[0], source[2]) if fresh else source
    tok = arrays[0].shape[0]
    count = len(arrays)
    inputs = (*arrays, staged) + (() if arrived is None else (arrived,))

    def body(place_ref, *refs):
        array_refs, staged_ref = refs[:count], refs[count]
        out_ref = refs[len(inputs)]
        if fresh:
            scaled_ref, squares_ref = refs[len(inputs) + 1 :]
            pieces, slots, _ = source
            scaled_by(
                slots,
                layer,
                feats,
                place_ref,
                array_refs[: len(pieces)],
                array_refs[len(pieces)],
                scaled_ref,
            )
            squares_ref[...] = jnp.zeros_like(squares_ref)
            for run in range(tok // HD):
                total = jnp.zeros((HD, HD), jnp.float32)
                for ref in array_refs[: len(pieces)]:
                    for lane in range(ref.shape[1] // HD):
                        part = ref[pl.ds(run * HD, HD), pl.ds(lane * HD, HD)].astype(jnp.float32)
                        total += part * part
                squares_ref[pl.ds(run, 1), :] = jnp.sum(total.T, axis=0, keepdims=True)
        else:
            scaled_ref, squares_ref = array_refs
        chunk = lax.rem(place_ref[0] + chunk_shift, sp_count)
        total = jnp.dot(scaled_ref[...], staged_ref[chunk], preferred_element_type=jnp.float32)
        squares = squares_ref[...]
        if arrived is not None:
            arrived_ref = refs[count + 1]
            total += arrived_ref[pl.ds(0, tok), :].astype(jnp.float32)
            squares += get_squares(arrived_ref, tok)
        out_ref[pl.ds(0, tok), :] = total.astype(jnp.bfloat16)
        put_squares(out_ref, squares, tok)

    outs = [shaped(tok + EXTRA, total_width)]
    if fresh:
        outs += [shaped(tok, feats), shaped(EXTRA, HD, dtype=jnp.float32)]
    return local_kernel(body, place, inputs, outs, flops=2 * tok * feats * total_width)


def own_share(scaled, staged, place):
    tok = scaled.shape[0]
    total_width = staged.shape[2]

    def body(place_ref, scaled_ref, staged_ref, out_ref):
        out_ref[...] = jnp.dot(
            scaled_ref[...], staged_ref[place_ref[0]], preferred_element_type=jnp.float32
        )

    return local_kernel(
        body,
        place,
        (scaled, staged),
        [shaped(tok, total_width, dtype=jnp.float32)],
        flops=2 * tok * scaled.shape[1] * total_width,
    )[0]


def attend_rows(qkv_ref, bias_ref, out_ref, part, sp_count, heads, layer):
    grid_rows = qkv_ref.shape[0] // GRID_W
    width = heads * HD
    part_grid = grid_rows // sp_count // 2
    for head in range(heads):
        lanes = head * HD
        for index in range(sp_count * part_grid):
            plane, inner = divmod(index, part_grid)
            row = (2 * plane + part) * part_grid + inner
            first = min(max(row - KR // 2, 0), grid_rows - KR)
            offset = first - row + KR - 1
            queries = qkv_ref[pl.ds(row * GRID_W, GRID_W), pl.ds(lanes, HD)]
            span = pl.ds(first * GRID_W, KR * GRID_W)
            keys = qkv_ref[span, pl.ds(width + lanes, HD)]
            values = qkv_ref[span, pl.ds(2 * width + lanes, HD)]
            scores = lax.dot_general(
                queries, keys, (((1,), (1,)), ((), ())), preferred_element_type=jnp.float32
            )
            bias_here = bias_ref[layer * heads + head, :, pl.ds(offset * GRID_W, KR * GRID_W)]
            scores = scores * HD ** (-0.5) + bias_here
            powers = jnp.exp(scores - jnp.max(scores, axis=-1, keepdims=True))
            weights = powers * (1.0 / jnp.sum(powers, axis=-1, keepdims=True))
            mixed = jnp.dot(
                weights.astype(jnp.bfloat16), values, preferred_element_type=jnp.float32
            )
            out_ref[pl.ds(index * GRID_W, GRID_W), pl.ds(lanes, HD)] = mixed.astype(jnp.bfloat16)


def attend(arrived, own, squares, bias, place, sp_count, heads, layer, every_feat, after):
    rows, total_width = own[0].shape
    width = heads * HD
    part_rows = rows // sp_count
    runs = rows // HD
    flops = 4 * heads * rows * KR * GRID_W * HD
    count = len(arrived[0])

    def low(place_ref, *refs):
        arrived_refs, refs = (refs[:count], refs[count : 2 * count]), refs[2 * count :]
        own_refs, square_refs, (bias_ref, out_ref, qkv_ref) = refs[:2], refs[2:4], refs[4:]
        for part in range(2):
            total_squares = square_refs[part][...]
            for ref in arrived_refs[part]:
                total_squares += get_squares(ref, rows)
            norm = lax.rsqrt(total_squares / every_feat + norm_eps)
            for run in range(runs):
                factor = jnp.broadcast_to(norm[run : run + 1, :], (HD, HD)).T
                plane, inner = divmod(run * HD, part_rows)
                to = pl.ds((2 * plane + part) * part_rows + inner, HD)
                span = pl.ds(run * HD, HD)
                for lane in range(total_width // HD):
                    lanes = pl.ds(lane * HD, HD)
                    total = own_refs[part][span, lanes]
                    for ref in arrived_refs[part]:
                        total += ref[span, lanes].astype(jnp.float32)
                    qkv_ref[to, lanes] = (total * factor).astype(jnp.bfloat16)
        attend_rows(qkv_ref, bias_ref, out_ref, 0, sp_count, heads, layer)

    def high(place_ref, qkv_ref, bias_ref, out_ref):
        attend_rows(qkv_ref, bias_ref, out_ref, 1, sp_count, heads, layer)

    out0, qkv = local_kernel(
        low,
        place,
        (*arrived[0], *arrived[1], *own, *squares, bias),
        [shaped(rows, width), shaped(2 * rows, total_width)],
        flops=flops,
        after=after,
    )
    out1 = local_kernel(high, place, (qkv, bias), [shaped(rows, width)], flops=flops)
    return out0, out1[0]


def spread(attended, w_out, layer, place, after):
    sp_count = lax.axis_size("sp")
    rows, width = attended[0].shape
    inner, feats = w_out.shape[1:]
    half = feats // 2

    def body(place_ref, *refs):
        piece_refs, (w_ref, sent_ref, kept_ref, gathered) = refs[:sp_count], refs[sp_count:]
        for shift in range(sp_count):
            source = lax.rem(place_ref[0] + sp_count - shift, sp_count)
            gathered[:, aligned(source, width)] = piece_refs[shift][...]
        core = place_ref[1]
        for index, out_ref in ((1 - core, sent_ref), (core, kept_ref)):
            out_ref[...] = jnp.dot(
                gathered[...],
                w_ref[layer, :, aligned(index, half)],
                preferred_element_type=jnp.float32,
            ).astype(jnp.bfloat16)

    return local_kernel(
        body,
        place,
        (*attended, w_out),
        [shaped(rows, half)] * 2,
        scratch=[pltpu.VMEM((rows, inner), jnp.bfloat16)],
        flops=2 * rows * inner * feats,
        after=after,
    )


def total_of(*refs):
    total = refs[0][...].astype(jnp.float32)
    for ref in refs[1:]:
        total += ref[...].astype(jnp.float32)
    return total


def pair_up(kept, came, place):
    def body(place_ref, kept_ref, came_ref, out_ref):
        out_ref[...] = total_of(kept_ref, came_ref).astype(jnp.bfloat16)

    return local_kernel(body, place, (kept, came), [shaped(*kept.shape)])


def pair_apart(kept, came, place):
    rows, half = kept.shape
    piece = half // 2

    def body(place_ref, kept_ref, came_ref, sent_ref, stay_ref):
        far = place_ref[2]
        for index, out_ref in ((1 - far, sent_ref), (far, stay_ref)):
            span = aligned(index, piece)
            out_ref[...] = (
                kept_ref[:, span].astype(jnp.float32) + came_ref[:, span].astype(jnp.float32)
            ).astype(jnp.bfloat16)

    return local_kernel(body, place, (kept, came), [shaped(rows, piece)] * 2)


def renew(residual, pair, came, place, after):
    count = len(residual)

    def body(place_ref, *refs):
        piece_refs, (pair_ref, came_ref, out_ref) = refs[:count], refs[count:]
        if count == 1:
            branch = total_of(pair_ref, came_ref)
            out_ref[...] = (piece_refs[0][...].astype(jnp.float32) + branch).astype(jnp.bfloat16)
            return
        far = place_ref[2]
        for index, ref in ((far, piece_refs[0]), (1 - far, piece_refs[1])):
            span = aligned(index, ref.shape[1])
            branch = pair_ref[:, span].astype(jnp.float32) + came_ref[:, span].astype(jnp.float32)
            out_ref[:, span] = (ref[...].astype(jnp.float32) + branch).astype(jnp.bfloat16)

    return local_kernel(body, place, (*residual, pair, came), [shaped(*pair.shape)], after=after)[0]


def finish(residual, stay, came, place, sp_count):
    rows, piece = stay.shape
    part = rows // sp_count

    def body(place_ref, x_ref, stay_ref, came_ref, *out_refs):
        for shift in range(sp_count):
            target = lax.rem(place_ref[0] + shift, sp_count)
            span = aligned(target, part)
            branch = stay_ref[span, :].astype(jnp.float32) + came_ref[span, :].astype(jnp.float32)
            x_here = x_ref[span, aligned(place_ref[2], piece)].astype(jnp.float32)
            out_refs[shift][...] = (x_here + branch).astype(jnp.bfloat16)

    return local_kernel(body, place, (residual, stay, came), [shaped(part, piece)] * sp_count)


SLOTS = (
    lambda core, far: core * 2 + far,
    lambda core, far: core * 2 + 1 - far,
    lambda core, far: (1 - core) * 2 + far,
    lambda core, far: (1 - core) * 2 + 1 - far,
)


HALF_SLOTS = (lambda core, far: core, lambda core, far: 1 - core)


def assemble(parts, place, sp_count):
    rows, piece = parts[0][0].shape
    part = rows // sp_count
    count = len(parts[0])

    def body(place_ref, *refs):
        out_ref = refs[-1]
        for index in range(len(parts)):
            for which in range(count):
                slot = SLOTS[which](place_ref[1], place_ref[2])
                for plane in range(sp_count):
                    out_ref[pl.ds(index * part, part), aligned(plane * count + slot, piece)] = refs[
                        index * count + which
                    ][pl.ds(plane * part, part), :]

    flat = [array for pieces in parts for array in pieces]
    return local_kernel(body, place, flat, [shaped(part * len(parts), piece * count * sp_count)])[0]


def exchanged(held):
    far = swapped(held, "tp", 2)
    return [held, far, swapped(held, "tp", 1), swapped(far, "tp", 1)]


def stationary_plan(tokens, norm_gain, w_query, w_key, w_value, w_out, offset_bias):
    sp_count = lax.axis_size("sp")
    sp_index, tp_index = lax.axis_index("sp"), lax.axis_index("tp")
    place = jnp.stack([sp_index, tp_index % 2, tp_index // 2]).astype(jnp.int32)
    feats = w_query.shape[1]
    heads = offset_bias.shape[1] // sp_count
    piece = feats // 4
    every_feat = feats * sp_count
    weights = (w_query, w_key, w_value)
    halves = [None, None]
    sources = [None, None]
    shifts = (1, -1)

    def sent_on(block, part):
        return lax.ppermute(block, "sp", ring(sp_count, shifts[part]))

    def made(layer, part, step, arrived=None):
        chunk = (-shifts[part] * (step + 1)) % sp_count
        return share(sources[part], staged[layer], layer, place, chunk, arrived)

    def first_made(layer, part):
        sources[part] = (halves[part], SLOTS if layer == 0 else HALF_SLOTS, norm_gain)
        block, scaled, squares = made(layer, part, 0)
        sources[part] = (scaled, squares)
        return block

    bias = window_bias(offset_bias, place, heads)
    staged = []
    for layer in range(LAYERS):
        staged.append(stage_weights(weights, layer, place, sp_count))
    blocks = over_sp(scatter_tokens(tokens, place, sp_count, feats, piece), sp_count)
    held = stack_blocks(blocks, place, 2, (bias, staged[0]))
    far = [swapped(h, "tp", 2) for h in held]
    near = [swapped(h, "tp", 1) for h in held]
    halves[0] = [held[0], far[0], near[0], swapped(far[0], "tp", 1)]
    first = [first_made(0, 0), None]
    far[1] = lax.optimization_barrier((far[1], first[0]))[0]
    near_far = swapped(far[1], "tp", 1)
    halves[1] = [held[1], far[1], near[1], near_far]
    first[1] = first_made(0, 1)

    for layer in range(LAYERS):
        travelling = [sent_on(first[part], part) for part in range(2)]
        for step in range(1, sp_count - 1):
            for part in range(2):
                block = made(layer, part, step, travelling[part])[0]
                travelling[part] = sent_on(block, part)
        own = []
        for part in range(2):
            own.append(own_share(sources[part][0], staged[layer], place))
        squares = [source[1] for source in sources]
        attended = attend(
            [travelling[:1], travelling[1:]],
            own,
            squares,
            bias,
            place,
            sp_count,
            heads,
            layer,
            every_feat,
            staged[layer + 1 : layer + 2],
        )

        residuals = [pieces[:2] if layer == 0 else pieces[:1] for pieces in halves]
        pairs, after = [], (attended[1],)
        for part in range(2):
            gathered = over_sp([attended[part]] * sp_count, sp_count)
            sent, kept = spread(gathered, w_out, layer, place, after)
            other = swapped(sent, "tp", 1)
            pair = (pair_up if layer < LAYERS - 1 else pair_apart)(kept, other, place)
            pairs.append((pair, swapped(pair[0], "tp", 2)))
            after = (pair[0],)
        after = ()
        for part in range(2):
            pair, other = pairs[part]
            if layer < LAYERS - 1:
                mine = renew(residuals[part], pair[0], other, place, after)
                halves[part] = [mine, swapped(mine, "tp", 1)]
                first[part] = first_made(layer + 1, part)
                after = (first[part],)
            else:
                blocks = finish(residuals[part][0], pair[1], other, place, sp_count)
                stacked = stack_blocks(over_sp(blocks, sp_count), place)[0]
                halves[part] = exchanged(stacked)
    return assemble(halves, place, sp_count)


def on_device(tokens, norm_gain, w_query, w_key, w_value, w_out, offset_bias):
    heads_here, sp_count = offset_bias.shape[1], lax.axis_size("sp")
    part_rows = tokens.shape[0] // 2
    arrays = (tokens, norm_gain, w_query, w_key, w_value, w_out, offset_bias)
    if heads_here % sp_count == 0 and lax.axis_size("tp") == 4 and part_rows % HD == 0:
        return stationary_plan(*arrays)
    return gathered_plan(*arrays)


def solution(mesh):
    return jax.shard_map(
        on_device,
        mesh=mesh,
        in_specs=(
            P(("grp", "sp"), None),
            P(),
            P(None, "sp", "tp"),
            P(None, "sp", "tp"),
            P(None, "sp", "tp"),
            P(None, "tp", "sp"),
            P(None, "tp", None, None),
        ),
        out_specs=P(("grp", "sp"), None),
        check_vma=False,
    )
```

```python
import jax
import jax.numpy as jnp
from jax import lax
from jax.experimental import pallas as pl
from jax.experimental.pallas import tpu as pltpu
from jax.sharding import PartitionSpec as P


HD = 128
GRID_W = 64
KR = 8
KC = 16
LAYERS = 2


norm_eps = 1e-06


def with_halo(block, sides, width):
    for axis, dim in sides:
        count = lax.axis_size(axis)
        forward = [(i, i + 1) for i in range(count - 1)]
        backward = [(target, source) for source, target in forward]
        low = lax.ppermute(
            lax.slice_in_dim(block, block.shape[dim] - width, None, axis=dim), axis, forward
        )
        high = lax.ppermute(lax.slice_in_dim(block, 0, width, axis=dim), axis, backward)
        block = jnp.concatenate([low, block, high], axis=dim)
    return block


def rms_rows(values, gain):
    wide = values.astype(jnp.float32)
    scaled = wide * lax.rsqrt(jnp.mean(wide * wide, axis=-1, keepdims=True) + norm_eps)
    return (scaled * gain.astype(jnp.float32)).astype(jnp.bfloat16)


def gathered_plan(tokens, norm_gain, w_query, w_key, w_value, w_out, offset_bias):
    sp_count = lax.axis_size("sp")
    sp_index = lax.axis_index("sp")
    tok_rows = tokens.shape[0]
    local_rows = tok_rows // GRID_W
    grid_rows = local_rows * sp_count
    heads_here = offset_bias.shape[1]
    head_width = heads_here * HD
    reach = KR // 2
    scale = HD ** (-0.5)
    columns = jnp.arange(GRID_W, dtype=jnp.int32)
    col_first = jnp.clip(columns - KC // 2, 0, GRID_W - KC)
    col_inside = (columns[None, :] >= col_first[:, None]) & (
        columns[None, :] < col_first[:, None] + KC
    )
    col_offset = jnp.clip(columns[None, :] - columns[:, None], 1 - KC, KC - 1) + KC - 1
    col_onehot = (
        jnp.arange(2 * KC - 1, dtype=jnp.int32)[:, None, None] == col_offset[None, :, :]
    ).astype(jnp.float32)
    first_row = sp_index * local_rows
    own_rows = first_row + jnp.arange(local_rows, dtype=jnp.int32)
    row_first = jnp.clip(own_rows - reach, 0, grid_rows - KR)
    band_start = row_first - first_row + reach
    row_offset = (
        row_first[:, None] + jnp.arange(KR, dtype=jnp.int32)[None, :] - own_rows[:, None] + KR - 1
    )
    row_onehot = (
        row_offset[:, :, None] == jnp.arange(2 * KR - 1, dtype=jnp.int32)[None, None, :]
    ).astype(jnp.float32)
    every_query, every_key, every_value, every_out = (
        lax.all_gather(w_query, "sp", axis=1, tiled=True),
        lax.all_gather(w_key, "sp", axis=1, tiled=True),
        lax.all_gather(w_value, "sp", axis=1, tiled=True),
        lax.all_gather(w_out, "sp", axis=2, tiled=True),
    )
    residual = tokens
    for layer_index in range(LAYERS):
        normed = rms_rows(residual, norm_gain[layer_index])
        queries = jnp.dot(normed, every_query[layer_index], preferred_element_type=jnp.float32)
        keys = jnp.dot(normed, every_key[layer_index], preferred_element_type=jnp.float32)
        values = jnp.dot(normed, every_value[layer_index], preferred_element_type=jnp.float32)
        out_weight = every_out[layer_index]
        queries = queries.astype(jnp.bfloat16).reshape(local_rows, GRID_W, heads_here, HD)
        key_values = jnp.concatenate(
            [keys.astype(jnp.bfloat16), values.astype(jnp.bfloat16)], axis=1
        )
        key_values = key_values.reshape(local_rows, GRID_W, 2 * head_width)
        padded = with_halo(key_values, (("sp", 0),), reach)
        bands = jax.vmap(lambda band_begin: lax.dynamic_slice_in_dim(padded, band_begin, KR, 0))(
            band_start
        )
        band_keys = bands[..., :head_width].reshape(local_rows, KR, GRID_W, heads_here, HD)
        band_values = bands[..., head_width:].reshape(local_rows, KR, GRID_W, heads_here, HD)
        col_bias = jnp.einsum(
            "hro,oqk->hrqk", offset_bias[layer_index], col_onehot, precision=lax.Precision.HIGHEST
        )
        full_bias = jnp.einsum(
            "ijr,hrqk->hiqjk", row_onehot, col_bias, precision=lax.Precision.HIGHEST
        )
        scores = jnp.einsum(
            "iqhd,ijkhd->hiqjk", queries, band_keys, preferred_element_type=jnp.float32
        )
        scores = scores * scale + full_bias
        scores = jnp.where(col_inside[None, None, :, None, :], scores, -jnp.inf)
        flattened = scores.reshape(heads_here, local_rows, GRID_W, KR * GRID_W)
        weights = jax.nn.softmax(flattened, axis=-1).astype(jnp.bfloat16)
        weights = weights.reshape(heads_here, local_rows, GRID_W, KR, GRID_W)
        attended = jnp.einsum(
            "hiqjk,ijkhd->iqhd", weights, band_values, preferred_element_type=jnp.float32
        )
        attended = attended.astype(jnp.bfloat16).reshape(tok_rows, head_width)
        branch = lax.psum(
            jnp.dot(attended, out_weight, preferred_element_type=jnp.float32).astype(jnp.bfloat16),
            "tp",
        ).astype(jnp.float32)
        residual = (residual.astype(jnp.float32) + branch).astype(jnp.bfloat16)
    return residual


VMEM_BYTES = 24 * 1024 * 1024


def ring(count, shift):
    return [(i, (i + shift) % count) for i in range(count)]


def swapped(array, axis, distance):
    count = lax.axis_size(axis)
    return lax.ppermute(array, axis, [(i, i ^ distance) for i in range(count)])


def aligned(index, size):
    return pl.ds(pl.multiple_of(index * size, size), size)


def local_kernel(body, place, arrays, outs, scratch=(), hbm=(), flops=0, after=()):
    vmem, smem = pl.BlockSpec(memory_space=pltpu.VMEM), pl.BlockSpec(memory_space=pltpu.SMEM)
    moved = sum(a.size * a.dtype.itemsize for a in (*arrays, *outs))
    inputs = 1 + len(arrays) + len(hbm)

    def ordered(*refs):
        body(*refs[:inputs], *refs[inputs + len(after) :])

    return pl.pallas_call(
        ordered,
        out_shape=list(outs),
        in_specs=[smem]
        + [vmem] * len(arrays)
        + [pl.BlockSpec(memory_space=pltpu.HBM)] * len(hbm)
        + [pl.BlockSpec(memory_space=pl.ANY)] * len(after),
        out_specs=[vmem] * len(outs),
        scratch_shapes=list(scratch),
        compiler_params=pltpu.CompilerParams(vmem_limit_bytes=VMEM_BYTES),
        cost_estimate=pl.CostEstimate(flops=flops, bytes_accessed=moved, transcendentals=0),
    )(place, *arrays, *(pltpu.with_memory_space_constraint(a, pltpu.HBM) for a in hbm), *after)


def shaped(*shape, dtype=jnp.bfloat16):
    return jax.ShapeDtypeStruct(shape, dtype)


def window_bias(offset_bias, place, heads):
    layers, _, offsets, reach = offset_bias.shape
    pairs = -(-offsets // 2)
    lanes = 2 * GRID_W

    def body(place_ref, table_ref, out_ref, padded):
        padded[...] = jnp.zeros_like(padded)
        lane = lax.broadcasted_iota(jnp.int32, (GRID_W, lanes), 1)
        query = lax.broadcasted_iota(jnp.int32, (GRID_W, lanes), 0)
        column = jnp.where(lane < GRID_W, lane, lane - GRID_W)
        first = jnp.clip(query - KC // 2, 0, GRID_W - KC)
        inside = (column >= first) & (column < first + KC)
        for layer in range(layers):
            for head in range(heads):
                padded[pl.ds(0, offsets), pl.ds(0, reach)] = table_ref[
                    layer, place_ref[0] * heads + head
                ]
                for pair in range(pairs):
                    sides = []
                    for side in range(2):
                        row = jnp.broadcast_to(
                            padded[pl.ds(2 * pair + side, 1), :], (GRID_W, lanes)
                        )
                        start = (side * GRID_W - (KC - 1)) % lanes
                        sides.append(pltpu.roll(row, start, 1, stride=1, stride_axis=0))
                    both = jnp.where(lane < GRID_W, sides[0], sides[1])
                    out_ref[layer * heads + head, :, pl.ds(pair * lanes, lanes)] = jnp.where(
                        inside, both, -jnp.inf
                    )

    return local_kernel(
        body,
        place,
        (offset_bias,),
        [shaped(layers * heads, GRID_W, pairs * lanes, dtype=jnp.float32)],
        scratch=[pltpu.VMEM((2 * pairs, lanes), jnp.float32)],
    )[0]


def scatter_tokens(tokens, place, sp_count, feats, piece):
    tok_here = tokens.shape[0]

    def body(place_ref, tokens_ref, *rest):
        out_refs, sem = rest[:-1], rest[-1]
        slot = place_ref[1] * 2 + place_ref[2]
        copies = []
        for shift in range(sp_count):
            target = lax.rem(place_ref[0] + shift, sp_count)
            column = pl.multiple_of(target * feats + slot * piece, piece)
            copy = pltpu.make_async_copy(
                tokens_ref.at[:, pl.ds(column, piece)], out_refs[shift], sem.at[shift]
            )
            copy.start()
            copies.append(copy)
        for copy in copies:
            copy.wait()

    return local_kernel(
        body,
        place,
        (),
        [shaped(tok_here, piece)] * sp_count,
        scratch=[pltpu.SemaphoreType.DMA((sp_count,))],
        hbm=(tokens,),
    )


def stack_blocks(blocks, place, parts=1, after=()):
    count = len(blocks)
    rows, width = blocks[0].shape
    rows = rows // parts

    def body(place_ref, *refs):
        for part in range(parts):
            for shift in range(count):
                source = lax.rem(place_ref[0] + count - shift, count)
                refs[count + part][aligned(source, rows), :] = refs[shift][
                    pl.ds(part * rows, rows), :
                ]

    return local_kernel(body, place, blocks, [shaped(rows * count, width)] * parts, after=after)


def over_sp(blocks, count):
    return [blocks[0]] + [
        lax.ppermute(blocks[shift], "sp", ring(count, shift)) for shift in range(1, count)
    ]


def scaled_by(slots, layer, feats, place_ref, piece_refs, gain_ref, out_ref):
    for piece_ref, slot in zip(piece_refs, slots):
        span = aligned(slot(place_ref[1], place_ref[2]), piece_ref.shape[1])
        start = pl.multiple_of(
            place_ref[0] * feats + slot(place_ref[1], place_ref[2]) * piece_ref.shape[1],
            piece_ref.shape[1],
        )
        factor = gain_ref[pl.ds(layer, 1), pl.ds(start, piece_ref.shape[1])].astype(jnp.float32)
        out_ref[:, span] = (piece_ref[...].astype(jnp.float32) * factor).astype(jnp.bfloat16)


def stage_weights(weights, layer, place, sp_count):
    feats, every_width = weights[0].shape[1:]
    width = every_width // sp_count
    count = len(weights)

    def body(place_ref, *refs):
        weight_refs, (out_ref, sem) = refs[:count], refs[count:]
        copies = []
        for chunk in range(sp_count):
            for index, weight_ref in enumerate(weight_refs):
                copy = pltpu.make_async_copy(
                    weight_ref.at[layer, :, pl.ds(chunk * width, width)],
                    out_ref.at[chunk, :, pl.ds(index * width, width)],
                    sem.at[chunk, index],
                )
                copy.start()
                copies.append(copy)
        for copy in copies:
            copy.wait()

    return local_kernel(
        body,
        place,
        (),
        [shaped(sp_count, feats, count * width)],
        scratch=[pltpu.SemaphoreType.DMA((sp_count, count))],
        hbm=weights,
    )[0]


EXTRA = 16


def put_squares(out_ref, squares, tok):
    for term in range(3):
        part = squares.astype(jnp.bfloat16)
        out_ref[pl.ds(tok, EXTRA), pl.ds(term * HD, HD)] = part
        squares = squares - part.astype(jnp.float32)


def get_squares(ref, tok):
    terms = [ref[pl.ds(tok, EXTRA), pl.ds(term * HD, HD)].astype(jnp.float32) for term in range(3)]
    return terms[0] + (terms[1] + terms[2])


def share(source, staged, layer, place, chunk_shift, arrived=None):
    fresh = len(source) == 3
    sp_count, feats, total_width = staged.shape
    arrays = (*source[0], source[2]) if fresh else source
    tok = arrays[0].shape[0]
    count = len(arrays)
    inputs = (*arrays, staged) + (() if arrived is None else (arrived,))

    def body(place_ref, *refs):
        array_refs, staged_ref = refs[:count], refs[count]
        out_ref = refs[len(inputs)]
        if fresh:
            scaled_ref, squares_ref = refs[len(inputs) + 1 :]
            pieces, slots, _ = source
            scaled_by(
                slots,
                layer,
                feats,
                place_ref,
                array_refs[: len(pieces)],
                array_refs[len(pieces)],
                scaled_ref,
            )
            squares_ref[...] = jnp.zeros_like(squares_ref)
            for run in range(tok // HD):
                total = jnp.zeros((HD, HD), jnp.float32)
                for ref in array_refs[: len(pieces)]:
                    for lane in range(ref.shape[1] // HD):
                        part = ref[pl.ds(run * HD, HD), pl.ds(lane * HD, HD)].astype(jnp.float32)
                        total += part * part
                squares_ref[pl.ds(run, 1), :] = jnp.sum(total.T, axis=0, keepdims=True)
        else:
            scaled_ref, squares_ref = array_refs
        chunk = lax.rem(place_ref[0] + chunk_shift, sp_count)
        total = jnp.dot(scaled_ref[...], staged_ref[chunk], preferred_element_type=jnp.float32)
        squares = squares_ref[...]
        if arrived is not None:
            arrived_ref = refs[count + 1]
            total += arrived_ref[pl.ds(0, tok), :].astype(jnp.float32)
            squares += get_squares(arrived_ref, tok)
        out_ref[pl.ds(0, tok), :] = total.astype(jnp.bfloat16)
        put_squares(out_ref, squares, tok)

    outs = [shaped(tok + EXTRA, total_width)]
    if fresh:
        outs += [shaped(tok, feats), shaped(EXTRA, HD, dtype=jnp.float32)]
    return local_kernel(body, place, inputs, outs, flops=2 * tok * feats * total_width)


def own_share(scaled, staged, place):
    tok = scaled.shape[0]
    total_width = staged.shape[2]

    def body(place_ref, scaled_ref, staged_ref, out_ref):
        out_ref[...] = jnp.dot(
            scaled_ref[...], staged_ref[place_ref[0]], preferred_element_type=jnp.float32
        )

    return local_kernel(
        body,
        place,
        (scaled, staged),
        [shaped(tok, total_width, dtype=jnp.float32)],
        flops=2 * tok * scaled.shape[1] * total_width,
    )[0]


def attend_rows(qkv_ref, bias_ref, out_ref, part, sp_count, heads, layer):
    grid_rows = qkv_ref.shape[0] // GRID_W
    width = heads * HD
    part_grid = grid_rows // sp_count // 2
    done = []
    for head in range(heads):
        lanes = head * HD
        for plane in range(sp_count):
            rows = [(2 * plane + part) * part_grid + inner for inner in range(part_grid)]
            firsts = [min(max(row - KR // 2, 0), grid_rows - KR) for row in rows]
            low, reach = firsts[0], firsts[-1] - firsts[0] + KR
            queries = qkv_ref[pl.ds(rows[0] * GRID_W, part_grid * GRID_W), pl.ds(lanes, HD)]
            span = pl.ds(low * GRID_W, reach * GRID_W)
            keys = qkv_ref[span, pl.ds(width + lanes, HD)]
            values = qkv_ref[span, pl.ds(2 * width + lanes, HD)]
            scores = lax.dot_general(
                queries, keys, (((1,), (1,)), ((), ())), preferred_element_type=jnp.float32
            )
            biases = []
            for row, first in zip(rows, firsts):
                offset = low - row + KR - 1
                here = bias_ref[layer * heads + head, :, pl.ds(offset * GRID_W, reach * GRID_W)]
                if reach > KR:
                    key_row = lax.broadcasted_iota(jnp.int32, here.shape, 1) // GRID_W + low
                    here = jnp.where((key_row >= first) & (key_row < first + KR), here, -jnp.inf)
                biases.append(here)
            scores = scores * HD ** (-0.5) + jnp.concatenate(biases, axis=0)
            powers = jnp.exp(scores - jnp.max(scores, axis=-1, keepdims=True))
            weights = powers * (1.0 / jnp.sum(powers, axis=-1, keepdims=True))
            mixed = jnp.dot(
                weights.astype(jnp.bfloat16), values, preferred_element_type=jnp.float32
            )
            done.append((plane * part_grid * GRID_W, lanes, mixed.astype(jnp.bfloat16)))
    for at, lanes, block in done:
        out_ref[pl.ds(at, part_grid * GRID_W), pl.ds(lanes, HD)] = block


def attend(arrived, own, squares, bias, place, sp_count, heads, layer, every_feat, after):
    rows, total_width = own[0].shape
    width = heads * HD
    part_rows = rows // sp_count
    runs = rows // HD
    flops = 4 * heads * rows * KR * GRID_W * HD
    count = len(arrived[0])

    def low(place_ref, *refs):
        arrived_refs, refs = (refs[:count], refs[count : 2 * count]), refs[2 * count :]
        own_refs, square_refs, (bias_ref, out_ref, qkv_ref) = refs[:2], refs[2:4], refs[4:]
        for part in range(2):
            total_squares = square_refs[part][...]
            for ref in arrived_refs[part]:
                total_squares += get_squares(ref, rows)
            norm = lax.rsqrt(total_squares / every_feat + norm_eps)
            for run in range(runs):
                factor = jnp.broadcast_to(norm[run : run + 1, :], (HD, HD)).T
                plane, inner = divmod(run * HD, part_rows)
                to = pl.ds((2 * plane + part) * part_rows + inner, HD)
                span = pl.ds(run * HD, HD)
                for lane in range(total_width // HD):
                    lanes = pl.ds(lane * HD, HD)
                    total = own_refs[part][span, lanes]
                    for ref in arrived_refs[part]:
                        total += ref[span, lanes].astype(jnp.float32)
                    qkv_ref[to, lanes] = (total * factor).astype(jnp.bfloat16)
        attend_rows(qkv_ref, bias_ref, out_ref, 0, sp_count, heads, layer)

    def high(place_ref, qkv_ref, bias_ref, out_ref):
        attend_rows(qkv_ref, bias_ref, out_ref, 1, sp_count, heads, layer)

    out0, qkv = local_kernel(
        low,
        place,
        (*arrived[0], *arrived[1], *own, *squares, bias),
        [shaped(rows, width), shaped(2 * rows, total_width)],
        flops=flops,
        after=after,
    )
    out1 = local_kernel(high, place, (qkv, bias), [shaped(rows, width)], flops=flops)
    return out0, out1[0]


def spread(attended, w_out, layer, place, after):
    sp_count = lax.axis_size("sp")
    rows, width = attended[0].shape
    inner, feats = w_out.shape[1:]
    half = feats // 2

    def body(place_ref, *refs):
        piece_refs, (w_ref, sent_ref, kept_ref, gathered) = refs[:sp_count], refs[sp_count:]
        for shift in range(sp_count):
            source = lax.rem(place_ref[0] + sp_count - shift, sp_count)
            gathered[:, aligned(source, width)] = piece_refs[shift][...]
        core = place_ref[1]
        for index, out_ref in ((1 - core, sent_ref), (core, kept_ref)):
            out_ref[...] = jnp.dot(
                gathered[...],
                w_ref[layer, :, aligned(index, half)],
                preferred_element_type=jnp.float32,
            ).astype(jnp.bfloat16)

    return local_kernel(
        body,
        place,
        (*attended, w_out),
        [shaped(rows, half)] * 2,
        scratch=[pltpu.VMEM((rows, inner), jnp.bfloat16)],
        flops=2 * rows * inner * feats,
        after=after,
    )


def total_of(*refs):
    total = refs[0][...].astype(jnp.float32)
    for ref in refs[1:]:
        total += ref[...].astype(jnp.float32)
    return total


def pair_up(kept, came, place):
    def body(place_ref, kept_ref, came_ref, out_ref):
        out_ref[...] = total_of(kept_ref, came_ref).astype(jnp.bfloat16)

    return local_kernel(body, place, (kept, came), [shaped(*kept.shape)])


def pair_apart(kept, came, place):
    rows, half = kept.shape
    piece = half // 2

    def body(place_ref, kept_ref, came_ref, sent_ref, stay_ref):
        far = place_ref[2]
        for index, out_ref in ((1 - far, sent_ref), (far, stay_ref)):
            span = aligned(index, piece)
            out_ref[...] = (
                kept_ref[:, span].astype(jnp.float32) + came_ref[:, span].astype(jnp.float32)
            ).astype(jnp.bfloat16)

    return local_kernel(body, place, (kept, came), [shaped(rows, piece)] * 2)


def renew(residual, pair, came, place, after):
    count = len(residual)

    def body(place_ref, *refs):
        piece_refs, (pair_ref, came_ref, out_ref) = refs[:count], refs[count:]
        if count == 1:
            branch = total_of(pair_ref, came_ref)
            out_ref[...] = (piece_refs[0][...].astype(jnp.float32) + branch).astype(jnp.bfloat16)
            return
        far = place_ref[2]
        for index, ref in ((far, piece_refs[0]), (1 - far, piece_refs[1])):
            span = aligned(index, ref.shape[1])
            branch = pair_ref[:, span].astype(jnp.float32) + came_ref[:, span].astype(jnp.float32)
            out_ref[:, span] = (ref[...].astype(jnp.float32) + branch).astype(jnp.bfloat16)

    return local_kernel(body, place, (*residual, pair, came), [shaped(*pair.shape)], after=after)[0]


def finish(residual, stay, came, place, sp_count):
    rows, piece = stay.shape
    part = rows // sp_count

    def body(place_ref, x_ref, stay_ref, came_ref, *out_refs):
        for shift in range(sp_count):
            target = lax.rem(place_ref[0] + shift, sp_count)
            span = aligned(target, part)
            branch = stay_ref[span, :].astype(jnp.float32) + came_ref[span, :].astype(jnp.float32)
            x_here = x_ref[span, aligned(place_ref[2], piece)].astype(jnp.float32)
            out_refs[shift][...] = (x_here + branch).astype(jnp.bfloat16)

    return local_kernel(body, place, (residual, stay, came), [shaped(part, piece)] * sp_count)


SLOTS = (
    lambda core, far: core * 2 + far,
    lambda core, far: core * 2 + 1 - far,
    lambda core, far: (1 - core) * 2 + far,
    lambda core, far: (1 - core) * 2 + 1 - far,
)


HALF_SLOTS = (lambda core, far: core, lambda core, far: 1 - core)


def assemble(parts, place, sp_count):
    rows, piece = parts[0][0].shape
    part = rows // sp_count
    count = len(parts[0])

    def body(place_ref, *refs):
        out_ref = refs[-1]
        for index in range(len(parts)):
            for which in range(count):
                slot = SLOTS[which](place_ref[1], place_ref[2])
                for plane in range(sp_count):
                    out_ref[pl.ds(index * part, part), aligned(plane * count + slot, piece)] = refs[
                        index * count + which
                    ][pl.ds(plane * part, part), :]

    flat = [array for pieces in parts for array in pieces]
    return local_kernel(body, place, flat, [shaped(part * len(parts), piece * count * sp_count)])[0]


def exchanged(held):
    far = swapped(held, "tp", 2)
    return [held, far, swapped(held, "tp", 1), swapped(far, "tp", 1)]


def stationary_plan(tokens, norm_gain, w_query, w_key, w_value, w_out, offset_bias):
    sp_count = lax.axis_size("sp")
    sp_index, tp_index = lax.axis_index("sp"), lax.axis_index("tp")
    place = jnp.stack([sp_index, tp_index % 2, tp_index // 2]).astype(jnp.int32)
    feats = w_query.shape[1]
    heads = offset_bias.shape[1] // sp_count
    piece = feats // 4
    every_feat = feats * sp_count
    weights = (w_query, w_key, w_value)
    halves = [None, None]
    sources = [None, None]
    shifts = (1, -1)

    def sent_on(block, part):
        return lax.ppermute(block, "sp", ring(sp_count, shifts[part]))

    def made(layer, part, step, arrived=None):
        chunk = (-shifts[part] * (step + 1)) % sp_count
        return share(sources[part], staged[layer], layer, place, chunk, arrived)

    def first_made(layer, part):
        sources[part] = (halves[part], SLOTS if layer == 0 else HALF_SLOTS, norm_gain)
        block, scaled, squares = made(layer, part, 0)
        sources[part] = (scaled, squares)
        return block

    bias = window_bias(offset_bias, place, heads)
    staged = []
    for layer in range(LAYERS):
        staged.append(stage_weights(weights, layer, place, sp_count))
    blocks = over_sp(scatter_tokens(tokens, place, sp_count, feats, piece), sp_count)
    held = stack_blocks(blocks, place, 2, (bias, staged[0]))
    far = [swapped(h, "tp", 2) for h in held]
    near = [swapped(h, "tp", 1) for h in held]
    halves[0] = [held[0], far[0], near[0], swapped(far[0], "tp", 1)]
    first = [first_made(0, 0), None]
    far[1] = lax.optimization_barrier((far[1], first[0]))[0]
    near_far = swapped(far[1], "tp", 1)
    halves[1] = [held[1], far[1], near[1], near_far]
    first[1] = first_made(0, 1)

    for layer in range(LAYERS):
        travelling = [sent_on(first[part], part) for part in range(2)]
        for step in range(1, sp_count - 1):
            for part in range(2):
                block = made(layer, part, step, travelling[part])[0]
                travelling[part] = sent_on(block, part)
        own = []
        for part in range(2):
            own.append(own_share(sources[part][0], staged[layer], place))
        squares = [source[1] for source in sources]
        attended = attend(
            [travelling[:1], travelling[1:]],
            own,
            squares,
            bias,
            place,
            sp_count,
            heads,
            layer,
            every_feat,
            staged[layer + 1 : layer + 2],
        )

        residuals = [pieces[:2] if layer == 0 else pieces[:1] for pieces in halves]
        pairs, after = [], (attended[1],)
        for part in range(2):
            gathered = over_sp([attended[part]] * sp_count, sp_count)
            sent, kept = spread(gathered, w_out, layer, place, after)
            other = swapped(sent, "tp", 1)
            pair = (pair_up if layer < LAYERS - 1 else pair_apart)(kept, other, place)
            pairs.append((pair, swapped(pair[0], "tp", 2)))
            after = (pair[0],)
        after = ()
        for part in range(2):
            pair, other = pairs[part]
            if layer < LAYERS - 1:
                mine = renew(residuals[part], pair[0], other, place, after)
                halves[part] = [mine, swapped(mine, "tp", 1)]
                first[part] = first_made(layer + 1, part)
                after = (first[part],)
            else:
                blocks = finish(residuals[part][0], pair[1], other, place, sp_count)
                stacked = stack_blocks(over_sp(blocks, sp_count), place)[0]
                halves[part] = exchanged(stacked)
    return assemble(halves, place, sp_count)


def on_device(tokens, norm_gain, w_query, w_key, w_value, w_out, offset_bias):
    heads_here, sp_count = offset_bias.shape[1], lax.axis_size("sp")
    part_rows = tokens.shape[0] // 2
    arrays = (tokens, norm_gain, w_query, w_key, w_value, w_out, offset_bias)
    if heads_here % sp_count == 0 and lax.axis_size("tp") == 4 and part_rows % HD == 0:
        return stationary_plan(*arrays)
    return gathered_plan(*arrays)


def solution(mesh):
    return jax.shard_map(
        on_device,
        mesh=mesh,
        in_specs=(
            P(("grp", "sp"), None),
            P(),
            P(None, "sp", "tp"),
            P(None, "sp", "tp"),
            P(None, "sp", "tp"),
            P(None, "tp", "sp"),
            P(None, "tp", None, None),
        ),
        out_specs=P(("grp", "sp"), None),
        check_vma=False,
    )
```

```python
import jax
import jax.numpy as jnp
from jax import lax
from jax.experimental import pallas as pl
from jax.experimental.pallas import tpu as pltpu
from jax.sharding import PartitionSpec as P


HD = 128
GRID_W = 64
KR = 8
KC = 16
LAYERS = 2


norm_eps = 1e-06


def with_halo(block, sides, width):
    for axis, dim in sides:
        count = lax.axis_size(axis)
        forward = [(i, i + 1) for i in range(count - 1)]
        backward = [(target, source) for source, target in forward]
        low = lax.ppermute(
            lax.slice_in_dim(block, block.shape[dim] - width, None, axis=dim), axis, forward
        )
        high = lax.ppermute(lax.slice_in_dim(block, 0, width, axis=dim), axis, backward)
        block = jnp.concatenate([low, block, high], axis=dim)
    return block


def rms_rows(values, gain):
    wide = values.astype(jnp.float32)
    scaled = wide * lax.rsqrt(jnp.mean(wide * wide, axis=-1, keepdims=True) + norm_eps)
    return (scaled * gain.astype(jnp.float32)).astype(jnp.bfloat16)


def gathered_plan(tokens, norm_gain, w_query, w_key, w_value, w_out, offset_bias):
    sp_count = lax.axis_size("sp")
    sp_index = lax.axis_index("sp")
    tok_rows = tokens.shape[0]
    local_rows = tok_rows // GRID_W
    grid_rows = local_rows * sp_count
    heads_here = offset_bias.shape[1]
    head_width = heads_here * HD
    reach = KR // 2
    scale = HD ** (-0.5)
    columns = jnp.arange(GRID_W, dtype=jnp.int32)
    col_first = jnp.clip(columns - KC // 2, 0, GRID_W - KC)
    col_inside = (columns[None, :] >= col_first[:, None]) & (
        columns[None, :] < col_first[:, None] + KC
    )
    col_offset = jnp.clip(columns[None, :] - columns[:, None], 1 - KC, KC - 1) + KC - 1
    col_onehot = (
        jnp.arange(2 * KC - 1, dtype=jnp.int32)[:, None, None] == col_offset[None, :, :]
    ).astype(jnp.float32)
    first_row = sp_index * local_rows
    own_rows = first_row + jnp.arange(local_rows, dtype=jnp.int32)
    row_first = jnp.clip(own_rows - reach, 0, grid_rows - KR)
    band_start = row_first - first_row + reach
    row_offset = (
        row_first[:, None] + jnp.arange(KR, dtype=jnp.int32)[None, :] - own_rows[:, None] + KR - 1
    )
    row_onehot = (
        row_offset[:, :, None] == jnp.arange(2 * KR - 1, dtype=jnp.int32)[None, None, :]
    ).astype(jnp.float32)
    every_query, every_key, every_value, every_out = (
        lax.all_gather(w_query, "sp", axis=1, tiled=True),
        lax.all_gather(w_key, "sp", axis=1, tiled=True),
        lax.all_gather(w_value, "sp", axis=1, tiled=True),
        lax.all_gather(w_out, "sp", axis=2, tiled=True),
    )
    residual = tokens
    for layer_index in range(LAYERS):
        normed = rms_rows(residual, norm_gain[layer_index])
        queries = jnp.dot(normed, every_query[layer_index], preferred_element_type=jnp.float32)
        keys = jnp.dot(normed, every_key[layer_index], preferred_element_type=jnp.float32)
        values = jnp.dot(normed, every_value[layer_index], preferred_element_type=jnp.float32)
        out_weight = every_out[layer_index]
        queries = queries.astype(jnp.bfloat16).reshape(local_rows, GRID_W, heads_here, HD)
        key_values = jnp.concatenate(
            [keys.astype(jnp.bfloat16), values.astype(jnp.bfloat16)], axis=1
        )
        key_values = key_values.reshape(local_rows, GRID_W, 2 * head_width)
        padded = with_halo(key_values, (("sp", 0),), reach)
        bands = jax.vmap(lambda band_begin: lax.dynamic_slice_in_dim(padded, band_begin, KR, 0))(
            band_start
        )
        band_keys = bands[..., :head_width].reshape(local_rows, KR, GRID_W, heads_here, HD)
        band_values = bands[..., head_width:].reshape(local_rows, KR, GRID_W, heads_here, HD)
        col_bias = jnp.einsum(
            "hro,oqk->hrqk", offset_bias[layer_index], col_onehot, precision=lax.Precision.HIGHEST
        )
        full_bias = jnp.einsum(
            "ijr,hrqk->hiqjk", row_onehot, col_bias, precision=lax.Precision.HIGHEST
        )
        scores = jnp.einsum(
            "iqhd,ijkhd->hiqjk", queries, band_keys, preferred_element_type=jnp.float32
        )
        scores = scores * scale + full_bias
        scores = jnp.where(col_inside[None, None, :, None, :], scores, -jnp.inf)
        flattened = scores.reshape(heads_here, local_rows, GRID_W, KR * GRID_W)
        weights = jax.nn.softmax(flattened, axis=-1).astype(jnp.bfloat16)
        weights = weights.reshape(heads_here, local_rows, GRID_W, KR, GRID_W)
        attended = jnp.einsum(
            "hiqjk,ijkhd->iqhd", weights, band_values, preferred_element_type=jnp.float32
        )
        attended = attended.astype(jnp.bfloat16).reshape(tok_rows, head_width)
        branch = lax.psum(
            jnp.dot(attended, out_weight, preferred_element_type=jnp.float32).astype(jnp.bfloat16),
            "tp",
        ).astype(jnp.float32)
        residual = (residual.astype(jnp.float32) + branch).astype(jnp.bfloat16)
    return residual


VMEM_BYTES = 24 * 1024 * 1024


def ring(count, shift):
    return [(i, (i + shift) % count) for i in range(count)]


def swapped(array, axis, distance):
    count = lax.axis_size(axis)
    return lax.ppermute(array, axis, [(i, i ^ distance) for i in range(count)])


def aligned(index, size):
    return pl.ds(pl.multiple_of(index * size, size), size)


def local_kernel(body, place, arrays, outs, scratch=(), hbm=(), flops=0, after=()):
    vmem, smem = pl.BlockSpec(memory_space=pltpu.VMEM), pl.BlockSpec(memory_space=pltpu.SMEM)
    moved = sum(a.size * a.dtype.itemsize for a in (*arrays, *outs))
    inputs = 1 + len(arrays) + len(hbm)

    def ordered(*refs):
        body(*refs[:inputs], *refs[inputs + len(after) :])

    return pl.pallas_call(
        ordered,
        out_shape=list(outs),
        in_specs=[smem]
        + [vmem] * len(arrays)
        + [pl.BlockSpec(memory_space=pltpu.HBM)] * len(hbm)
        + [pl.BlockSpec(memory_space=pl.ANY)] * len(after),
        out_specs=[vmem] * len(outs),
        scratch_shapes=list(scratch),
        compiler_params=pltpu.CompilerParams(vmem_limit_bytes=VMEM_BYTES),
        cost_estimate=pl.CostEstimate(flops=flops, bytes_accessed=moved, transcendentals=0),
    )(place, *arrays, *(pltpu.with_memory_space_constraint(a, pltpu.HBM) for a in hbm), *after)


def shaped(*shape, dtype=jnp.bfloat16):
    return jax.ShapeDtypeStruct(shape, dtype)


def window_bias(offset_bias, place, heads):
    layers, _, offsets, reach = offset_bias.shape
    pairs = -(-offsets // 2)
    lanes = 2 * GRID_W

    def body(place_ref, table_ref, out_ref, padded):
        padded[...] = jnp.zeros_like(padded)
        lane = lax.broadcasted_iota(jnp.int32, (GRID_W, lanes), 1)
        query = lax.broadcasted_iota(jnp.int32, (GRID_W, lanes), 0)
        column = jnp.where(lane < GRID_W, lane, lane - GRID_W)
        first = jnp.clip(query - KC // 2, 0, GRID_W - KC)
        inside = (column >= first) & (column < first + KC)
        for layer in range(layers):
            for head in range(heads):
                padded[pl.ds(0, offsets), pl.ds(0, reach)] = table_ref[
                    layer, place_ref[0] * heads + head
                ]
                for pair in range(pairs):
                    sides = []
                    for side in range(2):
                        row = jnp.broadcast_to(
                            padded[pl.ds(2 * pair + side, 1), :], (GRID_W, lanes)
                        )
                        start = (side * GRID_W - (KC - 1)) % lanes
                        sides.append(pltpu.roll(row, start, 1, stride=1, stride_axis=0))
                    both = jnp.where(lane < GRID_W, sides[0], sides[1])
                    out_ref[layer * heads + head, :, pl.ds(pair * lanes, lanes)] = jnp.where(
                        inside, both, -jnp.inf
                    )

    return local_kernel(
        body,
        place,
        (offset_bias,),
        [shaped(layers * heads, GRID_W, pairs * lanes, dtype=jnp.float32)],
        scratch=[pltpu.VMEM((2 * pairs, lanes), jnp.float32)],
    )[0]


def scatter_tokens(tokens, place, sp_count, feats, piece):
    tok_here = tokens.shape[0]

    def body(place_ref, tokens_ref, *rest):
        out_refs, sem = rest[:-1], rest[-1]
        slot = place_ref[1] * 2 + place_ref[2]
        copies = []
        for shift in range(sp_count):
            target = lax.rem(place_ref[0] + shift, sp_count)
            column = pl.multiple_of(target * feats + slot * piece, piece)
            copy = pltpu.make_async_copy(
                tokens_ref.at[:, pl.ds(column, piece)], out_refs[shift], sem.at[shift]
            )
            copy.start()
            copies.append(copy)
        for copy in copies:
            copy.wait()

    return local_kernel(
        body,
        place,
        (),
        [shaped(tok_here, piece)] * sp_count,
        scratch=[pltpu.SemaphoreType.DMA((sp_count,))],
        hbm=(tokens,),
    )


def stack_blocks(blocks, place, parts=1, after=()):
    count = len(blocks)
    rows, width = blocks[0].shape
    rows = rows // parts

    def body(place_ref, *refs):
        for part in range(parts):
            for shift in range(count):
                source = lax.rem(place_ref[0] + count - shift, count)
                refs[count + part][aligned(source, rows), :] = refs[shift][
                    pl.ds(part * rows, rows), :
                ]

    return local_kernel(body, place, blocks, [shaped(rows * count, width)] * parts, after=after)


def over_sp(blocks, count):
    return [blocks[0]] + [
        lax.ppermute(blocks[shift], "sp", ring(count, shift)) for shift in range(1, count)
    ]


def scaled_by(slots, layer, feats, place_ref, piece_refs, gain_ref, out_ref):
    for piece_ref, slot in zip(piece_refs, slots):
        span = aligned(slot(place_ref[1], place_ref[2]), piece_ref.shape[1])
        start = pl.multiple_of(
            place_ref[0] * feats + slot(place_ref[1], place_ref[2]) * piece_ref.shape[1],
            piece_ref.shape[1],
        )
        factor = gain_ref[pl.ds(layer, 1), pl.ds(start, piece_ref.shape[1])].astype(jnp.float32)
        out_ref[:, span] = (piece_ref[...].astype(jnp.float32) * factor).astype(jnp.bfloat16)


def stage_weights(weights, layer, place, sp_count):
    feats, every_width = weights[0].shape[1:]
    width = every_width // sp_count
    count = len(weights)

    def body(place_ref, *refs):
        weight_refs, (out_ref, sem) = refs[:count], refs[count:]
        copies = []
        for chunk in range(sp_count):
            for index, weight_ref in enumerate(weight_refs):
                copy = pltpu.make_async_copy(
                    weight_ref.at[layer, :, pl.ds(chunk * width, width)],
                    out_ref.at[chunk, :, pl.ds(index * width, width)],
                    sem.at[chunk, index],
                )
                copy.start()
                copies.append(copy)
        for copy in copies:
            copy.wait()

    return local_kernel(
        body,
        place,
        (),
        [shaped(sp_count, feats, count * width)],
        scratch=[pltpu.SemaphoreType.DMA((sp_count, count))],
        hbm=weights,
    )[0]


EXTRA = 16


def put_squares(out_ref, squares, tok):
    for term in range(3):
        part = squares.astype(jnp.bfloat16)
        out_ref[pl.ds(tok, EXTRA), pl.ds(term * HD, HD)] = part
        squares = squares - part.astype(jnp.float32)


def get_squares(ref, tok):
    terms = [ref[pl.ds(tok, EXTRA), pl.ds(term * HD, HD)].astype(jnp.float32) for term in range(3)]
    return terms[0] + (terms[1] + terms[2])


def share(source, staged, layer, place, chunk_shift, arrived=None, others=None, extra=0):
    fresh = len(source) == 3
    sp_count, feats, total_width = staged.shape
    arrays = (*source[0], source[2]) if fresh else source
    tok = arrays[0].shape[0]
    count = len(arrays)
    inputs = (*arrays, staged)
    inputs += () if arrived is None else (arrived,)
    inputs += () if others is None else (others,)

    def body(place_ref, *refs):
        array_refs, staged_ref = refs[:count], refs[count]
        out_ref = refs[len(inputs)]
        if fresh:
            scaled_ref, squares_ref = refs[len(inputs) + 1 :]
            pieces, slots, _ = source
            scaled_by(
                slots,
                layer,
                feats,
                place_ref,
                array_refs[: len(pieces)],
                array_refs[len(pieces)],
                scaled_ref,
            )
            squares_ref[...] = jnp.zeros_like(squares_ref) if others is None else refs[count + 1][...]
            start = 0 if others is None else tok // HD
            for run in range(tok // HD):
                total = jnp.zeros((HD, HD), jnp.float32)
                for ref in array_refs[: len(pieces)]:
                    for lane in range(ref.shape[1] // HD):
                        part = ref[pl.ds(run * HD, HD), pl.ds(lane * HD, HD)].astype(jnp.float32)
                        total += part * part
                squares_ref[pl.ds(start + run, 1), :] = jnp.sum(total.T, axis=0, keepdims=True)
        else:
            scaled_ref, squares_ref = array_refs
        chunk = lax.rem(place_ref[0] + chunk_shift, sp_count)
        total = jnp.dot(scaled_ref[...], staged_ref[chunk], preferred_element_type=jnp.float32)
        if arrived is not None:
            total += refs[count + 1][pl.ds(0, tok), :].astype(jnp.float32)
        out_ref[pl.ds(0, tok), :] = total.astype(jnp.bfloat16)
        if extra:
            squares = squares_ref[...]
            if arrived is not None:
                squares += get_squares(refs[count + 1], tok)
            put_squares(out_ref, squares, tok)

    outs = [shaped(tok + extra, total_width)]
    if fresh:
        outs += [shaped(tok, feats), shaped(EXTRA, HD, dtype=jnp.float32)]
    return local_kernel(body, place, inputs, outs, flops=2 * tok * feats * total_width)


def own_share(scaled, staged, place):
    tok = scaled.shape[0]
    total_width = staged.shape[2]

    def body(place_ref, scaled_ref, staged_ref, out_ref):
        out_ref[...] = jnp.dot(
            scaled_ref[...], staged_ref[place_ref[0]], preferred_element_type=jnp.float32
        )

    return local_kernel(
        body,
        place,
        (scaled, staged),
        [shaped(tok, total_width, dtype=jnp.float32)],
        flops=2 * tok * scaled.shape[1] * total_width,
    )[0]


def attend_rows(qkv_ref, bias_ref, out_ref, part, sp_count, heads, layer):
    grid_rows = qkv_ref.shape[0] // GRID_W
    width = heads * HD
    part_grid = grid_rows // sp_count // 2
    done = []
    for head in range(heads):
        lanes = head * HD
        for plane in range(sp_count):
            rows = [(2 * plane + part) * part_grid + inner for inner in range(part_grid)]
            firsts = [min(max(row - KR // 2, 0), grid_rows - KR) for row in rows]
            low, reach = firsts[0], firsts[-1] - firsts[0] + KR
            queries = qkv_ref[pl.ds(rows[0] * GRID_W, part_grid * GRID_W), pl.ds(lanes, HD)]
            span = pl.ds(low * GRID_W, reach * GRID_W)
            keys = qkv_ref[span, pl.ds(width + lanes, HD)]
            values = qkv_ref[span, pl.ds(2 * width + lanes, HD)]
            scores = lax.dot_general(
                queries, keys, (((1,), (1,)), ((), ())), preferred_element_type=jnp.float32
            )
            biases = []
            for row, first in zip(rows, firsts):
                offset = low - row + KR - 1
                here = bias_ref[layer * heads + head, :, pl.ds(offset * GRID_W, reach * GRID_W)]
                if reach > KR:
                    key_row = lax.broadcasted_iota(jnp.int32, here.shape, 1) // GRID_W + low
                    here = jnp.where((key_row >= first) & (key_row < first + KR), here, -jnp.inf)
                biases.append(here)
            scores = scores * HD ** (-0.5) + jnp.concatenate(biases, axis=0)
            powers = jnp.exp(scores - jnp.max(scores, axis=-1, keepdims=True))
            weights = powers * (1.0 / jnp.sum(powers, axis=-1, keepdims=True))
            mixed = jnp.dot(
                weights.astype(jnp.bfloat16), values, preferred_element_type=jnp.float32
            )
            done.append((plane * part_grid * GRID_W, lanes, mixed.astype(jnp.bfloat16)))
    for at, lanes, block in done:
        out_ref[pl.ds(at, part_grid * GRID_W), pl.ds(lanes, HD)] = block


def attend(arrived, own, squares, bias, place, sp_count, heads, layer, every_feat, after):
    rows, total_width = own[0].shape
    width = heads * HD
    part_rows = rows // sp_count
    runs = rows // HD
    flops = 4 * heads * rows * KR * GRID_W * HD
    count = len(arrived[0])

    def low(place_ref, *refs):
        arrived_refs, refs = (refs[:count], refs[count : 2 * count]), refs[2 * count :]
        own_refs, (squares_ref, bias_ref, out_ref, qkv_ref) = refs[:2], refs[2:]
        squares = squares_ref[...]
        for ref in arrived_refs[1]:
            squares += get_squares(ref, rows)
        norm = lax.rsqrt(squares / every_feat + norm_eps)
        for part in range(2):
            for run in range(runs):
                at = part * runs + run
                factor = jnp.broadcast_to(norm[at : at + 1, :], (HD, HD)).T
                plane, inner = divmod(run * HD, part_rows)
                to = pl.ds((2 * plane + part) * part_rows + inner, HD)
                span = pl.ds(run * HD, HD)
                for lane in range(total_width // HD):
                    lanes = pl.ds(lane * HD, HD)
                    total = own_refs[part][span, lanes]
                    for ref in arrived_refs[part]:
                        total += ref[span, lanes].astype(jnp.float32)
                    qkv_ref[to, lanes] = (total * factor).astype(jnp.bfloat16)
        attend_rows(qkv_ref, bias_ref, out_ref, 0, sp_count, heads, layer)

    def high(place_ref, qkv_ref, bias_ref, out_ref):
        attend_rows(qkv_ref, bias_ref, out_ref, 1, sp_count, heads, layer)

    out0, qkv = local_kernel(
        low,
        place,
        (*arrived[0], *arrived[1], *own, squares, bias),
        [shaped(rows, width), shaped(2 * rows, total_width)],
        flops=flops,
        after=after,
    )
    out1 = local_kernel(high, place, (qkv, bias), [shaped(rows, width)], flops=flops)
    return out0, out1[0]


def spread(attended, w_out, layer, place, after):
    sp_count = lax.axis_size("sp")
    rows, width = attended[0].shape
    inner, feats = w_out.shape[1:]
    half = feats // 2

    def body(place_ref, *refs):
        piece_refs, (w_ref, sent_ref, kept_ref, gathered) = refs[:sp_count], refs[sp_count:]
        for shift in range(sp_count):
            source = lax.rem(place_ref[0] + sp_count - shift, sp_count)
            gathered[:, aligned(source, width)] = piece_refs[shift][...]
        core = place_ref[1]
        for index, out_ref in ((1 - core, sent_ref), (core, kept_ref)):
            out_ref[...] = jnp.dot(
                gathered[...],
                w_ref[layer, :, aligned(index, half)],
                preferred_element_type=jnp.float32,
            ).astype(jnp.bfloat16)

    return local_kernel(
        body,
        place,
        (*attended, w_out),
        [shaped(rows, half)] * 2,
        scratch=[pltpu.VMEM((rows, inner), jnp.bfloat16)],
        flops=2 * rows * inner * feats,
        after=after,
    )


def total_of(*refs):
    total = refs[0][...].astype(jnp.float32)
    for ref in refs[1:]:
        total += ref[...].astype(jnp.float32)
    return total


def pair_up(kept, came, place):
    def body(place_ref, kept_ref, came_ref, out_ref):
        out_ref[...] = total_of(kept_ref, came_ref).astype(jnp.bfloat16)

    return local_kernel(body, place, (kept, came), [shaped(*kept.shape)])


def pair_apart(kept, came, place):
    rows, half = kept.shape
    piece = half // 2

    def body(place_ref, kept_ref, came_ref, sent_ref, stay_ref):
        far = place_ref[2]
        for index, out_ref in ((1 - far, sent_ref), (far, stay_ref)):
            span = aligned(index, piece)
            out_ref[...] = (
                kept_ref[:, span].astype(jnp.float32) + came_ref[:, span].astype(jnp.float32)
            ).astype(jnp.bfloat16)

    return local_kernel(body, place, (kept, came), [shaped(rows, piece)] * 2)


def renew(residual, pair, came, place, after):
    count = len(residual)

    def body(place_ref, *refs):
        piece_refs, (pair_ref, came_ref, out_ref) = refs[:count], refs[count:]
        if count == 1:
            branch = total_of(pair_ref, came_ref)
            out_ref[...] = (piece_refs[0][...].astype(jnp.float32) + branch).astype(jnp.bfloat16)
            return
        far = place_ref[2]
        for index, ref in ((far, piece_refs[0]), (1 - far, piece_refs[1])):
            span = aligned(index, ref.shape[1])
            branch = pair_ref[:, span].astype(jnp.float32) + came_ref[:, span].astype(jnp.float32)
            out_ref[:, span] = (ref[...].astype(jnp.float32) + branch).astype(jnp.bfloat16)

    return local_kernel(body, place, (*residual, pair, came), [shaped(*pair.shape)], after=after)[0]


def finish(residual, stay, came, place, sp_count):
    rows, piece = stay.shape
    part = rows // sp_count

    def body(place_ref, x_ref, stay_ref, came_ref, *out_refs):
        for shift in range(sp_count):
            target = lax.rem(place_ref[0] + shift, sp_count)
            span = aligned(target, part)
            branch = stay_ref[span, :].astype(jnp.float32) + came_ref[span, :].astype(jnp.float32)
            x_here = x_ref[span, aligned(place_ref[2], piece)].astype(jnp.float32)
            out_refs[shift][...] = (x_here + branch).astype(jnp.bfloat16)

    return local_kernel(body, place, (residual, stay, came), [shaped(part, piece)] * sp_count)


SLOTS = (
    lambda core, far: core * 2 + far,
    lambda core, far: core * 2 + 1 - far,
    lambda core, far: (1 - core) * 2 + far,
    lambda core, far: (1 - core) * 2 + 1 - far,
)


HALF_SLOTS = (lambda core, far: core, lambda core, far: 1 - core)


def assemble(pieces, place, sp_count, index, so_far):
    rows, piece = pieces[0].shape
    part = rows // sp_count
    count = len(pieces)
    width = piece * count * sp_count
    earlier = () if so_far is None else (so_far,)

    def body(place_ref, *refs):
        out_ref, laid, sem = refs[-3:]
        for which in range(count):
            slot = SLOTS[which](place_ref[1], place_ref[2])
            for plane in range(sp_count):
                laid[:, aligned(plane * count + slot, piece)] = refs[which][
                    pl.ds(plane * part, part), :
                ]
        copy = pltpu.make_async_copy(laid, out_ref.at[pl.ds(index * part, part), :], sem)
        copy.start()
        copy.wait()

    vmem, hbm = pl.BlockSpec(memory_space=pltpu.VMEM), pl.BlockSpec(memory_space=pltpu.HBM)
    return pl.pallas_call(
        body,
        out_shape=shaped(2 * part, width),
        in_specs=[pl.BlockSpec(memory_space=pltpu.SMEM)] + [vmem] * count + [hbm] * len(earlier),
        out_specs=hbm,
        scratch_shapes=[pltpu.VMEM((part, width), jnp.bfloat16), pltpu.SemaphoreType.DMA],
        input_output_aliases={1 + count: 0} if earlier else {},
        compiler_params=pltpu.CompilerParams(vmem_limit_bytes=VMEM_BYTES),
        cost_estimate=pl.CostEstimate(flops=0, bytes_accessed=4 * part * width, transcendentals=0),
        name="assemble",
    )(place, *pieces, *earlier)


def exchanged(held):
    far = swapped(held, "tp", 2)
    near = swapped(held, "tp", 1)
    return [held, far, near, swapped(far, "tp", 1)]


def stationary_plan(tokens, norm_gain, w_query, w_key, w_value, w_out, offset_bias):
    sp_count = lax.axis_size("sp")
    sp_index, tp_index = lax.axis_index("sp"), lax.axis_index("tp")
    place = jnp.stack([sp_index, tp_index % 2, tp_index // 2]).astype(jnp.int32)
    feats = w_query.shape[1]
    heads = offset_bias.shape[1] // sp_count
    piece = feats // 4
    every_feat = feats * sp_count
    weights = (w_query, w_key, w_value)
    halves = [None, None]
    sources = [None, None]
    shifts = (1, -1)

    def sent_on(block, part):
        return lax.ppermute(block, "sp", ring(sp_count, shifts[part]))

    def made(layer, part, step, arrived=None):
        chunk = (-shifts[part] * (step + 1)) % sp_count
        others = sources[0][1] if part and not step else None
        extra = EXTRA if part else 0
        return share(sources[part], staged[layer], layer, place, chunk, arrived, others, extra)

    def first_made(layer, part):
        sources[part] = (halves[part], SLOTS if layer == 0 else HALF_SLOTS, norm_gain)
        block, scaled, squares = made(layer, part, 0)
        sources[part] = (scaled, squares)
        return block

    bias = window_bias(offset_bias, place, heads)
    staged = []
    for layer in range(LAYERS):
        staged.append(stage_weights(weights, layer, place, sp_count))
    blocks = over_sp(scatter_tokens(tokens, place, sp_count, feats, piece), sp_count)
    held = stack_blocks(blocks, place, 2, (bias, staged[0]))
    far = [swapped(h, "tp", 2) for h in held]
    near = [swapped(h, "tp", 1) for h in held]
    halves[0] = [held[0], far[0], near[0], swapped(far[0], "tp", 1)]
    first = [first_made(0, 0), None]
    far[1] = lax.optimization_barrier((far[1], first[0]))[0]
    near_far = swapped(far[1], "tp", 1)
    halves[1] = [held[1], far[1], near[1], near_far]
    first[1] = first_made(0, 1)

    for layer in range(LAYERS):
        travelling = [sent_on(first[part], part) for part in range(2)]
        for step in range(1, sp_count - 1):
            for part in range(2):
                block = made(layer, part, step, travelling[part])[0]
                travelling[part] = sent_on(block, part)
        own = []
        for part in range(2):
            own.append(own_share(sources[part][0], staged[layer], place))
        squares = sources[1][1]
        attended = attend(
            [travelling[:1], travelling[1:]],
            own,
            squares,
            bias,
            place,
            sp_count,
            heads,
            layer,
            every_feat,
            staged[layer + 1 : layer + 2],
        )

        residuals = [pieces[:2] if layer == 0 else pieces[:1] for pieces in halves]
        pairs, after = [], (attended[1],)
        for part in range(2):
            gathered = over_sp([attended[part]] * sp_count, sp_count)
            sent, kept = spread(gathered, w_out, layer, place, after)
            other = swapped(sent, "tp", 1)
            pair = (pair_up if layer < LAYERS - 1 else pair_apart)(kept, other, place)
            pairs.append((pair, swapped(pair[0], "tp", 2)))
            after = (pair[0],)
        after = ()
        for part in range(2):
            pair, other = pairs[part]
            if layer < LAYERS - 1:
                mine = renew(residuals[part], pair[0], other, place, after)
                halves[part] = [mine, swapped(mine, "tp", 1)]
                first[part] = first_made(layer + 1, part)
            else:
                blocks = finish(residuals[part][0], pair[1], other, place, sp_count)
                stacked = stack_blocks(over_sp(blocks, sp_count), place)[0]
                halves[part] = exchanged(stacked)
    mixed = None
    for part in range(2):
        mixed = assemble(halves[part], place, sp_count, part, mixed)
    return mixed


def on_device(tokens, norm_gain, w_query, w_key, w_value, w_out, offset_bias):
    heads_here, sp_count = offset_bias.shape[1], lax.axis_size("sp")
    part_rows = tokens.shape[0] // 2
    arrays = (tokens, norm_gain, w_query, w_key, w_value, w_out, offset_bias)
    if heads_here % sp_count == 0 and lax.axis_size("tp") == 4 and part_rows % HD == 0:
        return stationary_plan(*arrays)
    return gathered_plan(*arrays)


def solution(mesh):
    return jax.shard_map(
        on_device,
        mesh=mesh,
        in_specs=(
            P(("grp", "sp"), None),
            P(),
            P(None, "sp", "tp"),
            P(None, "sp", "tp"),
            P(None, "sp", "tp"),
            P(None, "tp", "sp"),
            P(None, "tp", None, None),
        ),
        out_specs=P(("grp", "sp"), None),
        check_vma=False,
    )
```

```python
import jax
import jax.numpy as jnp
from jax import lax
from jax.experimental import pallas as pl
from jax.experimental.pallas import tpu as pltpu
from jax.sharding import PartitionSpec as P


HD = 128
GRID_W = 64
KR = 8
KC = 16
LAYERS = 2


norm_eps = 1e-06


def with_halo(block, sides, width):
    for axis, dim in sides:
        count = lax.axis_size(axis)
        forward = [(i, i + 1) for i in range(count - 1)]
        backward = [(target, source) for source, target in forward]
        low = lax.ppermute(
            lax.slice_in_dim(block, block.shape[dim] - width, None, axis=dim), axis, forward
        )
        high = lax.ppermute(lax.slice_in_dim(block, 0, width, axis=dim), axis, backward)
        block = jnp.concatenate([low, block, high], axis=dim)
    return block


def rms_rows(values, gain):
    wide = values.astype(jnp.float32)
    scaled = wide * lax.rsqrt(jnp.mean(wide * wide, axis=-1, keepdims=True) + norm_eps)
    return (scaled * gain.astype(jnp.float32)).astype(jnp.bfloat16)


def gathered_plan(tokens, norm_gain, w_query, w_key, w_value, w_out, offset_bias):
    sp_count = lax.axis_size("sp")
    sp_index = lax.axis_index("sp")
    tok_rows = tokens.shape[0]
    local_rows = tok_rows // GRID_W
    grid_rows = local_rows * sp_count
    heads_here = offset_bias.shape[1]
    head_width = heads_here * HD
    reach = KR // 2
    scale = HD ** (-0.5)
    columns = jnp.arange(GRID_W, dtype=jnp.int32)
    col_first = jnp.clip(columns - KC // 2, 0, GRID_W - KC)
    col_inside = (columns[None, :] >= col_first[:, None]) & (
        columns[None, :] < col_first[:, None] + KC
    )
    col_offset = jnp.clip(columns[None, :] - columns[:, None], 1 - KC, KC - 1) + KC - 1
    col_onehot = (
        jnp.arange(2 * KC - 1, dtype=jnp.int32)[:, None, None] == col_offset[None, :, :]
    ).astype(jnp.float32)
    first_row = sp_index * local_rows
    own_rows = first_row + jnp.arange(local_rows, dtype=jnp.int32)
    row_first = jnp.clip(own_rows - reach, 0, grid_rows - KR)
    band_start = row_first - first_row + reach
    row_offset = (
        row_first[:, None] + jnp.arange(KR, dtype=jnp.int32)[None, :] - own_rows[:, None] + KR - 1
    )
    row_onehot = (
        row_offset[:, :, None] == jnp.arange(2 * KR - 1, dtype=jnp.int32)[None, None, :]
    ).astype(jnp.float32)
    every_query, every_key, every_value, every_out = (
        lax.all_gather(w_query, "sp", axis=1, tiled=True),
        lax.all_gather(w_key, "sp", axis=1, tiled=True),
        lax.all_gather(w_value, "sp", axis=1, tiled=True),
        lax.all_gather(w_out, "sp", axis=2, tiled=True),
    )
    residual = tokens
    for layer_index in range(LAYERS):
        normed = rms_rows(residual, norm_gain[layer_index])
        queries = jnp.dot(normed, every_query[layer_index], preferred_element_type=jnp.float32)
        keys = jnp.dot(normed, every_key[layer_index], preferred_element_type=jnp.float32)
        values = jnp.dot(normed, every_value[layer_index], preferred_element_type=jnp.float32)
        out_weight = every_out[layer_index]
        queries = queries.astype(jnp.bfloat16).reshape(local_rows, GRID_W, heads_here, HD)
        key_values = jnp.concatenate(
            [keys.astype(jnp.bfloat16), values.astype(jnp.bfloat16)], axis=1
        )
        key_values = key_values.reshape(local_rows, GRID_W, 2 * head_width)
        padded = with_halo(key_values, (("sp", 0),), reach)
        bands = jax.vmap(lambda band_begin: lax.dynamic_slice_in_dim(padded, band_begin, KR, 0))(
            band_start
        )
        band_keys = bands[..., :head_width].reshape(local_rows, KR, GRID_W, heads_here, HD)
        band_values = bands[..., head_width:].reshape(local_rows, KR, GRID_W, heads_here, HD)
        col_bias = jnp.einsum(
            "hro,oqk->hrqk", offset_bias[layer_index], col_onehot, precision=lax.Precision.HIGHEST
        )
        full_bias = jnp.einsum(
            "ijr,hrqk->hiqjk", row_onehot, col_bias, precision=lax.Precision.HIGHEST
        )
        scores = jnp.einsum(
            "iqhd,ijkhd->hiqjk", queries, band_keys, preferred_element_type=jnp.float32
        )
        scores = scores * scale + full_bias
        scores = jnp.where(col_inside[None, None, :, None, :], scores, -jnp.inf)
        flattened = scores.reshape(heads_here, local_rows, GRID_W, KR * GRID_W)
        weights = jax.nn.softmax(flattened, axis=-1).astype(jnp.bfloat16)
        weights = weights.reshape(heads_here, local_rows, GRID_W, KR, GRID_W)
        attended = jnp.einsum(
            "hiqjk,ijkhd->iqhd", weights, band_values, preferred_element_type=jnp.float32
        )
        attended = attended.astype(jnp.bfloat16).reshape(tok_rows, head_width)
        branch = lax.psum(
            jnp.dot(attended, out_weight, preferred_element_type=jnp.float32).astype(jnp.bfloat16),
            "tp",
        ).astype(jnp.float32)
        residual = (residual.astype(jnp.float32) + branch).astype(jnp.bfloat16)
    return residual


VMEM_BYTES = 24 * 1024 * 1024


def ring(count, shift):
    return [(i, (i + shift) % count) for i in range(count)]


def fold(count):
    return [2 * i if 2 * i < count else 2 * (count - 1 - i) + 1 for i in range(count)]


def folded_ring(count, shift):
    order = fold(count)
    return [(order[i], order[(i + shift) % count]) for i in range(count)]


def swapped(array, axis, distance):
    count = lax.axis_size(axis)
    return lax.ppermute(array, axis, [(i, i ^ distance) for i in range(count)])


def aligned(index, size):
    return pl.ds(pl.multiple_of(index * size, size), size)


def local_kernel(body, place, arrays, outs, scratch=(), hbm=(), flops=0, after=()):
    vmem, smem = pl.BlockSpec(memory_space=pltpu.VMEM), pl.BlockSpec(memory_space=pltpu.SMEM)
    moved = sum(a.size * a.dtype.itemsize for a in (*arrays, *outs))
    inputs = 1 + len(arrays) + len(hbm)

    def ordered(*refs):
        body(*refs[:inputs], *refs[inputs + len(after) :])

    return pl.pallas_call(
        ordered,
        out_shape=list(outs),
        in_specs=[smem]
        + [vmem] * len(arrays)
        + [pl.BlockSpec(memory_space=pltpu.HBM)] * len(hbm)
        + [pl.BlockSpec(memory_space=pl.ANY)] * len(after),
        out_specs=[vmem] * len(outs),
        scratch_shapes=list(scratch),
        compiler_params=pltpu.CompilerParams(vmem_limit_bytes=VMEM_BYTES),
        cost_estimate=pl.CostEstimate(flops=flops, bytes_accessed=moved, transcendentals=0),
    )(place, *arrays, *(pltpu.with_memory_space_constraint(a, pltpu.HBM) for a in hbm), *after)


def shaped(*shape, dtype=jnp.bfloat16):
    return jax.ShapeDtypeStruct(shape, dtype)


def window_bias(offset_bias, place, heads):
    layers, _, offsets, reach = offset_bias.shape
    pairs = -(-offsets // 2)
    lanes = 2 * GRID_W

    def body(place_ref, table_ref, out_ref, padded):
        padded[...] = jnp.zeros_like(padded)
        lane = lax.broadcasted_iota(jnp.int32, (GRID_W, lanes), 1)
        query = lax.broadcasted_iota(jnp.int32, (GRID_W, lanes), 0)
        column = jnp.where(lane < GRID_W, lane, lane - GRID_W)
        first = jnp.clip(query - KC // 2, 0, GRID_W - KC)
        inside = (column >= first) & (column < first + KC)
        for layer in range(layers):
            for head in range(heads):
                padded[pl.ds(0, offsets), pl.ds(0, reach)] = table_ref[
                    layer, place_ref[0] * heads + head
                ]
                for pair in range(pairs):
                    sides = []
                    for side in range(2):
                        row = jnp.broadcast_to(
                            padded[pl.ds(2 * pair + side, 1), :], (GRID_W, lanes)
                        )
                        start = (side * GRID_W - (KC - 1)) % lanes
                        sides.append(pltpu.roll(row, start, 1, stride=1, stride_axis=0))
                    both = jnp.where(lane < GRID_W, sides[0], sides[1])
                    out_ref[layer * heads + head, :, pl.ds(pair * lanes, lanes)] = jnp.where(
                        inside, both, -jnp.inf
                    )

    return local_kernel(
        body,
        place,
        (offset_bias,),
        [shaped(layers * heads, GRID_W, pairs * lanes, dtype=jnp.float32)],
        scratch=[pltpu.VMEM((2 * pairs, lanes), jnp.float32)],
    )[0]


def scatter_tokens(tokens, place, sp_count, feats, piece):
    rows = tokens.shape[0] // 2

    def body(place_ref, tokens_ref, *rest):
        out_refs, sem = rest[:-1], rest[-1]
        slot = place_ref[1] * 2 + place_ref[2]
        copies = []
        for part, shift in [(part, shift) for part in range(2) for shift in range(sp_count)]:
            target = lax.rem(place_ref[0] + shift, sp_count)
            column = pl.multiple_of(target * feats + slot * piece, piece)
            copy = pltpu.make_async_copy(
                tokens_ref.at[pl.ds(part * rows, rows), pl.ds(column, piece)],
                out_refs[part * sp_count + shift],
                sem.at[part, shift],
            )
            copy.start()
            copies.append(copy)
        for copy in copies:
            copy.wait()

    blocks = local_kernel(
        body,
        place,
        (),
        [shaped(rows, piece)] * (2 * sp_count),
        scratch=[pltpu.SemaphoreType.DMA((2, sp_count))],
        hbm=(tokens,),
    )
    return blocks[:sp_count], blocks[sp_count:]


def stack_blocks(blocks, place, parts=1, after=()):
    count = len(blocks)
    rows, width = blocks[0].shape
    rows = rows // parts

    def body(place_ref, *refs):
        for part in range(parts):
            for shift in range(count):
                source = lax.rem(place_ref[0] + count - shift, count)
                refs[count + part][aligned(source, rows), :] = refs[shift][
                    pl.ds(part * rows, rows), :
                ]

    return local_kernel(body, place, blocks, [shaped(rows * count, width)] * parts, after=after)


def over_sp(blocks, count):
    return [blocks[0]] + [
        lax.ppermute(blocks[shift], "sp", ring(count, shift)) for shift in range(1, count)
    ]


def scaled_by(slots, layer, feats, place_ref, piece_refs, gain_ref, out_ref):
    for piece_ref, slot in zip(piece_refs, slots):
        span = aligned(slot(place_ref[1], place_ref[2]), piece_ref.shape[1])
        start = pl.multiple_of(
            place_ref[0] * feats + slot(place_ref[1], place_ref[2]) * piece_ref.shape[1],
            piece_ref.shape[1],
        )
        factor = gain_ref[pl.ds(layer, 1), pl.ds(start, piece_ref.shape[1])].astype(jnp.float32)
        out_ref[:, span] = (piece_ref[...].astype(jnp.float32) * factor).astype(jnp.bfloat16)


def stage_weights(weights, layer, place, sp_count):
    feats, every_width = weights[0].shape[1:]
    width = every_width // sp_count
    count = len(weights)

    def body(place_ref, *refs):
        weight_refs, (out_ref, sem) = refs[:count], refs[count:]
        copies = []
        for chunk in range(sp_count):
            for index, weight_ref in enumerate(weight_refs):
                copy = pltpu.make_async_copy(
                    weight_ref.at[layer, :, pl.ds(chunk * width, width)],
                    out_ref.at[chunk, :, pl.ds(index * width, width)],
                    sem.at[chunk, index],
                )
                copy.start()
                copies.append(copy)
        for copy in copies:
            copy.wait()

    return local_kernel(
        body,
        place,
        (),
        [shaped(sp_count, feats, count * width)],
        scratch=[pltpu.SemaphoreType.DMA((sp_count, count))],
        hbm=weights,
    )[0]


EXTRA = 16


def put_squares(out_ref, squares, tok):
    for term in range(3):
        part = squares.astype(jnp.bfloat16)
        out_ref[pl.ds(tok, EXTRA), pl.ds(term * HD, HD)] = part
        squares = squares - part.astype(jnp.float32)


def get_squares(ref, tok):
    terms = [ref[pl.ds(tok, EXTRA), pl.ds(term * HD, HD)].astype(jnp.float32) for term in range(3)]
    return terms[0] + (terms[1] + terms[2])


def share(source, staged, layer, place, chunk_shift, arrived=None, others=None, extra=0):
    fresh = len(source) == 3
    sp_count, feats, total_width = staged.shape
    arrays = (*source[0], source[2]) if fresh else source
    tok = arrays[0].shape[0]
    count = len(arrays)
    inputs = (*arrays, staged)
    inputs += () if arrived is None else (arrived,)
    inputs += () if others is None else (others,)

    def body(place_ref, *refs):
        array_refs, staged_ref = refs[:count], refs[count]
        out_ref = refs[len(inputs)]
        if fresh:
            scaled_ref, squares_ref = refs[len(inputs) + 1 :]
            pieces, slots, _ = source
            scaled_by(
                slots,
                layer,
                feats,
                place_ref,
                array_refs[: len(pieces)],
                array_refs[len(pieces)],
                scaled_ref,
            )
            squares_ref[...] = jnp.zeros_like(squares_ref) if others is None else refs[count + 1][...]
            start = 0 if others is None else tok // HD
            for run in range(tok // HD):
                total = jnp.zeros((HD, HD), jnp.float32)
                for ref in array_refs[: len(pieces)]:
                    for lane in range(ref.shape[1] // HD):
                        part = ref[pl.ds(run * HD, HD), pl.ds(lane * HD, HD)].astype(jnp.float32)
                        total += part * part
                squares_ref[pl.ds(start + run, 1), :] = jnp.sum(total.T, axis=0, keepdims=True)
        else:
            scaled_ref, squares_ref = array_refs
        at = lax.rem(place_ref[3] + chunk_shift, sp_count)
        chunk = jnp.where(2 * at < sp_count, 2 * at, 2 * (sp_count - 1 - at) + 1)
        total = jnp.dot(scaled_ref[...], staged_ref[chunk], preferred_element_type=jnp.float32)
        if arrived is not None:
            total += refs[count + 1][pl.ds(0, tok), :].astype(jnp.float32)
        out_ref[pl.ds(0, tok), :] = total.astype(jnp.bfloat16)
        if extra:
            squares = squares_ref[...]
            if arrived is not None:
                squares += get_squares(refs[count + 1], tok)
            put_squares(out_ref, squares, tok)

    outs = [shaped(tok + extra, total_width)]
    if fresh:
        outs += [shaped(tok, feats), shaped(EXTRA, HD, dtype=jnp.float32)]
    return local_kernel(body, place, inputs, outs, flops=2 * tok * feats * total_width)


def own_share(scaled, staged, place):
    tok = scaled.shape[0]
    total_width = staged.shape[2]

    def body(place_ref, scaled_ref, staged_ref, out_ref):
        out_ref[...] = jnp.dot(
            scaled_ref[...], staged_ref[place_ref[0]], preferred_element_type=jnp.float32
        )

    return local_kernel(
        body,
        place,
        (scaled, staged),
        [shaped(tok, total_width, dtype=jnp.float32)],
        flops=2 * tok * scaled.shape[1] * total_width,
    )[0]


def attend_rows(qkv_ref, bias_ref, out_ref, part, sp_count, heads, layer):
    grid_rows = qkv_ref.shape[0] // GRID_W
    width = heads * HD
    part_grid = grid_rows // sp_count // 2
    done = []
    for head in range(heads):
        lanes = head * HD
        for plane in range(sp_count):
            rows = [(2 * plane + part) * part_grid + inner for inner in range(part_grid)]
            firsts = [min(max(row - KR // 2, 0), grid_rows - KR) for row in rows]
            low, reach = firsts[0], firsts[-1] - firsts[0] + KR
            queries = qkv_ref[pl.ds(rows[0] * GRID_W, part_grid * GRID_W), pl.ds(lanes, HD)]
            span = pl.ds(low * GRID_W, reach * GRID_W)
            keys = qkv_ref[span, pl.ds(width + lanes, HD)]
            values = qkv_ref[span, pl.ds(2 * width + lanes, HD)]
            scores = lax.dot_general(
                queries, keys, (((1,), (1,)), ((), ())), preferred_element_type=jnp.float32
            )
            biases = []
            for row, first in zip(rows, firsts):
                offset = low - row + KR - 1
                here = bias_ref[layer * heads + head, :, pl.ds(offset * GRID_W, reach * GRID_W)]
                if reach > KR:
                    key_row = lax.broadcasted_iota(jnp.int32, here.shape, 1) // GRID_W + low
                    here = jnp.where((key_row >= first) & (key_row < first + KR), here, -jnp.inf)
                biases.append(here)
            scores = scores * HD ** (-0.5) + jnp.concatenate(biases, axis=0)
            powers = jnp.exp(scores - jnp.max(scores, axis=-1, keepdims=True))
            weights = powers * (1.0 / jnp.sum(powers, axis=-1, keepdims=True))
            mixed = jnp.dot(
                weights.astype(jnp.bfloat16), values, preferred_element_type=jnp.float32
            )
            done.append((plane * part_grid * GRID_W, lanes, mixed.astype(jnp.bfloat16)))
    for at, lanes, block in done:
        out_ref[pl.ds(at, part_grid * GRID_W), pl.ds(lanes, HD)] = block


def attend(arrived, own, squares, bias, place, sp_count, heads, layer, every_feat, after):
    rows, total_width = own[0].shape
    width = heads * HD
    part_rows = rows // sp_count
    runs = rows // HD
    flops = 4 * heads * rows * KR * GRID_W * HD
    count = len(arrived[0])

    def low(place_ref, *refs):
        arrived_refs, refs = (refs[:count], refs[count : 2 * count]), refs[2 * count :]
        own_refs, (squares_ref, bias_ref, out_ref, qkv_ref) = refs[:2], refs[2:]
        squares = squares_ref[...]
        for ref in arrived_refs[1]:
            squares += get_squares(ref, rows)
        norm = lax.rsqrt(squares / every_feat + norm_eps)
        for part in range(2):
            for run in range(runs):
                at = part * runs + run
                factor = jnp.broadcast_to(norm[at : at + 1, :], (HD, HD)).T
                plane, inner = divmod(run * HD, part_rows)
                to = pl.ds((2 * plane + part) * part_rows + inner, HD)
                span = pl.ds(run * HD, HD)
                for lane in range(total_width // HD):
                    lanes = pl.ds(lane * HD, HD)
                    total = own_refs[part][span, lanes]
                    for ref in arrived_refs[part]:
                        total += ref[span, lanes].astype(jnp.float32)
                    qkv_ref[to, lanes] = (total * factor).astype(jnp.bfloat16)
        attend_rows(qkv_ref, bias_ref, out_ref, 0, sp_count, heads, layer)

    def high(place_ref, qkv_ref, bias_ref, out_ref):
        attend_rows(qkv_ref, bias_ref, out_ref, 1, sp_count, heads, layer)

    out0, qkv = local_kernel(
        low,
        place,
        (*arrived[0], *arrived[1], *own, squares, bias),
        [shaped(rows, width), shaped(2 * rows, total_width)],
        flops=flops,
        after=after,
    )
    out1 = local_kernel(high, place, (qkv, bias), [shaped(rows, width)], flops=flops)
    return out0, out1[0]


def spread(attended, w_out, layer, place, after):
    sp_count = lax.axis_size("sp")
    rows, width = attended[0].shape
    inner, feats = w_out.shape[1:]
    half = feats // 2

    def body(place_ref, *refs):
        piece_refs, (w_ref, sent_ref, kept_ref, gathered) = refs[:sp_count], refs[sp_count:]
        for shift in range(sp_count):
            source = lax.rem(place_ref[0] + sp_count - shift, sp_count)
            gathered[:, aligned(source, width)] = piece_refs[shift][...]
        core = place_ref[1]
        for index, out_ref in ((1 - core, sent_ref), (core, kept_ref)):
            out_ref[...] = jnp.dot(
                gathered[...],
                w_ref[layer, :, aligned(index, half)],
                preferred_element_type=jnp.float32,
            ).astype(jnp.bfloat16)

    return local_kernel(
        body,
        place,
        (*attended, w_out),
        [shaped(rows, half)] * 2,
        scratch=[pltpu.VMEM((rows, inner), jnp.bfloat16)],
        flops=2 * rows * inner * feats,
        after=after,
    )


def total_of(*refs):
    total = refs[0][...].astype(jnp.float32)
    for ref in refs[1:]:
        total += ref[...].astype(jnp.float32)
    return total


def pair_up(kept, came, place):
    def body(place_ref, kept_ref, came_ref, out_ref):
        out_ref[...] = total_of(kept_ref, came_ref).astype(jnp.bfloat16)

    return local_kernel(body, place, (kept, came), [shaped(*kept.shape)])


def pair_apart(kept, came, place):
    rows, half = kept.shape
    piece = half // 2

    def body(place_ref, kept_ref, came_ref, sent_ref, stay_ref):
        far = place_ref[2]
        for index, out_ref in ((1 - far, sent_ref), (far, stay_ref)):
            span = aligned(index, piece)
            out_ref[...] = (
                kept_ref[:, span].astype(jnp.float32) + came_ref[:, span].astype(jnp.float32)
            ).astype(jnp.bfloat16)

    return local_kernel(body, place, (kept, came), [shaped(rows, piece)] * 2)


def renew(residual, pair, came, place, after):
    count = len(residual)

    def body(place_ref, *refs):
        piece_refs, (pair_ref, came_ref, out_ref) = refs[:count], refs[count:]
        if count == 1:
            branch = total_of(pair_ref, came_ref)
            out_ref[...] = (piece_refs[0][...].astype(jnp.float32) + branch).astype(jnp.bfloat16)
            return
        far = place_ref[2]
        for index, ref in ((far, piece_refs[0]), (1 - far, piece_refs[1])):
            span = aligned(index, ref.shape[1])
            branch = pair_ref[:, span].astype(jnp.float32) + came_ref[:, span].astype(jnp.float32)
            out_ref[:, span] = (ref[...].astype(jnp.float32) + branch).astype(jnp.bfloat16)

    return local_kernel(body, place, (*residual, pair, came), [shaped(*pair.shape)], after=after)[0]


def finish(residual, stay, came, place, sp_count):
    rows, piece = stay.shape
    part = rows // sp_count

    def body(place_ref, x_ref, stay_ref, came_ref, *out_refs):
        for shift in range(sp_count):
            target = lax.rem(place_ref[0] + shift, sp_count)
            span = aligned(target, part)
            branch = stay_ref[span, :].astype(jnp.float32) + came_ref[span, :].astype(jnp.float32)
            x_here = x_ref[span, aligned(place_ref[2], piece)].astype(jnp.float32)
            out_refs[shift][...] = (x_here + branch).astype(jnp.bfloat16)

    return local_kernel(body, place, (residual, stay, came), [shaped(part, piece)] * sp_count)


SLOTS = (
    lambda core, far: core * 2 + far,
    lambda core, far: core * 2 + 1 - far,
    lambda core, far: (1 - core) * 2 + far,
    lambda core, far: (1 - core) * 2 + 1 - far,
)


HALF_SLOTS = (lambda core, far: core, lambda core, far: 1 - core)


def assemble(pieces, place, sp_count, index, so_far):
    rows, piece = pieces[0].shape
    part = rows // sp_count
    count = len(pieces)
    width = piece * count * sp_count
    earlier = () if so_far is None else (so_far,)

    def body(place_ref, *refs):
        out_ref, laid, sem = refs[-3:]
        for which in range(count):
            slot = SLOTS[which](place_ref[1], place_ref[2])
            for plane in range(sp_count):
                laid[:, aligned(plane * count + slot, piece)] = refs[which][
                    pl.ds(plane * part, part), :
                ]
        copy = pltpu.make_async_copy(laid, out_ref.at[pl.ds(index * part, part), :], sem)
        copy.start()
        copy.wait()

    vmem, hbm = pl.BlockSpec(memory_space=pltpu.VMEM), pl.BlockSpec(memory_space=pltpu.HBM)
    return pl.pallas_call(
        body,
        out_shape=shaped(2 * part, width),
        in_specs=[pl.BlockSpec(memory_space=pltpu.SMEM)] + [vmem] * count + [hbm] * len(earlier),
        out_specs=hbm,
        scratch_shapes=[pltpu.VMEM((part, width), jnp.bfloat16), pltpu.SemaphoreType.DMA],
        input_output_aliases={1 + count: 0} if earlier else {},
        compiler_params=pltpu.CompilerParams(vmem_limit_bytes=VMEM_BYTES),
        cost_estimate=pl.CostEstimate(flops=0, bytes_accessed=4 * part * width, transcendentals=0),
        name="assemble",
    )(place, *pieces, *earlier)


def exchanged(held):
    far = swapped(held, "tp", 2)
    near = swapped(held, "tp", 1)
    return [held, far, near, swapped(far, "tp", 1)]


def stationary_plan(tokens, norm_gain, w_query, w_key, w_value, w_out, offset_bias):
    sp_count = lax.axis_size("sp")
    sp_index, tp_index = lax.axis_index("sp"), lax.axis_index("tp")
    folded = jnp.where(sp_index % 2 == 0, sp_index // 2, sp_count - 1 - sp_index // 2)
    place = jnp.stack([sp_index, tp_index % 2, tp_index // 2, folded]).astype(jnp.int32)
    feats = w_query.shape[1]
    heads = offset_bias.shape[1] // sp_count
    piece = feats // 4
    every_feat = feats * sp_count
    weights = (w_query, w_key, w_value)
    halves = [None, None]
    sources = [None, None]
    shifts = (-1, -1)

    def sent_on(block, part):
        return lax.ppermute(block, "sp", folded_ring(sp_count, shifts[part]))

    def made(layer, part, step, arrived=None):
        chunk = (-shifts[part] * (step + 1)) % sp_count
        others = sources[0][1] if part and not step else None
        extra = EXTRA if part else 0
        return share(sources[part], staged[layer], layer, place, chunk, arrived, others, extra)

    def first_made(layer, part):
        sources[part] = (halves[part], SLOTS if layer == 0 else HALF_SLOTS, norm_gain)
        block, scaled, squares = made(layer, part, 0)
        sources[part] = (scaled, squares)
        return block

    bias = window_bias(offset_bias, place, heads)
    staged = []
    for layer in range(LAYERS):
        staged.append(stage_weights(weights, layer, place, sp_count))
    held, far = [], []
    for part, blocks in enumerate(scatter_tokens(tokens, place, sp_count, feats, piece)):
        blocks = over_sp(blocks, sp_count)
        held += stack_blocks(blocks, place)
        far.append(swapped(held[part], "tp", 2))
    near = [swapped(h, "tp", 1) for h in held]
    near_far = swapped(far[0], "tp", 1)
    halves[0] = [held[0], far[0], near[0], near_far]
    first = [first_made(0, 0), None]
    far[1] = lax.optimization_barrier((far[1], first[0]))[0]
    near_far = swapped(far[1], "tp", 1)
    halves[1] = [held[1], far[1], near[1], near_far]
    first[1] = first_made(0, 1)

    for layer in range(LAYERS):
        travelling = [sent_on(first[part], part) for part in range(2)]
        for step in range(1, sp_count - 1):
            for part in range(2):
                block = made(layer, part, step, travelling[part])[0]
                travelling[part] = sent_on(block, part)
        own = []
        for part in range(2):
            own.append(own_share(sources[part][0], staged[layer], place))
        squares = sources[1][1]
        attended = attend(
            [travelling[:1], travelling[1:]],
            own,
            squares,
            bias,
            place,
            sp_count,
            heads,
            layer,
            every_feat,
            staged[layer + 1 : layer + 2],
        )

        residuals = [pieces[:2] if layer == 0 else pieces[:1] for pieces in halves]
        pairs, after = [], (attended[1],)
        for part in range(2):
            gathered = over_sp([attended[part]] * sp_count, sp_count)
            sent, kept = spread(gathered, w_out, layer, place, after)
            other = swapped(sent, "tp", 1)
            pair = (pair_up if layer < LAYERS - 1 else pair_apart)(kept, other, place)
            pairs.append((pair, swapped(pair[0], "tp", 2)))
            after = (pair[0],)
        after = ()
        for part in range(2):
            pair, other = pairs[part]
            if layer < LAYERS - 1:
                mine = renew(residuals[part], pair[0], other, place, after)
                halves[part] = [mine, swapped(mine, "tp", 1)]
                first[part] = first_made(layer + 1, part)
            else:
                blocks = finish(residuals[part][0], pair[1], other, place, sp_count)
                stacked = stack_blocks(over_sp(blocks, sp_count), place)[0]
                halves[part] = exchanged(stacked)
    mixed = None
    for part in range(2):
        mixed = assemble(halves[part], place, sp_count, part, mixed)
    return mixed


def on_device(tokens, norm_gain, w_query, w_key, w_value, w_out, offset_bias):
    heads_here, sp_count = offset_bias.shape[1], lax.axis_size("sp")
    part_rows = tokens.shape[0] // 2
    arrays = (tokens, norm_gain, w_query, w_key, w_value, w_out, offset_bias)
    if heads_here % sp_count == 0 and lax.axis_size("tp") == 4 and part_rows % HD == 0:
        return stationary_plan(*arrays)
    return gathered_plan(*arrays)


def solution(mesh):
    return jax.shard_map(
        on_device,
        mesh=mesh,
        in_specs=(
            P(("grp", "sp"), None),
            P(),
            P(None, "sp", "tp"),
            P(None, "sp", "tp"),
            P(None, "sp", "tp"),
            P(None, "tp", "sp"),
            P(None, "tp", None, None),
        ),
        out_specs=P(("grp", "sp"), None),
        check_vma=False,
    )
```
